256 devices in a mesh: sp: 64 (over z, x, core), tp: 4 (over y).
Axes of the slice: x: 4, y: 4, z: 8, core: 2. Of those that a mesh axis runs over, the one named last changes fastest.
Arguments:
- mixer_input: bfloat16 [8192, 512], P('sp', 'tp'), may hold values from -8 to 8
- step_shift: float32 [8192, 32], P('sp', 'tp')
- log_step: float32 [32], P('tp'), may hold values from -12 to -1
- decay_real: float32 [32, 64], P('tp'), may hold values from -0.7 to -0.35
- freq_imag: float32 [32, 64], P('tp'), may hold values from 0 to 201.0624
- in_real: float32 [32, 64, 16], P('tp'), may hold values from -1 to 1
- in_imag: float32 [32, 64, 16], P('tp'), may hold values from -1 to 1
- out_real: float32 [32, 16, 64], P('tp'), may hold values from -0.75 to 0.75
- out_imag: float32 [32, 16, 64], P('tp'), may hold values from -0.75 to 0.75
- skip_gain: float32 [512], P('tp'), may hold values from -4 to 4
- out_weight: bfloat16 [512, 2048], P('tp'), may hold values from -0.25 to 0.25
- residual: bfloat16 [8192, 2048], P(('sp', 'tp')), may hold values from -6 to 6
- post_gain: float32 [2048], replicated, may hold values from 0.1 to 1.9
- pre_gain: float32 [2048], replicated, may hold values from 0.1 to 1.9
- final_gain: float32 [2048], replicated, may hold values from 0.1 to 1.9
- route_ids: int32 [8192, 2], P('sp'), may hold values from 0 to 63, all different within a row; in each aligned block of 32 rows (0 to 31, 32 to 63, ...) at most 2 rows name the same one
- route_logits: float32 [8192, 2], P('sp'), may hold values from -8 to 8
- expert_gate: bfloat16 [64, 2048, 3584], P('sp', None, 'tp'), may hold values from -0.125 to 0.125
- expert_up: bfloat16 [64, 2048, 3584], P('sp', None, 'tp'), may hold values from -0.125 to 0.125
- expert_down: bfloat16 [64, 3584, 2048], P('sp', 'tp'), may hold values from -0.09375 to 0.09375
Outputs:
- layer_out: bfloat16 [8192, 2048], P(('sp', 'tp'))
The draws below stay inside these ranges and needn't reach their ends.
Inputs may be any that keep to these rules, and one draw needn't show every extreme that they name: `route_ids`: each row names 2 different experts; in the 32 rows of one device no expert is named more than 2 times, a bound that some block reaches in some devices' rows.
All inputs are finite; a program needn't handle non-finite values.
Results may differ from the reference program's by a relative error of at most 0.0095.
Values may be sent and summed in bfloat16 or wider, within the bound.
No kernel may reach another device: no remote copies, remote signals or barrier semaphores. Data moves between devices by JAX's collectives and lax.ppermute only.
A program may use at most 64 MiB of HBM per device.

```python
import math
import jax
import jax.numpy as jnp
import numpy as np
from jax import lax

D = 2048
GROUPS = 32
CH = 16
N_STATE = 64
EXP_W = 3584
TOP = 2
TOK_DEV = 128
S5W = 512
SEQUENCE_TOKENS = 8192
ROW_DEV = 32
EXPERTS = 64
CAP = 2
N_TP = 4


def draw_mixer_input(key, part):
    noise_key, offset_key = jax.random.split(key)
    jitter_vals = jnp.clip(jax.random.normal(noise_key, (SEQUENCE_TOKENS, S5W), jnp.float32), -6.0, 6.0)
    offset = jax.random.uniform(offset_key, (S5W,), jnp.float32, -1.2, 1.2)
    return (jitter_vals + offset[None, :]).astype(jnp.bfloat16)


def draw_step_shift(key, part):
    block_random_key, wobble_random_key, spike_random_key = jax.random.split(key, 3)
    blocks = SEQUENCE_TOKENS // TOK_DEV
    block_noise_level = jax.random.uniform(block_random_key, (blocks, 1, 1), jnp.float32, math.log(0.6), math.log(1.6))
    block_noise_level = jnp.broadcast_to(block_noise_level, (blocks, TOK_DEV, GROUPS)).reshape(SEQUENCE_TOKENS, GROUPS)
    wobble_portion = jax.random.uniform(wobble_random_key, (SEQUENCE_TOKENS, GROUPS), jnp.float32, -0.3, 0.3)
    spike_locations = jax.random.randint(spike_random_key, (4,), 0, SEQUENCE_TOKENS)
    location_mask = jnp.any(jnp.arange(SEQUENCE_TOKENS)[:, None] == spike_locations[None, :], axis=1)
    spike_magnitude = math.log(0.4 * SEQUENCE_TOKENS)
    return (block_noise_level + wobble_portion + jnp.where(location_mask[:, None], spike_magnitude, 0.0)).astype(jnp.float32)


def draw_log_step(key, part):
    pick_key, fast_key, slow_key = jax.random.split(key, 3)
    fast_share = 0.5
    is_fast = jax.random.uniform(pick_key, (GROUPS,), jnp.float32) < fast_share
    fast_value = jnp.log(jax.random.uniform(fast_key, (GROUPS,), jnp.float32, 0.05, 0.15))
    slow_value = jnp.log(jax.random.uniform(slow_key, (GROUPS,), jnp.float32, 1.0, 2.3) / SEQUENCE_TOKENS)
    return jnp.where(is_fast, fast_value, slow_value).astype(jnp.float32)


def level_of(stream_key, dims, shards, least, top_value):
    factor_of = 1.0
    for position, parts in shards:
        heights = jax.random.uniform(jax.random.fold_in(jax.random.fold_in(stream_key, 6), position), (parts,), jnp.float32, least / len(shards), top_value / len(shards))
        factor_of = factor_of * jnp.repeat(jnp.exp(heights), dims[position] // parts).reshape((-1,) + (1,) * (len(dims) - 1 - position))
    return factor_of


def deal_out(own_key, own, number, rows, count, top, most, slope):
    sequence = jax.random.permutation(own_key, count)
    packed, usual = load_shares(count, rows * top, most, slope, True), load_shares(count, rows * top, most, slope, False)
    places = jnp.arange(count)

    def named(tallies, offset_by):
        used = int((tallies > 0).sum())
        fixed = max(1, used // 4)
        shifted = fixed + (places - fixed + offset_by * (used - fixed)) % max(1, count - fixed)
        return jnp.zeros((count,), jnp.int32).at[sequence[jnp.where(places < fixed, places, shifted)]].set(jnp.asarray(tallies, jnp.int32))

    tallies = jnp.where(number % 4 == 0, named(packed, number // 4), named(usual, number - number // 4 - 1))
    mixed = jax.random.permutation(jax.random.fold_in(own, 3), count)
    source_of, sink = mixed[0:count // 2 * 2:2], mixed[1:count // 2 * 2:2]
    room = jnp.minimum(tallies[source_of] - 1, most - tallies[sink]) // 2
    room = jnp.where((source_of == sequence[0]) | (sink == sequence[0]) | (tallies[sink] == 0), 0, jnp.maximum(room, 0))
    shifted = jax.random.randint(jax.random.fold_in(own, 4), (count // 2,), 0, 1 << 20) % (room + 1)
    tallies = tallies.at[source_of].add(-shifted).at[sink].add(shifted)
    labels = jnp.searchsorted(jnp.cumsum(tallies), jnp.arange(rows * top), side="right").astype(jnp.int32)
    listing = labels.reshape(top, rows).T
    listing = listing[jax.random.permutation(jax.random.fold_in(own, 1), rows)]
    offset_by = jax.random.randint(jax.random.fold_in(own, 2), (rows, 1), 0, top)
    return jnp.take_along_axis(listing, (jnp.arange(top)[None, :] + offset_by) % top, axis=1)


def load_shares(number_of, total, most, slope, full):
    loads = [(1 << 20) // math.isqrt(rank ** slope) + 1 for rank in range(1, number_of + 1)]
    largest = most if full else min(most, max(-(-total // number_of), total * loads[0] // sum(loads)))
    least = 1 if total - largest >= number_of - 1 else 0
    holding, surplus = [largest] + [least] * (number_of - 1), total - largest - least * (number_of - 1)
    while surplus > 0:
        movable = [i for i in range(1, number_of) if holding[i] < largest] or [i for i in range(1, number_of) if holding[i] < most]
        pool, remaining = sum([loads[i] for i in movable]), surplus
        for i in movable:
            more = min(most - holding[i], max(1, remaining * loads[i] // pool), surplus)
            holding[i] = holding[i] + more
            surplus = surplus - more
    return np.array(holding)


def centred(own_key, dims, scale, limit, cuts=(), kind=jnp.bfloat16):
    level = level_of(own_key, dims, cuts, -0.22, 0.18) if cuts else 1.0
    values = jax.random.normal(own_key, dims, jnp.float32) * scale * level
    return jnp.minimum(jnp.maximum(values, -limit), limit).astype(kind)


def setup_inputs(seed: int = 0) -> dict:
    key_list = jax.random.split(jax.random.key(seed), 21)
    mixer_input = draw_mixer_input(jax.random.fold_in(key_list[20], 71), 0)
    step_shift = draw_step_shift(jax.random.fold_in(key_list[20], 71), 0)
    log_step = draw_log_step(jax.random.fold_in(key_list[20], 71), 0)
    decay_real = jnp.clip(-0.7 + 0.35 * jax.random.uniform(key_list[3], (GROUPS, N_STATE), jnp.float32) ** level_of(key_list[3], (GROUPS, N_STATE), ((0, 4),), -0.2, 0.2), -0.7, -0.35)
    freq_imag = jnp.clip(201.0624 * jax.random.uniform(key_list[4], (GROUPS, N_STATE), jnp.float32) ** level_of(key_list[4], (GROUPS, N_STATE), ((0, 4),), -0.2, 0.2), 0.0, 201.0624)
    in_real = centred(key_list[5], (GROUPS, N_STATE, CH), (2 * CH) ** -0.5, 1.0, ((0, 4),), jnp.float32)
    in_imag = centred(key_list[6], (GROUPS, N_STATE, CH), (2 * CH) ** -0.5, 1.0, ((0, 4),), jnp.float32)
    out_real = centred(key_list[7], (GROUPS, CH, N_STATE), N_STATE ** -0.5, 0.75, ((0, 4),), jnp.float32)
    out_imag = centred(key_list[8], (GROUPS, CH, N_STATE), N_STATE ** -0.5, 0.75, ((0, 4),), jnp.float32)
    skip_gain = centred(key_list[9], (S5W,), 1.0, 4.0, ((0, 4),), jnp.float32)
    out_weight = centred(key_list[10], (S5W, D), S5W ** -0.5, 0.25, ((0, 4),))
    residual = centred(key_list[11], (SEQUENCE_TOKENS, D), 1.0, 6.0, ((0, 256),))
    post_gain = jnp.clip(1.0 + 0.18 * jax.random.normal(key_list[12], (D,), jnp.float32), 0.1, 1.9)
    pre_gain = jnp.clip(1.0 + 0.18 * jax.random.normal(key_list[13], (D,), jnp.float32), 0.1, 1.9)
    final_gain = jnp.clip(1.0 + 0.18 * jax.random.normal(key_list[14], (D,), jnp.float32), 0.1, 1.9)
    route_ids_keys = jax.random.split(jax.random.fold_in(key_list[15], 1), SEQUENCE_TOKENS // ROW_DEV)
    route_ids_turns = jax.random.permutation(jax.random.fold_in(key_list[15], 3), SEQUENCE_TOKENS // ROW_DEV)
    route_ids = jax.vmap(lambda own, number: deal_out(jax.random.fold_in(key_list[15], 2), own, number, ROW_DEV, EXPERTS, TOP, CAP, 2))(route_ids_keys, route_ids_turns).reshape((SEQUENCE_TOKENS, TOP))
    route_logits = centred(key_list[16], (SEQUENCE_TOKENS, TOP), 1.5, 8.0, ((0, 64),), jnp.float32)
    expert_gate = centred(key_list[17], (EXPERTS, D, EXP_W), D ** -0.5, 0.125, ((0, 64), (2, 4)))
    expert_up = centred(key_list[18], (EXPERTS, D, EXP_W), D ** -0.5, 0.125, ((0, 64), (2, 4)))
    expert_down = centred(key_list[19], (EXPERTS, EXP_W, D), EXP_W ** -0.5, 0.09375, ((0, 64), (1, 4)))
    return dict(mixer_input=mixer_input, step_shift=step_shift, log_step=log_step, decay_real=decay_real, freq_imag=freq_imag, in_real=in_real, in_imag=in_imag, out_real=out_real, out_imag=out_imag, skip_gain=skip_gain, out_weight=out_weight, residual=residual, post_gain=post_gain, pre_gain=pre_gain, final_gain=final_gain, route_ids=route_ids, route_logits=route_logits, expert_gate=expert_gate, expert_up=expert_up, expert_down=expert_down)


def combine(first_pair, second_pair):
    one_rot_real, one_rot_imag, one_state_real, one_state_imag = first_pair
    two_rot_real, two_rot_imag, two_state_real, two_state_imag = second_pair
    return (two_rot_real * one_rot_real - two_rot_imag * one_rot_imag, two_rot_real * one_rot_imag + two_rot_imag * one_rot_real, two_rot_real * one_state_real - two_rot_imag * one_state_imag + two_state_real, two_rot_real * one_state_imag + two_rot_imag * one_state_real + two_state_imag)

def scaled(values, gain_vec):
    return values * lax.rsqrt(lax.optimization_barrier(jnp.mean(values * values, axis=-1, keepdims=True)) + 1e-06) * gain_vec

def mixer_full(mixer_input, step_shift, log_step, decay_real, freq_imag, in_real, in_imag, out_real, out_imag, skip_gain):
    inputs = mixer_input.astype(jnp.float32)
    length, groups = step_shift.shape
    channels = in_real.shape[2]
    states = in_real.shape[1]
    step_size = jnp.exp(log_step[None, :] + step_shift)[:, :, None]
    magnitude = jnp.exp(decay_real[None] * step_size)
    rot_angle = freq_imag[None] * step_size
    rot_real = magnitude * jnp.cos(rot_angle)
    rot_imag = magnitude * jnp.sin(rot_angle)
    denominator = decay_real * decay_real + freq_imag * freq_imag
    minus_one = rot_real - 1.0
    coef_real = (minus_one * decay_real + rot_imag * freq_imag) / denominator
    coef_imag = (rot_imag * decay_real - minus_one * freq_imag) / denominator
    grouped = inputs.reshape(length, groups, channels)
    into_real = jnp.einsum('tgc,gnc->tgn', grouped, in_real, precision=lax.Precision.HIGHEST)
    into_imag = jnp.einsum('tgc,gnc->tgn', grouped, in_imag, precision=lax.Precision.HIGHEST)
    drive_real = coef_real * into_real - coef_imag * into_imag
    drive_imag = coef_real * into_imag + coef_imag * into_real
    flat_parts = tuple((part.reshape(length, groups * states) for part in (rot_real, rot_imag, drive_real, drive_imag)))
    scanned = lax.associative_scan(combine, flat_parts, axis=0)
    state_real = scanned[2].reshape(length, groups, states)
    state_imag = scanned[3].reshape(length, groups, states)
    readout = jnp.einsum('tgn,gcn->tgc', state_real, out_real, precision=lax.Precision.HIGHEST) - jnp.einsum('tgn,gcn->tgc', state_imag, out_imag, precision=lax.Precision.HIGHEST)
    result = readout.reshape(length, groups * channels) + skip_gain[None, :] * inputs
    return jax.nn.gelu(result).astype(jnp.bfloat16)

def reference(mixer_input, step_shift, log_step, decay_real, freq_imag, in_real, in_imag, out_real, out_imag, skip_gain, out_weight, residual, post_gain, pre_gain, final_gain, route_ids, route_logits, expert_gate, expert_up, expert_down):
    mixed_out = mixer_full(mixer_input, step_shift, log_step, decay_real, freq_imag, in_real, in_imag, out_real, out_imag, skip_gain)
    projected = jnp.dot(mixed_out, out_weight, preferred_element_type=jnp.float32)
    stream = (residual.astype(jnp.float32) + scaled(projected, post_gain)).astype(jnp.bfloat16)
    normed = scaled(stream.astype(jnp.float32), pre_gain).astype(jnp.bfloat16)
    padded = jnp.concatenate([normed, jnp.zeros((1, D), jnp.bfloat16)], axis=0)
    flat_ids = route_ids.reshape(-1)
    most_rows = SEQUENCE_TOKENS // ROW_DEV * CAP
    part_width = EXP_W // N_TP

    def one_expert(operands):
        gate_w, up_w, down_w, expert_id = operands
        chosen = jnp.nonzero(flat_ids == expert_id, size=most_rows, fill_value=2 * SEQUENCE_TOKENS)[0].astype(jnp.int32)
        token_rows = padded[chosen // 2]
        gate_hidden = jnp.dot(token_rows, gate_w, preferred_element_type=jnp.float32)
        up_hidden = jnp.dot(token_rows, up_w, preferred_element_type=jnp.float32)
        active = (jax.nn.silu(gate_hidden) * up_hidden).astype(jnp.bfloat16)
        down_total = jnp.zeros((most_rows, D), jnp.float32)
        for piece in range(N_TP):
            part_term = jnp.dot(active[:, piece * part_width:(piece + 1) * part_width], down_w[piece * part_width:(piece + 1) * part_width], preferred_element_type=jnp.float32)
            down_total = down_total + lax.optimization_barrier(part_term.astype(jnp.bfloat16)).astype(jnp.float32)
        return (down_total.astype(jnp.bfloat16), chosen)
    expert_out, chosen = lax.map(one_expert, (expert_gate, expert_up, expert_down, jnp.arange(EXPERTS, dtype=jnp.int32)))
    first_weight = jax.nn.sigmoid(route_logits[:, 0] - route_logits[:, 1])
    weights = jnp.stack([first_weight, 1.0 - first_weight], axis=1).reshape(-1)
    weights = jnp.concatenate([weights, jnp.zeros((1,), jnp.float32)])
    contrib = expert_out.astype(jnp.float32) * weights[chosen][..., None]
    mixture = jnp.zeros((SEQUENCE_TOKENS + 1, D), jnp.float32).at[(chosen // 2).reshape(-1)].add(contrib.reshape(-1, D))
    mixture = mixture[:SEQUENCE_TOKENS]
    return (stream.astype(jnp.float32) + scaled(mixture, final_gain)).astype(jnp.bfloat16)
```

```python
import jax
import jax.numpy as jnp
from jax import lax
from jax.experimental import pallas as pl
from jax.experimental.pallas import tpu as pltpu
from jax.sharding import PartitionSpec as P


F32 = jnp.float32
BF16 = jnp.bfloat16
EXACT = lax.Precision.HIGHEST
EPS = 1e-06
STEP_LIMIT = 300.0
MESSAGE = (8, 256)


def dot(first, second, over=(1, 0), precision=None):
    dims = (((over[0],), (over[1],)), ((), ()))
    return lax.dot_general(first, second, dims, precision=precision, preferred_element_type=F32)


def iota(shape, dim):
    return lax.broadcasted_iota(jnp.int32, shape, dim)


def ones_where(mask, dtype=F32):
    return jnp.where(mask, 1.0, 0.0).astype(dtype)


def sine_cosine(angle):
    quarter = jnp.floor(angle * 0.6366197723675814 + 0.5)
    rest = angle - quarter * 1.5703125
    rest = rest - quarter * 0.0004825592041015625
    rest = rest - quarter * 1.26759079e-06
    square = rest * rest
    sine = ((-1.9515295891e-4 * square + 8.3321608736e-3) * square - 1.6666654611e-1) * square
    sine = sine * rest + rest
    cosine = (2.443315711809948e-5 * square - 1.388731625493765e-3) * square
    cosine = (cosine + 4.166664568298827e-2) * square * square - 0.5 * square + 1.0
    turn = quarter.astype(jnp.int32)
    odd = (turn & 1) == 1
    first, second = (jnp.where(odd, cosine, sine), jnp.where(odd, sine, cosine))
    return (
        jnp.where((turn & 2) == 2, -first, first),
        jnp.where(((turn + 1) & 2) == 2, -second, second),
    )


def rotation(decay, freq, step):
    sine, cosine = sine_cosine(freq * step)
    magnitude = jnp.exp(decay * step)
    return (magnitude * cosine, magnitude * sine)


def delayed(values, by, fill):
    if by >= 8:
        head = jnp.full((by, values.shape[1]), fill, F32)
        return jnp.concatenate([head, values[: values.shape[0] - by]], axis=0)
    return jnp.where(iota(values.shape, 0) >= by, pltpu.roll(values, by, 0), fill)


def mixer_kernel(
    shift, inputs, log_step, decay_real, freq_imag, in_real, in_imag, out_real, out_imag, skip,
    message, rates, read_real, read_imag, cum_real, cum_imag, local_out,
):
    groups, length = shift.shape
    states = decay_real.shape[1]
    channels = in_real.shape[1]
    width = groups * states
    own = ones_where(iota((groups, width), 1) // states == iota((groups, width), 0))
    repeat = ones_where(iota((states, width), 1) % states == iota((states, width), 0))
    square = (groups, groups)
    log_column = jnp.sum(
        jnp.where(iota(square, 0) == iota(square, 1), log_step[...], 0.0), axis=1, keepdims=True
    )
    small_step = jnp.minimum(jnp.exp(log_column + shift[...]), STEP_LIMIT)
    step = dot(small_step.T, own, precision=EXACT)
    decay = jnp.sum(dot(decay_real[...], repeat, precision=EXACT) * own, axis=0, keepdims=True)
    freq = jnp.sum(dot(freq_imag[...], repeat, precision=EXACT) * own, axis=0, keepdims=True)
    rates[...] = jnp.concatenate([decay, freq, jnp.zeros((6, width), F32)], axis=0)
    wide = (groups * channels, width)
    block = ones_where(iota(wide, 0) // channels == iota(wide, 1) // states)

    def spread(ref):
        return dot(ref[...].reshape(wide[0], states), repeat, precision=EXACT) * block

    values = inputs[...].astype(F32)
    into_real = dot(values, spread(in_real), precision=EXACT)
    into_imag = dot(values, spread(in_imag), precision=EXACT)
    read_real[...] = spread(out_real)
    read_imag[...] = spread(out_imag)
    inverse = 1.0 / (decay * decay + freq * freq)
    last_real, last_imag = ([], [])
    result = skip[...] * values
    for start in range(0, width, 128):
        cut = slice(start, start + 128)
        a_real, a_imag = rotation(decay[:, cut], freq[:, cut], step[:, cut])
        minus_one = a_real - 1.0
        coef_real = (minus_one * decay[:, cut] + a_imag * freq[:, cut]) * inverse[:, cut]
        coef_imag = (a_imag * decay[:, cut] - minus_one * freq[:, cut]) * inverse[:, cut]
        s_real = coef_real * into_real[:, cut] - coef_imag * into_imag[:, cut]
        s_imag = coef_real * into_imag[:, cut] + coef_imag * into_real[:, cut]
        by = 1
        while by < length:
            p_real, p_imag = (delayed(s_real, by, 0.0), delayed(s_imag, by, 0.0))
            b_real, b_imag = (delayed(a_real, by, 1.0), delayed(a_imag, by, 0.0))
            s_real, s_imag = (
                s_real + a_real * p_real - a_imag * p_imag,
                s_imag + a_real * p_imag + a_imag * p_real,
            )
            a_real, a_imag = (a_real * b_real - a_imag * b_imag, a_real * b_imag + a_imag * b_real)
            by *= 2
        cum_real[:, cut] = a_real
        cum_imag[:, cut] = a_imag
        last_real.append(s_real[length - 1 :])
        last_imag.append(s_imag[length - 1 :])
        result = result + dot(s_real, read_real[:, cut], (1, 1), EXACT)
        result = result - dot(s_imag, read_imag[:, cut], (1, 1), EXACT)
    local_out[...] = result
    rows, lanes = MESSAGE
    pick = (width, lanes)
    compress = ones_where(
        (iota(pick, 0) == (iota(pick, 1) % groups) * states) & (iota(pick, 1) < 3 * groups)
    )
    total = dot(jnp.sum(step, axis=0, keepdims=True), compress, precision=EXACT)
    first = total.astype(BF16).astype(F32)
    second = (total - first).astype(BF16).astype(F32)
    third = total - first - second
    lane = iota(total.shape, 1)
    total = jnp.where(lane < groups, first, jnp.where(lane < 2 * groups, second, third))
    per = lanes // 128
    lines = [
        jnp.concatenate(part[k : k + per], axis=1)
        for part in (last_real, last_imag)
        for k in range(0, len(part), per)
    ]
    lines.append(total)
    lines.append(jnp.zeros((rows - len(lines), lanes), F32))
    sent = jnp.concatenate(lines, axis=0).astype(BF16)
    message[...] = jnp.broadcast_to(sent[None], message.shape)


def carry_kernel(got, rates, read_real, read_imag, cum_real, cum_imag, local_out, mixed):
    rows, lanes = MESSAGE
    devices = got.shape[0] // rows
    width = rates.shape[1]
    groups = 8
    states = width // groups
    mine = lax.axis_index("sp")
    decay, freq = (rates[0:1, :], rates[1:2, :])
    pick = (devices, devices * rows)
    everything = got[...]

    def line(k):
        return dot(ones_where(iota(pick, 1) == iota(pick, 0) * rows + k, BF16), everything)

    per = width // lanes
    got_real = jnp.concatenate([line(k) for k in range(per)], axis=1)
    got_imag = jnp.concatenate([line(per + k) for k in range(per)], axis=1)
    wide = (lanes, width)
    spread = ones_where(
        (iota(wide, 0) < 3 * groups) & (iota(wide, 0) % groups == iota(wide, 1) // states), BF16
    )
    steps = dot(line(2 * per).astype(BF16), spread)
    square = (devices, devices)
    between = ones_where((iota(square, 0) < iota(square, 1)) & (iota(square, 1) < mine))
    elapsed = jnp.minimum(dot(between, steps, precision=EXACT), STEP_LIMIT)
    weight_real, weight_imag = rotation(decay, freq, elapsed)
    earlier = iota((devices, width), 0) < mine
    weight_real = jnp.where(earlier, weight_real, 0.0)
    weight_imag = jnp.where(earlier, weight_imag, 0.0)
    carry_real = jnp.sum(weight_real * got_real - weight_imag * got_imag, axis=0, keepdims=True)
    carry_imag = jnp.sum(weight_real * got_imag + weight_imag * got_real, axis=0, keepdims=True)
    c_real, c_imag = (cum_real[...], cum_imag[...])
    result = local_out[...]
    result = result + dot(c_real * carry_real - c_imag * carry_imag, read_real[...], (1, 1), EXACT)
    result = result - dot(c_real * carry_imag + c_imag * carry_real, read_imag[...], (1, 1), EXACT)
    mixed[...] = jax.nn.gelu(result).astype(BF16)


def route_kernel(ids, logits, place, weigh):
    slots = weigh.shape[1] // 4
    tall = (slots, slots)
    rows = slots // 4
    member, lane = (iota(tall, 0) % rows, iota(tall, 1))
    here = lane == lax.axis_index("tp") * rows + member

    def column(line):
        return jnp.sum(jnp.where(here, line, 0.0), axis=1, keepdims=True)

    named = ids[...].astype(F32)
    expert = (lane // 2).astype(F32)
    is_first = ones_where(column(named[0:1]) == expert)
    is_second = ones_where(column(named[1:2]) == expert)
    before = ones_where((lane % rows < member) & (lane // rows == iota(tall, 0) // rows), BF16)
    count = dot(before, (is_first + is_second).astype(BF16))
    kept = ones_where(count == (lane % 2).astype(F32))
    first = jax.nn.sigmoid(column(logits[0:1, :]) - column(logits[1:2, :]))
    long = (slots * 4, slots)
    repeat = ones_where(iota(long, 0) // 4 == iota(long, 1), BF16)
    put = dot(repeat, ((is_first + is_second) * kept).astype(BF16), (1, 1))
    place[...] = jnp.where(iota(long, 0) % 4 == iota(long, 1) // rows, put, 0.0).astype(BF16)
    weight = (is_first * first + is_second * (1.0 - first)) * kept
    back = (slots, slots * 4)
    repeat = ones_where(iota(back, 1) // 4 == iota(back, 0))
    took = dot(weight, repeat, precision=EXACT)
    weigh[...] = jnp.where(iota(back, 1) % 4 == iota(back, 0) // rows, took, 0.0)


def normalized(values, gain):
    return values * lax.rsqrt(jnp.mean(values * values, axis=-1, keepdims=True) + EPS) * gain


def project_kernel(
    tokens, weight_0, weight_1, weight_2, weight_3, residual, post_gain, pre_gain, place,
    stream, outgoing,
):
    rows, width = residual.shape
    quarter = lax.axis_index("tp")
    projected = jnp.zeros((rows, width), F32)
    for by, weight in enumerate((weight_0, weight_1, weight_2, weight_3)):
        source = lax.rem(quarter + 4 - by, 4)
        part = tokens[pl.ds(pl.multiple_of(source * rows, rows), rows), :]
        projected = projected + dot(part, weight[...])
    own = (residual[...].astype(F32) + normalized(projected, post_gain[...])).astype(BF16)
    stream[...] = own
    normed = normalized(own.astype(F32), pre_gain[...]).astype(BF16)
    cut = width // 4
    stacked = jnp.concatenate([normed[:, q * cut : (q + 1) * cut] for q in range(4)], axis=0)
    outgoing[...] = dot(place[...], stacked).astype(BF16)


def expert_kernel(halves, weights, results, arrived=lambda which, q: None):
    gate, up, down = weights
    count = len(halves) // 2
    lines, cut = (2 * halves[0].shape[0], halves[0].shape[1])
    slots = lines // 4
    whole = [
        jnp.concatenate([halves[2 * k][...], halves[2 * k + 1][...]], axis=0) for k in range(count)
    ]
    pick = (slots, lines)
    gate_hidden = up_hidden = None
    for q in range(4):
        chosen = ones_where(iota(pick, 1) == iota(pick, 0) * 4 + q, BF16)
        part = jnp.concatenate([dot(chosen, rows).astype(BF16) for rows in whole], axis=0)
        span = slice(q * cut, (q + 1) * cut)
        arrived(0, q)
        gate_part = dot(part, gate[0, span, :])
        arrived(1, q)
        up_part = dot(part, up[0, span, :])
        gate_hidden = gate_part if q == 0 else gate_hidden + gate_part
        up_hidden = up_part if q == 0 else up_hidden + up_part
    active = (jax.nn.silu(gate_hidden) * up_hidden).astype(BF16)
    made = []
    for q in range(4):
        arrived(2, q)
        made.append(dot(active, down[0, :, q * cut : (q + 1) * cut]).astype(BF16))
    half = (lines // 2, lines)
    for k in range(count):
        stacked = jnp.concatenate([m[k * slots : (k + 1) * slots] for m in made], axis=0)
        for side in range(2):
            line = iota(half, 0) + side * (lines // 2)
            order = ones_where(iota(half, 1) == (line % 4) * slots + line // 4, BF16)
            results[2 * k + side][...] = dot(order, stacked).astype(BF16)


def own_rows_kernel(first, last, gate, up, down, made_first, made_last, *held):
    *weights, semaphores = held
    cut = first.shape[1]

    def fetch(which, q):
        source = (gate, up, down)[which]
        span = pl.ds(q * cut, cut)
        place = (0, slice(None), span) if which == 2 else (0, span, slice(None))
        return pltpu.make_async_copy(
            source.at[place], weights[which].at[place], semaphores.at[which * 4 + q]
        )

    for q in range(4):
        fetch(0, q).start()
        fetch(1, q).start()
    for q in range(4):
        fetch(2, q).start()
    expert_kernel(
        (first, last), weights, (made_first, made_last), lambda which, q: fetch(which, q).wait()
    )


def other_rows_kernel(count, *refs):
    expert_kernel(refs[:count], refs[count : count + 3], refs[count + 3 : 2 * count + 3])


def combine_kernel(results, weigh, stream, final_gain, out):
    rows = stream.shape[0]
    mixture = dot(weigh[...], results[...].astype(F32), precision=EXACT)
    mixture = jnp.concatenate([mixture[q * rows : (q + 1) * rows] for q in range(4)], axis=1)
    out[...] = (stream[...].astype(F32) + normalized(mixture, final_gain[...])).astype(BF16)


def call(kernel, outs, *args, flops=0, in_place=(), scratch=()):
    whole = pl.BlockSpec(memory_space=pltpu.VMEM)
    left = pl.BlockSpec(memory_space=pl.ANY)
    single = not isinstance(outs, list)
    shapes = [
        jax.ShapeDtypeStruct(*out) if isinstance(out, tuple) else out
        for out in ([outs] if single else outs)
    ]
    made = pl.pallas_call(
        kernel,
        out_shape=shapes,
        in_specs=[left if k in in_place else whole for k in range(len(args))],
        out_specs=[whole] * len(shapes),
        scratch_shapes=list(scratch),
        cost_estimate=pl.CostEstimate(flops=flops, bytes_accessed=0, transcendentals=0),
        compiler_params=pltpu.CompilerParams(vmem_limit_bytes=VMEM_LIMIT),
    )(*args)
    return made[0] if single else made


VMEM_LIMIT = 24 * 2**20


def in_hbm(value):
    return pltpu.with_memory_space_constraint(value, pltpu.HBM)


def across_sp(pieces):
    return lax.all_to_all(pieces, "sp", split_axis=0, concat_axis=0, tiled=True)


def shifted(part, by):
    size = lax.axis_size("tp")
    return lax.ppermute(part, "tp", [(i, (i + by) % size) for i in range(size)])


def added(first, second):
    return (first.astype(F32) + second.astype(F32)).astype(BF16)


def run_expert(weights, own):
    lines, cut = own.shape
    half = (lines // 2, cut)
    work = 2 * (lines // 4) * 3 * weights[0].shape[1] * weights[0].shape[2]
    first, last = (own[: half[0]], own[half[0] :])
    left_first, right_last = (shifted(first, 1), shifted(last, -1))
    left_last, right_first = (shifted(last, 1), shifted(first, -1))
    across_first, across_last = (shifted(left_first, 1), shifted(right_last, -1))
    own_first, own_last, *held = call(
        own_rows_kernel,
        [(half, BF16), (half, BF16), *(pltpu.VMEM(w.shape, w.dtype) for w in weights)],
        first,
        last,
        *(in_hbm(w) for w in weights),
        flops=work,
        in_place=(2, 3, 4),
        scratch=[pltpu.SemaphoreType.DMA((12,))],
    )

    def part(*halves):
        count = len(halves)
        return call(
            lambda *refs: other_rows_kernel(count, *refs), [(half, BF16)] * count,
            *halves, *held, flops=work * count // 2,
        )

    to_left_first, to_left_last, to_right_first, to_right_last = part(
        left_first, left_last, right_first, right_last
    )
    from_left_last, from_right_first = (shifted(to_right_last, 1), shifted(to_left_first, -1))
    far_first, far_last = part(across_first, across_last)
    to_right_first = added(to_right_first, shifted(far_first, 1))
    to_left_last = added(to_left_last, shifted(far_last, -1))
    from_left_first, from_right_last = (shifted(to_right_first, 1), shifted(to_left_last, -1))

    def total(*parts):
        return sum(part.astype(F32) for part in parts).astype(BF16)

    return jnp.concatenate(
        [
            total(own_first, from_left_first, from_right_first),
            total(own_last, from_left_last, from_right_last),
        ]
    )


def on_device(
    mixer_input,
    step_shift,
    log_step,
    decay_real,
    freq_imag,
    in_real,
    in_imag,
    out_real,
    out_imag,
    skip_gain,
    out_weight,
    residual,
    post_gain,
    pre_gain,
    final_gain,
    route_ids,
    route_logits,
    expert_gate,
    expert_up,
    expert_down,
):
    devices, quarters = (lax.axis_size("sp"), lax.axis_size("tp"))
    rows, width = residual.shape
    length, wide = (mixer_input.shape[0], decay_real.size)
    channels = mixer_input.shape[1]
    slots = 2 * devices
    gathered = [out_weight, *(shifted(out_weight, by) for by in range(1, quarters))]
    message, rates, read_real, read_imag, cum_real, cum_imag, local_out = call(
        mixer_kernel,
        [
            ((devices, *MESSAGE), BF16),
            ((8, wide), F32),
            ((channels, wide), F32),
            ((channels, wide), F32),
            ((length, wide), F32),
            ((length, wide), F32),
            ((length, channels), F32),
        ],
        *map(
            in_hbm,
            (
                step_shift.T,
                mixer_input,
                log_step[None],
                decay_real,
                freq_imag,
                jnp.swapaxes(in_real, 1, 2),
                jnp.swapaxes(in_imag, 1, 2),
                out_real,
                out_imag,
                skip_gain[None],
            ),
        ),
        flops=10**9,
    )
    got = across_sp(message)
    place, weigh = call(
        route_kernel,
        [((4 * slots, slots), BF16), ((slots, 4 * slots), F32)],
        route_ids.T,
        route_logits.T,
        flops=10**8,
    )
    mixed = call(
        carry_kernel, ((length, channels), BF16),
        got.reshape(-1, MESSAGE[1]), rates, read_real, read_imag, cum_real, cum_imag, local_out,
        flops=10**9,
    )
    tokens = lax.all_to_all(
        mixed.reshape(quarters, rows, channels), "tp", split_axis=0, concat_axis=0, tiled=True
    )
    stream, outgoing = call(
        project_kernel,
        [((rows, width), BF16), ((4 * slots, width // 4), BF16)],
        tokens.reshape(-1, channels),
        *gathered,
        residual,
        post_gain[None],
        pre_gain[None],
        place,
        flops=10**9,
    )
    pieces = (devices, 4 * slots // devices, width // 4)
    arrived = across_sp(outgoing.reshape(pieces))
    summed = run_expert((expert_gate, expert_up, expert_down), arrived.reshape(outgoing.shape))
    results = across_sp(summed.reshape(pieces))
    return call(
        combine_kernel, ((rows, width), BF16),
        results.reshape(outgoing.shape), weigh, stream, final_gain[None], flops=10**9,
    )


def solution(mesh):
    in_specs = (
        P("sp", "tp"),
        P("sp", "tp"),
        P("tp"),
        P("tp", None),
        P("tp", None),
        P("tp", None, None),
        P("tp", None, None),
        P("tp", None, None),
        P("tp", None, None),
        P("tp"),
        P("tp", None),
        P(("sp", "tp"), None),
        P(),
        P(),
        P(),
        P("sp", None),
        P("sp", None),
        P("sp", None, "tp"),
        P("sp", None, "tp"),
        P("sp", "tp", None),
    )
    out_specs = P(("sp", "tp"), None)

    return jax.shard_map(
        on_device, mesh=mesh, in_specs=in_specs, out_specs=out_specs, check_vma=False
    )
```

```python
import jax
import jax.numpy as jnp
from jax import lax
from jax.experimental import pallas as pl
from jax.experimental.pallas import tpu as pltpu
from jax.sharding import PartitionSpec as P


F32 = jnp.float32
BF16 = jnp.bfloat16
EPS = 1e-06
STEP_LIMIT = 300.0
MESSAGE = (8, 256)


def dot(first, second, over=(1, 0)):
    dims = (((over[0],), (over[1],)), ((), ()))
    return lax.dot_general(first, second, dims, preferred_element_type=F32)


def iota(shape, dim):
    return lax.broadcasted_iota(jnp.int32, shape, dim)


def ones_where(mask, dtype=F32):
    return jnp.where(mask, 1.0, 0.0).astype(dtype)


def sine_cosine(angle):
    quarter = jnp.floor(angle * 0.6366197723675814 + 0.5)
    rest = angle - quarter * 1.5703125
    rest = rest - quarter * 0.0004825592041015625
    rest = rest - quarter * 1.26759079e-06
    square = rest * rest
    sine = ((-1.9515295891e-4 * square + 8.3321608736e-3) * square - 1.6666654611e-1) * square
    sine = sine * rest + rest
    cosine = (2.443315711809948e-5 * square - 1.388731625493765e-3) * square
    cosine = (cosine + 4.166664568298827e-2) * square * square - 0.5 * square + 1.0
    turn = quarter.astype(jnp.int32)
    odd = (turn & 1) == 1
    first, second = (jnp.where(odd, cosine, sine), jnp.where(odd, sine, cosine))
    return (
        jnp.where((turn & 2) == 2, -first, first),
        jnp.where(((turn + 1) & 2) == 2, -second, second),
    )


def rotation(decay, freq, step):
    sine, cosine = sine_cosine(freq * step)
    magnitude = jnp.exp(decay * step)
    return (magnitude * cosine, magnitude * sine)


def delayed(values, by, fill):
    if by >= 8:
        head = jnp.full((by, values.shape[1]), fill, F32)
        return jnp.concatenate([head, values[: values.shape[0] - by]], axis=0)
    return jnp.where(iota(values.shape, 0) >= by, pltpu.roll(values, by, 0), fill)


def split(values, count):
    found = []
    for _ in range(count):
        found.append(values.astype(BF16))
        values = values - found[-1].astype(F32)
    return found


def repeated(values, width):
    pair = jnp.concatenate([values, values], axis=1)
    return jnp.concatenate([pair] * (width // pair.shape[1]), axis=1)


def read_out(state_real, state_imag, read):
    high, low = split(jnp.concatenate([state_real, state_imag], axis=1), 2)
    both = dot(jnp.concatenate([high, low], axis=0), read[...])
    rows, cut = (state_real.shape[0], both.shape[1] // 2)
    return (both[:rows, :cut] + both[:rows, cut:]) + (both[rows:, :cut] + both[rows:, cut:])


def mixer_kernel(
    shift, inputs, log_step, decay_real, freq_imag, in_real, in_imag, out_real, out_imag, skip,
    message, rates, read, cum_real, cum_imag, local_out,
):
    groups, length = shift.shape
    states = decay_real.shape[1]
    channels = in_real.shape[1]
    width = groups * states
    own = iota((groups, width), 1) // states == iota((groups, width), 0)
    square = (groups, groups)
    log_column = jnp.sum(
        jnp.where(iota(square, 0) == iota(square, 1), log_step[...], 0.0), axis=1, keepdims=True
    )
    small_step = jnp.minimum(jnp.exp(log_column + shift[...]), STEP_LIMIT)
    step = dot(jnp.concatenate(split(small_step.T, 3), axis=0), ones_where(own, BF16))
    step = (step[:length] + step[length : 2 * length]) + step[2 * length :]

    def row(ref):
        return jnp.sum(jnp.where(own, repeated(ref[...], width), 0.0), axis=0, keepdims=True)

    decay, freq = (row(decay_real), row(freq_imag))
    rates[...] = jnp.concatenate([decay, freq, jnp.zeros((6, width), F32)], axis=0)
    wide = (groups * channels, width)
    block = iota(wide, 0) // channels == iota(wide, 1) // states
    values = inputs[...]
    doubled = jnp.concatenate([values, values], axis=1)

    def driven(ref):
        spread = jnp.where(block, repeated(ref[...].reshape(wide[0], states), width), 0.0)
        return dot(doubled, jnp.concatenate(split(spread, 2), axis=0))

    into_real, into_imag = (driven(in_real), driven(in_imag))
    tall = (width, wide[0])
    block = iota(tall, 0) // states == iota(tall, 1) // channels

    def reading(ref):
        turned = ref[...].reshape(wide[0], states).T
        return jnp.where(block, jnp.concatenate([turned] * groups, axis=0), 0.0)

    read[...] = jnp.concatenate(
        split(jnp.concatenate([reading(out_real), -reading(out_imag)], axis=0), 2), axis=1
    )
    inverse = 1.0 / (decay * decay + freq * freq)
    states_real, states_imag = ([], [])
    for start in range(0, width, 128):
        cut = slice(start, start + 128)
        a_real, a_imag = rotation(decay[:, cut], freq[:, cut], step[:, cut])
        minus_one = a_real - 1.0
        coef_real = (minus_one * decay[:, cut] + a_imag * freq[:, cut]) * inverse[:, cut]
        coef_imag = (a_imag * decay[:, cut] - minus_one * freq[:, cut]) * inverse[:, cut]
        s_real = coef_real * into_real[:, cut] - coef_imag * into_imag[:, cut]
        s_imag = coef_real * into_imag[:, cut] + coef_imag * into_real[:, cut]
        by = 1
        while by < length:
            p_real, p_imag = (delayed(s_real, by, 0.0), delayed(s_imag, by, 0.0))
            b_real, b_imag = (delayed(a_real, by, 1.0), delayed(a_imag, by, 0.0))
            s_real, s_imag = (
                s_real + a_real * p_real - a_imag * p_imag,
                s_imag + a_real * p_imag + a_imag * p_real,
            )
            a_real, a_imag = (a_real * b_real - a_imag * b_imag, a_real * b_imag + a_imag * b_real)
            by *= 2
        cum_real[:, cut] = a_real
        cum_imag[:, cut] = a_imag
        states_real.append(s_real)
        states_imag.append(s_imag)
    local_out[...] = skip[...] * values.astype(F32) + read_out(
        jnp.concatenate(states_real, axis=1), jnp.concatenate(states_imag, axis=1), read
    )
    rows, lanes = MESSAGE
    pick = (width, lanes)
    compress = ones_where(
        (iota(pick, 0) == (iota(pick, 1) % groups) * states) & (iota(pick, 1) < 3 * groups), BF16
    )
    total = jnp.concatenate(split(jnp.sum(step, axis=0, keepdims=True), 3), axis=0)
    first, second, third = [part[None] for part in dot(total, compress)]
    lane = iota(first.shape, 1)
    total = jnp.where(lane < groups, first, jnp.where(lane < 2 * groups, second, third))
    per = lanes // 128
    lines = [
        jnp.concatenate([s[length - 1 :] for s in part[k : k + per]], axis=1)
        for part in (states_real, states_imag)
        for k in range(0, len(part), per)
    ]
    lines.append(total)
    lines.append(jnp.zeros((rows - len(lines), lanes), F32))
    sent = jnp.concatenate(lines, axis=0).astype(BF16)
    message[...] = jnp.broadcast_to(sent[None], message.shape)


def carry_kernel(got, rates, read, cum_real, cum_imag, local_out, mixed):
    rows, lanes = MESSAGE
    devices = got.shape[0] // rows
    width = rates.shape[1]
    groups = 8
    states = width // groups
    mine = lax.axis_index("sp")
    decay, freq = (rates[0:1, :], rates[1:2, :])
    per = width // lanes
    used = 2 * per + 1
    pick = (used * devices, devices * rows)
    line, column = (iota(pick, 0), iota(pick, 1))
    chosen = ones_where(column == (line % devices) * rows + line // devices, BF16)
    lines = dot(chosen, got[...])
    lines = [lines[k * devices : (k + 1) * devices] for k in range(used)]
    got_real = jnp.concatenate(lines[:per], axis=1)
    got_imag = jnp.concatenate(lines[per : 2 * per], axis=1)
    square = (devices, devices)
    between = (iota(square, 0) < iota(square, 1)) & (iota(square, 1) < mine)
    sums = dot(ones_where(between, BF16), lines[2 * per].astype(BF16))
    wide = (lanes, width)
    spread = ones_where(
        (iota(wide, 0) < 3 * groups) & (iota(wide, 0) % groups == iota(wide, 1) // states), BF16
    )
    elapsed = dot(jnp.concatenate(split(sums, 3), axis=0), spread)
    elapsed = (elapsed[:devices] + elapsed[devices : 2 * devices]) + elapsed[2 * devices :]
    elapsed = jnp.minimum(elapsed, STEP_LIMIT)
    weight_real, weight_imag = rotation(decay, freq, elapsed)
    earlier = iota((devices, width), 0) < mine
    weight_real = jnp.where(earlier, weight_real, 0.0)
    weight_imag = jnp.where(earlier, weight_imag, 0.0)
    carry_real = jnp.sum(weight_real * got_real - weight_imag * got_imag, axis=0, keepdims=True)
    carry_imag = jnp.sum(weight_real * got_imag + weight_imag * got_real, axis=0, keepdims=True)
    c_real, c_imag = (cum_real[...], cum_imag[...])
    result = local_out[...] + read_out(
        c_real * carry_real - c_imag * carry_imag, c_real * carry_imag + c_imag * carry_real, read
    )
    mixed[...] = jax.nn.gelu(result).astype(BF16)


def route_kernel(ids, logits, place, weigh):
    slots = ids.shape[1]
    tall = (slots, slots)
    rows = slots // 4
    member, lane = (iota(tall, 0) % rows, iota(tall, 1))
    here = lane == lax.axis_index("tp") * rows + member

    def column(line):
        return jnp.sum(jnp.where(here, line, 0.0), axis=1, keepdims=True)

    named = ids[...].astype(F32)
    expert = (lane // 2).astype(F32)
    is_first = ones_where(column(named[0:1]) == expert)
    is_second = ones_where(column(named[1:2]) == expert)
    before = ones_where((lane % rows < member) & (lane // rows == iota(tall, 0) // rows), BF16)
    count = dot(before, (is_first + is_second).astype(BF16))
    kept = ones_where(count == (lane % 2).astype(F32))
    first = jax.nn.sigmoid(column(logits[0:1, :]) - column(logits[1:2, :]))
    long = (slots * 4, slots)
    repeat = ones_where(iota(long, 0) // 4 == iota(long, 1), BF16)
    put = dot(repeat, ((is_first + is_second) * kept).astype(BF16), (1, 1))
    place[...] = jnp.where(iota(long, 0) % 4 == iota(long, 1) // rows, put, 0.0).astype(BF16)
    weight = (is_first * first + is_second * (1.0 - first)) * kept
    back = (slots, slots * 4)
    repeat = ones_where(iota(back, 1) // 4 == iota(back, 0), BF16)
    took = dot(jnp.concatenate(split(weight, 3), axis=0), repeat)
    fits = iota(took.shape, 1) % 4 == (iota(took.shape, 0) % slots) // rows
    weigh[...] = jnp.where(fits, took, 0.0).astype(BF16)


def normalized(values, gain):
    return values * lax.rsqrt(jnp.mean(values * values, axis=-1, keepdims=True) + EPS) * gain


def project_kernel(
    tokens, weight_0, weight_1, weight_2, weight_3, residual, post_gain, pre_gain, place,
    stream, outgoing,
):
    rows, width = residual.shape
    quarter = lax.axis_index("tp")
    projected = jnp.zeros((rows, width), F32)
    for by, weight in enumerate((weight_0, weight_1, weight_2, weight_3)):
        source = lax.rem(quarter + 4 - by, 4)
        part = tokens[pl.ds(pl.multiple_of(source * rows, rows), rows), :]
        projected = projected + dot(part, weight[...])
    own = (residual[...].astype(F32) + normalized(projected, post_gain[...])).astype(BF16)
    stream[...] = own
    normed = normalized(own.astype(F32), pre_gain[...]).astype(BF16)
    cut = width // 4
    stacked = jnp.concatenate([normed[:, q * cut : (q + 1) * cut] for q in range(4)], axis=0)
    outgoing[...] = dot(place[...], stacked).astype(BF16)


def expert_kernel(halves, weights, results, arrived=None):
    gate, up, down = weights
    count = len(halves) // 2
    lines, cut = (2 * halves[0].shape[0], halves[0].shape[1])
    slots = lines // 4
    square = (lines, lines)
    by_quarter = ones_where(
        iota(square, 1) == (iota(square, 0) % slots) * 4 + iota(square, 0) // slots, BF16
    )
    parts = []
    for k in range(count):
        rows = jnp.concatenate([halves[2 * k][...], halves[2 * k + 1][...]], axis=0)
        rows = dot(by_quarter, rows).astype(BF16)
        parts.append([rows[q * slots : (q + 1) * slots] for q in range(4)])
    parts = [jnp.concatenate(part, axis=0) for part in zip(*parts)]
    if arrived is None:
        whole = jnp.concatenate(parts, axis=1)
        gate_hidden, up_hidden = (dot(whole, gate[0]), dot(whole, up[0]))
    else:
        gate_hidden = up_hidden = 0.0
        for q, part in enumerate(parts):
            span = slice(q * cut, (q + 1) * cut)
            arrived(0, q)
            gate_hidden = gate_hidden + dot(part, gate[0, span, :])
            arrived(1, q)
            up_hidden = up_hidden + dot(part, up[0, span, :])
    active = (jax.nn.silu(gate_hidden) * up_hidden).astype(BF16)
    made = []
    for q in range(4):
        if arrived is not None:
            arrived(2, q)
        made.append(dot(active, down[0, :, q * cut : (q + 1) * cut]).astype(BF16))
    in_lines = ones_where(
        iota(square, 1) == (iota(square, 0) % 4) * slots + iota(square, 0) // 4, BF16
    )
    for k in range(count):
        stacked = jnp.concatenate([m[k * slots : (k + 1) * slots] for m in made], axis=0)
        product = dot(in_lines, stacked).astype(BF16)
        results[2 * k][...] = product[: lines // 2]
        results[2 * k + 1][...] = product[lines // 2 :]


def own_rows_kernel(first, last, gate, up, down, made_first, made_last, *held):
    *weights, semaphores = held
    cut = first.shape[1]

    def fetch(which, q):
        source = (gate, up, down)[which]
        span = pl.ds(q * cut, cut)
        place = (0, slice(None), span) if which == 2 else (0, span, slice(None))
        return pltpu.make_async_copy(
            source.at[place], weights[which].at[place], semaphores.at[which * 4 + q]
        )

    for q in range(4):
        fetch(0, q).start()
        fetch(1, q).start()
    for q in range(4):
        fetch(2, q).start()
    expert_kernel(
        (first, last), weights, (made_first, made_last), lambda which, q: fetch(which, q).wait()
    )


def other_rows_kernel(count, *refs):
    expert_kernel(refs[:count], refs[count : count + 3], refs[count + 3 : 2 * count + 3])


def total_kernel(*refs):
    *parts, out = refs
    half = out.shape[0] // 2
    for side in range(2):
        chosen = parts[3 * side : 3 * side + 3]
        out[side * half : (side + 1) * half, :] = sum(p[...].astype(F32) for p in chosen).astype(BF16)


def combine_kernel(results, weigh, stream, final_gain, out):
    rows = stream.shape[0]
    mixture = dot(weigh[...], results[...])
    height = mixture.shape[0] // 3
    mixture = (mixture[:height] + mixture[height : 2 * height]) + mixture[2 * height :]
    mixture = jnp.concatenate([mixture[q * rows : (q + 1) * rows] for q in range(4)], axis=1)
    out[...] = (stream[...].astype(F32) + normalized(mixture, final_gain[...])).astype(BF16)


def call(kernel, outs, *args, flops=0, in_place=(), scratch=()):
    whole = pl.BlockSpec(memory_space=pltpu.VMEM)
    left = pl.BlockSpec(memory_space=pl.ANY)
    single = not isinstance(outs, list)
    shapes = [
        jax.ShapeDtypeStruct(*out) if isinstance(out, tuple) else out
        for out in ([outs] if single else outs)
    ]
    made = pl.pallas_call(
        kernel,
        out_shape=shapes,
        in_specs=[left if k in in_place else whole for k in range(len(args))],
        out_specs=[whole] * len(shapes),
        scratch_shapes=list(scratch),
        cost_estimate=pl.CostEstimate(flops=flops, bytes_accessed=0, transcendentals=0),
        compiler_params=pltpu.CompilerParams(vmem_limit_bytes=VMEM_LIMIT),
    )(*args)
    return made[0] if single else made


VMEM_LIMIT = 24 * 2**20


def in_hbm(value):
    return pltpu.with_memory_space_constraint(value, pltpu.HBM)


def across_sp(pieces):
    return lax.all_to_all(pieces, "sp", split_axis=0, concat_axis=0, tiled=True)


def shifted(part, by):
    size = lax.axis_size("tp")
    return lax.ppermute(part, "tp", [(i, (i + by) % size) for i in range(size)])


def added(first, second):
    return (first.astype(F32) + second.astype(F32)).astype(BF16)


def run_expert(weights, own):
    lines, cut = own.shape
    half = (lines // 2, cut)
    work = 2 * (lines // 4) * 3 * weights[0].shape[1] * weights[0].shape[2]
    first, last = (own[: half[0]], own[half[0] :])
    left_first, right_last = (shifted(first, 1), shifted(last, -1))
    left_last, right_first = (shifted(last, 1), shifted(first, -1))
    across_first, across_last = (shifted(left_first, 1), shifted(right_last, -1))
    own_first, own_last, *held = call(
        own_rows_kernel,
        [(half, BF16), (half, BF16), *(pltpu.VMEM(w.shape, w.dtype) for w in weights)],
        first,
        last,
        *(in_hbm(w) for w in weights),
        flops=work,
        in_place=(2, 3, 4),
        scratch=[pltpu.SemaphoreType.DMA((12,))],
    )

    def part(*halves):
        count = len(halves)
        return call(
            lambda *refs: other_rows_kernel(count, *refs), [(half, BF16)] * count,
            *halves, *held, flops=work * count // 2,
        )

    to_left_first, to_left_last, to_right_first, to_right_last = part(
        left_first, left_last, right_first, right_last
    )
    from_left_last, from_right_first = (shifted(to_right_last, 1), shifted(to_left_first, -1))
    far_first, far_last = part(across_first, across_last)
    to_right_first = added(to_right_first, shifted(far_first, 1))
    to_left_last = added(to_left_last, shifted(far_last, -1))
    from_left_first, from_right_last = (shifted(to_right_first, 1), shifted(to_left_last, -1))

    return call(
        total_kernel, (own.shape, BF16),
        own_first, from_left_first, from_right_first,
        own_last, from_left_last, from_right_last,
        flops=10**6,
    )


def on_device(
    mixer_input,
    step_shift,
    log_step,
    decay_real,
    freq_imag,
    in_real,
    in_imag,
    out_real,
    out_imag,
    skip_gain,
    out_weight,
    residual,
    post_gain,
    pre_gain,
    final_gain,
    route_ids,
    route_logits,
    expert_gate,
    expert_up,
    expert_down,
):
    devices, quarters = (lax.axis_size("sp"), lax.axis_size("tp"))
    rows, width = residual.shape
    length, wide = (mixer_input.shape[0], decay_real.size)
    channels = mixer_input.shape[1]
    slots = 2 * devices
    gathered = [out_weight, *(shifted(out_weight, by) for by in range(1, quarters))]
    message, rates, read, cum_real, cum_imag, local_out = call(
        mixer_kernel,
        [
            ((devices, *MESSAGE), BF16),
            ((8, wide), F32),
            ((2 * wide, 2 * channels), BF16),
            ((length, wide), F32),
            ((length, wide), F32),
            ((length, channels), F32),
        ],
        *map(
            in_hbm,
            (
                step_shift.T,
                mixer_input,
                log_step[None],
                decay_real,
                freq_imag,
                jnp.swapaxes(in_real, 1, 2),
                jnp.swapaxes(in_imag, 1, 2),
                out_real,
                out_imag,
                skip_gain[None],
            ),
        ),
        flops=10**9,
    )
    got = across_sp(message)
    place, weigh = call(
        route_kernel,
        [((4 * slots, slots), BF16), ((3 * slots, 4 * slots), BF16)],
        route_ids.T,
        route_logits.T,
        flops=10**8,
    )
    mixed = call(
        carry_kernel, ((length, channels), BF16),
        got.reshape(-1, MESSAGE[1]), rates, read, cum_real, cum_imag, local_out,
        flops=10**9,
    )
    tokens = lax.all_to_all(
        mixed.reshape(quarters, rows, channels), "tp", split_axis=0, concat_axis=0, tiled=True
    )
    stream, outgoing = call(
        project_kernel,
        [((rows, width), BF16), ((4 * slots, width // 4), BF16)],
        tokens.reshape(-1, channels),
        *gathered,
        residual,
        post_gain[None],
        pre_gain[None],
        place,
        flops=10**9,
    )
    pieces = (devices, 4 * slots // devices, width // 4)
    arrived = across_sp(outgoing.reshape(pieces))
    summed = run_expert((expert_gate, expert_up, expert_down), arrived.reshape(outgoing.shape))
    results = across_sp(summed.reshape(pieces))
    return call(
        combine_kernel, ((rows, width), BF16),
        results.reshape(outgoing.shape), weigh, stream, final_gain[None], flops=10**9,
    )


def solution(mesh):
    in_specs = (
        P("sp", "tp"),
        P("sp", "tp"),
        P("tp"),
        P("tp", None),
        P("tp", None),
        P("tp", None, None),
        P("tp", None, None),
        P("tp", None, None),
        P("tp", None, None),
        P("tp"),
        P("tp", None),
        P(("sp", "tp"), None),
        P(),
        P(),
        P(),
        P("sp", None),
        P("sp", None),
        P("sp", None, "tp"),
        P("sp", None, "tp"),
        P("sp", "tp", None),
    )
    out_specs = P(("sp", "tp"), None)

    return jax.shard_map(
        on_device, mesh=mesh, in_specs=in_specs, out_specs=out_specs, check_vma=False
    )
```

```python
import jax
import jax.numpy as jnp
from jax import lax
from jax.experimental import pallas as pl
from jax.experimental.pallas import tpu as pltpu
from jax.sharding import PartitionSpec as P


F32 = jnp.float32
BF16 = jnp.bfloat16
EPS = 1e-06
STEP_LIMIT = 300.0
MESSAGE = (8, 256)


def dot(first, second, over=(1, 0)):
    dims = (((over[0],), (over[1],)), ((), ()))
    return lax.dot_general(first, second, dims, preferred_element_type=F32)


def iota(shape, dim):
    return lax.broadcasted_iota(jnp.int32, shape, dim)


def ones_where(mask, dtype=F32):
    return jnp.where(mask, 1.0, 0.0).astype(dtype)


def sine_cosine(angle):
    quarter = jnp.floor(angle * 0.6366197723675814 + 0.5)
    rest = angle - quarter * 1.5703125
    rest = rest - quarter * 0.0004825592041015625
    rest = rest - quarter * 1.26759079e-06
    square = rest * rest
    sine = ((-1.9515295891e-4 * square + 8.3321608736e-3) * square - 1.6666654611e-1) * square
    sine = sine * rest + rest
    cosine = (2.443315711809948e-5 * square - 1.388731625493765e-3) * square
    cosine = (cosine + 4.166664568298827e-2) * square * square - 0.5 * square + 1.0
    turn = quarter.astype(jnp.int32)
    odd = (turn & 1) == 1
    first, second = (jnp.where(odd, cosine, sine), jnp.where(odd, sine, cosine))
    return (
        jnp.where((turn & 2) == 2, -first, first),
        jnp.where(((turn + 1) & 2) == 2, -second, second),
    )


def rotation(decay, freq, step):
    sine, cosine = sine_cosine(freq * step)
    magnitude = jnp.exp(decay * step)
    return (magnitude * cosine, magnitude * sine)


def delayed(values, by, fill):
    if by >= 8:
        head = jnp.full((by, values.shape[1]), fill, F32)
        return jnp.concatenate([head, values[: values.shape[0] - by]], axis=0)
    return jnp.where(iota(values.shape, 0) >= by, pltpu.roll(values, by, 0), fill)


def split(values, count):
    found = []
    for _ in range(count):
        found.append(values.astype(BF16))
        values = values - found[-1].astype(F32)
    return found


def repeated(values, width):
    pair = jnp.concatenate([values, values], axis=1)
    return jnp.concatenate([pair] * (width // pair.shape[1]), axis=1)


def read_out(state_real, state_imag, read):
    high, low = split(jnp.concatenate([state_real, state_imag], axis=1), 2)
    both = dot(jnp.concatenate([high, low], axis=0), read[...])
    rows, cut = (state_real.shape[0], both.shape[1] // 2)
    return (both[:rows, :cut] + both[:rows, cut:]) + (both[rows:, :cut] + both[rows:, cut:])


def mixer_kernel(
    shift, inputs, log_step, decay_real, freq_imag, in_real, in_imag, out_real, out_imag, skip,
    message, rates, read, cum_real, cum_imag, local_out,
):
    groups, length = shift.shape
    states = decay_real.shape[1]
    channels = in_real.shape[1]
    width = groups * states
    own = iota((groups, width), 1) // states == iota((groups, width), 0)
    square = (groups, groups)
    log_column = jnp.sum(
        jnp.where(iota(square, 0) == iota(square, 1), log_step[...], 0.0), axis=1, keepdims=True
    )
    small_step = jnp.minimum(jnp.exp(log_column + shift[...]), STEP_LIMIT)
    step = dot(jnp.concatenate(split(small_step.T, 3), axis=0), ones_where(own, BF16))
    step = (step[:length] + step[length : 2 * length]) + step[2 * length :]

    def row(ref):
        return jnp.sum(jnp.where(own, repeated(ref[...], width), 0.0), axis=0, keepdims=True)

    decay, freq = (row(decay_real), row(freq_imag))
    rates[...] = jnp.concatenate([decay, freq, jnp.zeros((6, width), F32)], axis=0)
    wide = (groups * channels, width)
    block = iota(wide, 0) // channels == iota(wide, 1) // states
    values = inputs[...]
    doubled = jnp.concatenate([values, values], axis=1)

    def driven(ref):
        spread = jnp.where(block, repeated(ref[...].reshape(wide[0], states), width), 0.0)
        return dot(doubled, jnp.concatenate(split(spread, 2), axis=0))

    into_real, into_imag = (driven(in_real), driven(in_imag))
    tall = (width, wide[0])
    block = iota(tall, 0) // states == iota(tall, 1) // channels

    def reading(ref):
        turned = ref[...].reshape(wide[0], states).T
        return jnp.where(block, jnp.concatenate([turned] * groups, axis=0), 0.0)

    read[...] = jnp.concatenate(
        split(jnp.concatenate([reading(out_real), -reading(out_imag)], axis=0), 2), axis=1
    )
    inverse = 1.0 / (decay * decay + freq * freq)
    states_real, states_imag = ([], [])
    for start in range(0, width, 128):
        cut = slice(start, start + 128)
        a_real, a_imag = rotation(decay[:, cut], freq[:, cut], step[:, cut])
        minus_one = a_real - 1.0
        coef_real = (minus_one * decay[:, cut] + a_imag * freq[:, cut]) * inverse[:, cut]
        coef_imag = (a_imag * decay[:, cut] - minus_one * freq[:, cut]) * inverse[:, cut]
        s_real = coef_real * into_real[:, cut] - coef_imag * into_imag[:, cut]
        s_imag = coef_real * into_imag[:, cut] + coef_imag * into_real[:, cut]
        by = 1
        while by < length:
            p_real, p_imag = (delayed(s_real, by, 0.0), delayed(s_imag, by, 0.0))
            b_real, b_imag = (delayed(a_real, by, 1.0), delayed(a_imag, by, 0.0))
            s_real, s_imag = (
                s_real + a_real * p_real - a_imag * p_imag,
                s_imag + a_real * p_imag + a_imag * p_real,
            )
            a_real, a_imag = (a_real * b_real - a_imag * b_imag, a_real * b_imag + a_imag * b_real)
            by *= 2
        cum_real[:, cut] = a_real
        cum_imag[:, cut] = a_imag
        states_real.append(s_real)
        states_imag.append(s_imag)
    local_out[...] = skip[...] * values.astype(F32) + read_out(
        jnp.concatenate(states_real, axis=1), jnp.concatenate(states_imag, axis=1), read
    )
    rows, lanes = MESSAGE
    pick = (width, lanes)
    compress = ones_where(
        (iota(pick, 0) == (iota(pick, 1) % groups) * states) & (iota(pick, 1) < 3 * groups), BF16
    )
    total = jnp.concatenate(split(jnp.sum(step, axis=0, keepdims=True), 3), axis=0)
    first, second, third = [part[None] for part in dot(total, compress)]
    lane = iota(first.shape, 1)
    total = jnp.where(lane < groups, first, jnp.where(lane < 2 * groups, second, third))
    per = lanes // 128
    lines = [
        jnp.concatenate([s[length - 1 :] for s in part[k : k + per]], axis=1)
        for part in (states_real, states_imag)
        for k in range(0, len(part), per)
    ]
    lines.append(total)
    lines.append(jnp.zeros((rows - len(lines), lanes), F32))
    sent = jnp.concatenate(lines, axis=0).astype(BF16)
    message[...] = jnp.broadcast_to(sent[None], message.shape)


def carry_kernel(got, rates, read, cum_real, cum_imag, local_out, routed, mixed):
    del routed
    rows, lanes = MESSAGE
    devices = got.shape[0] // rows
    width = rates.shape[1]
    groups = 8
    states = width // groups
    mine = lax.axis_index("sp")
    decay, freq = (rates[0:1, :], rates[1:2, :])
    per = width // lanes
    used = 2 * per + 1
    pick = (used * devices, devices * rows)
    line, column = (iota(pick, 0), iota(pick, 1))
    chosen = ones_where(column == (line % devices) * rows + line // devices, BF16)
    lines = dot(chosen, got[...])
    lines = [lines[k * devices : (k + 1) * devices] for k in range(used)]
    got_real = jnp.concatenate(lines[:per], axis=1)
    got_imag = jnp.concatenate(lines[per : 2 * per], axis=1)
    square = (devices, devices)
    between = (iota(square, 0) < iota(square, 1)) & (iota(square, 1) < mine)
    sums = dot(ones_where(between, BF16), lines[2 * per].astype(BF16))
    wide = (lanes, width)
    spread = ones_where(
        (iota(wide, 0) < 3 * groups) & (iota(wide, 0) % groups == iota(wide, 1) // states), BF16
    )
    elapsed = dot(jnp.concatenate(split(sums, 3), axis=0), spread)
    elapsed = (elapsed[:devices] + elapsed[devices : 2 * devices]) + elapsed[2 * devices :]
    elapsed = jnp.minimum(elapsed, STEP_LIMIT)
    weight_real, weight_imag = rotation(decay, freq, elapsed)
    earlier = iota((devices, width), 0) < mine
    weight_real = jnp.where(earlier, weight_real, 0.0)
    weight_imag = jnp.where(earlier, weight_imag, 0.0)
    carry_real = jnp.sum(weight_real * got_real - weight_imag * got_imag, axis=0, keepdims=True)
    carry_imag = jnp.sum(weight_real * got_imag + weight_imag * got_real, axis=0, keepdims=True)
    c_real, c_imag = (cum_real[...], cum_imag[...])
    result = local_out[...] + read_out(
        c_real * carry_real - c_imag * carry_imag, c_real * carry_imag + c_imag * carry_real, read
    )
    mixed[...] = jax.nn.gelu(result).astype(BF16)


def route_kernel(ids, logits, place, weigh):
    slots = ids.shape[1]
    tall = (slots, slots)
    rows = slots // 4
    member, lane = (iota(tall, 0) % rows, iota(tall, 1))
    here = lane == lax.axis_index("tp") * rows + member

    def column(line):
        return jnp.sum(jnp.where(here, line, 0.0), axis=1, keepdims=True)

    named = ids[...].astype(F32)
    expert = (lane // 2).astype(F32)
    is_first = ones_where(column(named[0:1]) == expert)
    is_second = ones_where(column(named[1:2]) == expert)
    before = ones_where((lane % rows < member) & (lane // rows == iota(tall, 0) // rows), BF16)
    count = dot(before, (is_first + is_second).astype(BF16))
    kept = ones_where(count == (lane % 2).astype(F32))
    first = jax.nn.sigmoid(column(logits[0:1, :]) - column(logits[1:2, :]))
    long = (slots * 4, slots)
    repeat = ones_where(iota(long, 0) // 4 == iota(long, 1), BF16)
    put = dot(repeat, ((is_first + is_second) * kept).astype(BF16), (1, 1))
    place[...] = jnp.where(iota(long, 0) % 4 == iota(long, 1) // rows, put, 0.0).astype(BF16)
    weight = (is_first * first + is_second * (1.0 - first)) * kept
    back = (slots, slots * 4)
    repeat = ones_where(iota(back, 1) // 4 == iota(back, 0), BF16)
    took = dot(jnp.concatenate(split(weight, 3), axis=0), repeat)
    fits = iota(took.shape, 1) % 4 == (iota(took.shape, 0) % slots) // rows
    weigh[...] = jnp.where(fits, took, 0.0).astype(BF16)


def normalized(values, gain):
    return values * lax.rsqrt(jnp.mean(values * values, axis=-1, keepdims=True) + EPS) * gain


def project_kernel(tokens, weight, *refs):
    *halves, residual, post_gain, pre_gain, place, stream, outgoing = refs
    rows, width = residual.shape
    quarter = lax.axis_index("tp")
    projected = None
    for by in range(4):
        source = lax.rem(quarter + 4 - by, 4)
        part = tokens[pl.ds(pl.multiple_of(source * rows, rows), rows), :]
        if by == 0:
            projected = dot(part, weight[...])
        else:
            whole = jnp.concatenate([half[...] for half in halves[2 * by - 2 : 2 * by]], axis=0)
            projected = projected + dot(part, whole)
    own = (residual[...].astype(F32) + normalized(projected, post_gain[...])).astype(BF16)
    stream[...] = own
    normed = normalized(own.astype(F32), pre_gain[...]).astype(BF16)
    cut = width // 4
    stacked = jnp.concatenate([normed[:, q * cut : (q + 1) * cut] for q in range(4)], axis=0)
    outgoing[...] = dot(place[...], stacked).astype(BF16)


def expert_kernel(halves, weights, results, arrived=None):
    gate, up, down = weights
    count = len(halves) // 2
    lines, cut = (2 * halves[0].shape[0], halves[0].shape[1])
    slots = lines // 4
    square = (lines, lines)
    by_quarter = ones_where(
        iota(square, 1) == (iota(square, 0) % slots) * 4 + iota(square, 0) // slots, BF16
    )
    parts = []
    for k in range(count):
        rows = jnp.concatenate([halves[2 * k][...], halves[2 * k + 1][...]], axis=0)
        rows = dot(by_quarter, rows).astype(BF16)
        parts.append([rows[q * slots : (q + 1) * slots] for q in range(4)])
    parts = [jnp.concatenate(part, axis=0) for part in zip(*parts)]
    if arrived is None:
        whole = jnp.concatenate(parts, axis=1)
        gate_hidden, up_hidden = (dot(whole, gate[0]), dot(whole, up[0]))
    else:
        gate_hidden = up_hidden = 0.0
        for q, part in enumerate(parts):
            span = slice(q * cut, (q + 1) * cut)
            arrived(0, q)
            gate_hidden = gate_hidden + dot(part, gate[0, span, :])
            arrived(1, q)
            up_hidden = up_hidden + dot(part, up[0, span, :])
    active = (jax.nn.silu(gate_hidden) * up_hidden).astype(BF16)
    made = []
    for q in range(4):
        if arrived is not None:
            arrived(2, q)
        made.append(dot(active, down[0, :, q * cut : (q + 1) * cut]).astype(BF16))
    in_lines = ones_where(
        iota(square, 1) == (iota(square, 0) % 4) * slots + iota(square, 0) // 4, BF16
    )
    for k in range(count):
        stacked = jnp.concatenate([m[k * slots : (k + 1) * slots] for m in made], axis=0)
        product = dot(in_lines, stacked).astype(BF16)
        results[2 * k][...] = product[: lines // 2]
        results[2 * k + 1][...] = product[lines // 2 :]


def own_rows_kernel(first, last, gate, up, down, made_first, made_last, *held):
    *weights, semaphores = held
    cut = first.shape[1]

    def fetch(which, q):
        source = (gate, up, down)[which]
        span = pl.ds(q * cut, cut)
        place = (0, slice(None), span) if which == 2 else (0, span, slice(None))
        return pltpu.make_async_copy(
            source.at[place], weights[which].at[place], semaphores.at[which * 4 + q]
        )

    for q in range(4):
        fetch(0, q).start()
        fetch(1, q).start()
    for q in range(4):
        fetch(2, q).start()
    expert_kernel(
        (first, last), weights, (made_first, made_last), lambda which, q: fetch(which, q).wait()
    )


def other_rows_kernel(count, *refs):
    expert_kernel(refs[:count], refs[count : count + 3], refs[count + 3 : 2 * count + 3])


def total_kernel(*refs):
    *parts, out = refs
    half = out.shape[0] // 2
    for side in range(2):
        chosen = parts[3 * side : 3 * side + 3]
        out[side * half : (side + 1) * half, :] = sum(p[...].astype(F32) for p in chosen).astype(BF16)


def combine_kernel(results, weigh, stream, final_gain, out):
    rows = stream.shape[0]
    mixture = dot(weigh[...], results[...])
    height = mixture.shape[0] // 3
    mixture = (mixture[:height] + mixture[height : 2 * height]) + mixture[2 * height :]
    mixture = jnp.concatenate([mixture[q * rows : (q + 1) * rows] for q in range(4)], axis=1)
    out[...] = (stream[...].astype(F32) + normalized(mixture, final_gain[...])).astype(BF16)


def call(kernel, outs, *args, flops=0, in_place=(), scratch=()):
    whole = pl.BlockSpec(memory_space=pltpu.VMEM)
    left = pl.BlockSpec(memory_space=pl.ANY)
    single = not isinstance(outs, list)
    shapes = [
        jax.ShapeDtypeStruct(*out) if isinstance(out, tuple) else out
        for out in ([outs] if single else outs)
    ]
    made = pl.pallas_call(
        kernel,
        out_shape=shapes,
        in_specs=[left if k in in_place else whole for k in range(len(args))],
        out_specs=[whole] * len(shapes),
        scratch_shapes=list(scratch),
        cost_estimate=pl.CostEstimate(flops=flops, bytes_accessed=0, transcendentals=0),
        compiler_params=pltpu.CompilerParams(vmem_limit_bytes=VMEM_LIMIT),
    )(*args)
    return made[0] if single else made


VMEM_LIMIT = 24 * 2**20


def in_hbm(value):
    return pltpu.with_memory_space_constraint(value, pltpu.HBM)


def in_vmem(value):
    return pltpu.with_memory_space_constraint(value, pltpu.VMEM)


def across_sp(pieces):
    return lax.all_to_all(pieces, "sp", split_axis=0, concat_axis=0, tiled=True)


def shifted(part, by):
    size = lax.axis_size("tp")
    return lax.ppermute(part, "tp", [(i, (i + by) % size) for i in range(size)])


def added(first, second):
    return (first.astype(F32) + second.astype(F32)).astype(BF16)


def run_expert(weights, own):
    lines, cut = own.shape
    half = (lines // 2, cut)
    work = 2 * (lines // 4) * 3 * weights[0].shape[1] * weights[0].shape[2]
    first, last = (own[: half[0]], own[half[0] :])
    left_first, right_last = (shifted(first, 1), shifted(last, -1))
    left_last, right_first = (shifted(last, 1), shifted(first, -1))
    across_first, across_last = (shifted(left_first, 1), shifted(right_last, -1))
    own_first, own_last, *held = call(
        own_rows_kernel,
        [(half, BF16), (half, BF16), *(pltpu.VMEM(w.shape, w.dtype) for w in weights)],
        first,
        last,
        *(in_hbm(w) for w in weights),
        flops=work,
        in_place=(2, 3, 4),
        scratch=[pltpu.SemaphoreType.DMA((12,))],
    )

    def part(*halves):
        count = len(halves)
        return call(
            lambda *refs: other_rows_kernel(count, *refs), [(half, BF16)] * count,
            *halves, *held, flops=work * count // 2,
        )

    to_left_first, to_left_last, to_right_first, to_right_last = part(
        left_first, left_last, right_first, right_last
    )
    from_left_last, from_right_first = (shifted(to_right_last, 1), shifted(to_left_first, -1))
    far_first, far_last = part(across_first, across_last)
    to_right_first = added(to_right_first, shifted(far_first, 1))
    to_left_last = added(to_left_last, shifted(far_last, -1))
    from_left_first, from_right_last = (shifted(to_right_first, 1), shifted(to_left_last, -1))

    return call(
        total_kernel, (own.shape, BF16),
        own_first, from_left_first, from_right_first,
        own_last, from_left_last, from_right_last,
        flops=10**6,
    )


def on_device(
    mixer_input,
    step_shift,
    log_step,
    decay_real,
    freq_imag,
    in_real,
    in_imag,
    out_real,
    out_imag,
    skip_gain,
    out_weight,
    residual,
    post_gain,
    pre_gain,
    final_gain,
    route_ids,
    route_logits,
    expert_gate,
    expert_up,
    expert_down,
):
    devices, quarters = (lax.axis_size("sp"), lax.axis_size("tp"))
    rows, width = residual.shape
    length, wide = (mixer_input.shape[0], decay_real.size)
    channels = mixer_input.shape[1]
    slots = 2 * devices
    half = channels // 2
    first, last = (out_weight[:half], out_weight[half:])
    behind_first, ahead_last = (shifted(first, 1), shifted(last, -1))
    behind_last, ahead_first = (shifted(last, 1), shifted(first, -1))
    across_first, across_last = (shifted(behind_first, 1), shifted(ahead_last, -1))
    gathered = (
        in_hbm(out_weight),
        behind_first, behind_last, across_first, across_last, ahead_first, ahead_last,
    )
    message, rates, read, cum_real, cum_imag, local_out = call(
        mixer_kernel,
        [
            ((devices, *MESSAGE), BF16),
            ((8, wide), F32),
            ((2 * wide, 2 * channels), BF16),
            ((length, wide), F32),
            ((length, wide), F32),
            ((length, channels), F32),
        ],
        *map(
            in_hbm,
            (
                step_shift.T,
                mixer_input,
                log_step[None],
                decay_real,
                freq_imag,
                jnp.swapaxes(in_real, 1, 2),
                jnp.swapaxes(in_imag, 1, 2),
                out_real,
                out_imag,
                skip_gain[None],
            ),
        ),
        flops=10**9,
    )
    got = across_sp(message)
    place, weigh = call(
        route_kernel,
        [((4 * slots, slots), BF16), ((3 * slots, 4 * slots), BF16)],
        route_ids.T,
        route_logits.T,
        flops=10**8,
    )
    mixed = call(
        carry_kernel, ((length, channels), BF16),
        got.reshape(-1, MESSAGE[1]), *map(in_vmem, (rates, read, cum_real, cum_imag, local_out)), place,
        flops=10**9, in_place=(6,),
    )
    tokens = lax.all_to_all(
        mixed.reshape(quarters, rows, channels), "tp", split_axis=0, concat_axis=0, tiled=True
    )
    stream, outgoing = call(
        project_kernel,
        [((rows, width), BF16), ((4 * slots, width // 4), BF16)],
        tokens.reshape(-1, channels),
        *gathered,
        residual,
        post_gain[None],
        pre_gain[None],
        place,
        flops=10**9,
    )
    pieces = (devices, 4 * slots // devices, width // 4)
    arrived = across_sp(outgoing.reshape(pieces))
    summed = run_expert((expert_gate, expert_up, expert_down), arrived.reshape(outgoing.shape))
    results = across_sp(summed.reshape(pieces))
    return call(
        combine_kernel, ((rows, width), BF16),
        results.reshape(outgoing.shape), weigh, stream, final_gain[None], flops=10**9,
    )


def solution(mesh):
    in_specs = (
        P("sp", "tp"),
        P("sp", "tp"),
        P("tp"),
        P("tp", None),
        P("tp", None),
        P("tp", None, None),
        P("tp", None, None),
        P("tp", None, None),
        P("tp", None, None),
        P("tp"),
        P("tp", None),
        P(("sp", "tp"), None),
        P(),
        P(),
        P(),
        P("sp", None),
        P("sp", None),
        P("sp", None, "tp"),
        P("sp", None, "tp"),
        P("sp", "tp", None),
    )
    out_specs = P(("sp", "tp"), None)

    return jax.shard_map(
        on_device, mesh=mesh, in_specs=in_specs, out_specs=out_specs, check_vma=False
    )
```

```python
import jax
import jax.numpy as jnp
from jax import lax
from jax.experimental import pallas as pl
from jax.experimental.pallas import tpu as pltpu
from jax.sharding import PartitionSpec as P


F32 = jnp.float32
BF16 = jnp.bfloat16
EPS = 1e-06
STEP_LIMIT = 300.0
MESSAGE = (8, 256)


def dot(first, second, over=(1, 0)):
    dims = (((over[0],), (over[1],)), ((), ()))
    return lax.dot_general(first, second, dims, preferred_element_type=F32)


def iota(shape, dim):
    return lax.broadcasted_iota(jnp.int32, shape, dim)


def ones_where(mask, dtype=F32):
    return jnp.where(mask, 1.0, 0.0).astype(dtype)


def sine_cosine(angle):
    quarter = jnp.floor(angle * 0.6366197723675814 + 0.5)
    rest = angle - quarter * 1.5703125
    rest = rest - quarter * 0.0004825592041015625
    rest = rest - quarter * 1.26759079e-06
    square = rest * rest
    sine = ((-1.9515295891e-4 * square + 8.3321608736e-3) * square - 1.6666654611e-1) * square
    sine = sine * rest + rest
    cosine = (2.443315711809948e-5 * square - 1.388731625493765e-3) * square
    cosine = (cosine + 4.166664568298827e-2) * square * square - 0.5 * square + 1.0
    turn = quarter.astype(jnp.int32)
    odd = (turn & 1) == 1
    first, second = (jnp.where(odd, cosine, sine), jnp.where(odd, sine, cosine))
    return (
        jnp.where((turn & 2) == 2, -first, first),
        jnp.where(((turn + 1) & 2) == 2, -second, second),
    )


def rotation(decay, freq, step):
    sine, cosine = sine_cosine(freq * step)
    magnitude = jnp.exp(decay * step)
    return (magnitude * cosine, magnitude * sine)


def delayed(values, by, fill):
    if by >= 8:
        head = jnp.full((by, values.shape[1]), fill, F32)
        return jnp.concatenate([head, values[: values.shape[0] - by]], axis=0)
    return jnp.where(iota(values.shape, 0) >= by, pltpu.roll(values, by, 0), fill)


def split(values, count):
    found = []
    for _ in range(count):
        found.append(values.astype(BF16))
        values = values - found[-1].astype(F32)
    return found


def repeated(values, width):
    pair = jnp.concatenate([values, values], axis=1)
    return jnp.concatenate([pair] * (width // pair.shape[1]), axis=1)


def read_out(state_real, state_imag, read):
    high, low = split(jnp.concatenate([state_real, state_imag], axis=1), 2)
    both = dot(jnp.concatenate([high, low], axis=0), read[...])
    rows, cut = (state_real.shape[0], both.shape[1] // 2)
    return (both[:rows, :cut] + both[:rows, cut:]) + (both[rows:, :cut] + both[rows:, cut:])


def mixer_kernel(
    shift, inputs, log_step, decay_real, freq_imag, in_real, in_imag, out_real, out_imag, skip,
    message, rates, read, cum_real, cum_imag, local_out,
):
    groups, length = shift.shape
    states = decay_real.shape[1]
    channels = in_real.shape[1]
    width = groups * states
    own = iota((groups, width), 1) // states == iota((groups, width), 0)
    square = (groups, groups)
    log_column = jnp.sum(
        jnp.where(iota(square, 0) == iota(square, 1), log_step[...], 0.0), axis=1, keepdims=True
    )
    small_step = jnp.minimum(jnp.exp(log_column + shift[...]), STEP_LIMIT)
    step = dot(jnp.concatenate(split(small_step.T, 3), axis=0), ones_where(own, BF16))
    step = (step[:length] + step[length : 2 * length]) + step[2 * length :]

    def row(ref):
        return jnp.sum(jnp.where(own, repeated(ref[...], width), 0.0), axis=0, keepdims=True)

    decay, freq = (row(decay_real), row(freq_imag))
    rates[...] = jnp.concatenate([decay, freq, jnp.zeros((6, width), F32)], axis=0)
    wide = (groups * channels, width)
    block = iota(wide, 0) // channels == iota(wide, 1) // states
    values = inputs[...]
    doubled = jnp.concatenate([values, values], axis=1)

    def driven(ref):
        spread = jnp.where(block, repeated(ref[...].reshape(wide[0], states), width), 0.0)
        return dot(doubled, jnp.concatenate(split(spread, 2), axis=0))

    into_real, into_imag = (driven(in_real), driven(in_imag))
    tall = (width, wide[0])
    block = iota(tall, 0) // states == iota(tall, 1) // channels

    def reading(ref):
        turned = ref[...].reshape(wide[0], states).T
        return jnp.where(block, jnp.concatenate([turned] * groups, axis=0), 0.0)

    read[...] = jnp.concatenate(
        split(jnp.concatenate([reading(out_real), -reading(out_imag)], axis=0), 2), axis=1
    )
    inverse = 1.0 / (decay * decay + freq * freq)
    states_real, states_imag = ([], [])
    for start in range(0, width, 128):
        cut = slice(start, start + 128)
        a_real, a_imag = rotation(decay[:, cut], freq[:, cut], step[:, cut])
        minus_one = a_real - 1.0
        coef_real = (minus_one * decay[:, cut] + a_imag * freq[:, cut]) * inverse[:, cut]
        coef_imag = (a_imag * decay[:, cut] - minus_one * freq[:, cut]) * inverse[:, cut]
        s_real = coef_real * into_real[:, cut] - coef_imag * into_imag[:, cut]
        s_imag = coef_real * into_imag[:, cut] + coef_imag * into_real[:, cut]
        by = 1
        while by < length:
            p_real, p_imag = (delayed(s_real, by, 0.0), delayed(s_imag, by, 0.0))
            b_real, b_imag = (delayed(a_real, by, 1.0), delayed(a_imag, by, 0.0))
            s_real, s_imag = (
                s_real + a_real * p_real - a_imag * p_imag,
                s_imag + a_real * p_imag + a_imag * p_real,
            )
            a_real, a_imag = (a_real * b_real - a_imag * b_imag, a_real * b_imag + a_imag * b_real)
            by *= 2
        cum_real[:, cut] = a_real
        cum_imag[:, cut] = a_imag
        states_real.append(s_real)
        states_imag.append(s_imag)
    local_out[...] = skip[...] * values.astype(F32) + read_out(
        jnp.concatenate(states_real, axis=1), jnp.concatenate(states_imag, axis=1), read
    )
    rows, lanes = MESSAGE
    pick = (width, lanes)
    compress = ones_where(
        (iota(pick, 0) == (iota(pick, 1) % groups) * states) & (iota(pick, 1) < 3 * groups), BF16
    )
    total = jnp.concatenate(split(jnp.sum(step, axis=0, keepdims=True), 3), axis=0)
    first, second, third = [part[None] for part in dot(total, compress)]
    lane = iota(first.shape, 1)
    total = jnp.where(lane < groups, first, jnp.where(lane < 2 * groups, second, third))
    per = lanes // 128
    lines = [
        jnp.concatenate([s[length - 1 :] for s in part[k : k + per]], axis=1)
        for part in (states_real, states_imag)
        for k in range(0, len(part), per)
    ]
    lines.append(total)
    lines.append(jnp.zeros((rows - len(lines), lanes), F32))
    sent = jnp.concatenate(lines, axis=0).astype(BF16)
    message[...] = jnp.broadcast_to(sent[None], message.shape)


def carry_kernel(
    got, rates, read, cum_real, cum_imag, local_out, ids, logits, mixed, place, weigh
):
    routing(ids, logits, place, weigh)
    rows, lanes = MESSAGE
    devices = got.shape[0] // rows
    width = rates.shape[1]
    groups = 8
    states = width // groups
    mine = lax.axis_index("sp")
    decay, freq = (rates[0:1, :], rates[1:2, :])
    per = width // lanes
    used = 2 * per + 1
    pick = (used * devices, devices * rows)
    line, column = (iota(pick, 0), iota(pick, 1))
    chosen = ones_where(column == (line % devices) * rows + line // devices, BF16)
    lines = dot(chosen, got[...])
    lines = [lines[k * devices : (k + 1) * devices] for k in range(used)]
    got_real = jnp.concatenate(lines[:per], axis=1)
    got_imag = jnp.concatenate(lines[per : 2 * per], axis=1)
    square = (devices, devices)
    between = (iota(square, 0) < iota(square, 1)) & (iota(square, 1) < mine)
    sums = dot(ones_where(between, BF16), lines[2 * per].astype(BF16))
    wide = (lanes, width)
    spread = ones_where(
        (iota(wide, 0) < 3 * groups) & (iota(wide, 0) % groups == iota(wide, 1) // states), BF16
    )
    elapsed = dot(jnp.concatenate(split(sums, 3), axis=0), spread)
    elapsed = (elapsed[:devices] + elapsed[devices : 2 * devices]) + elapsed[2 * devices :]
    elapsed = jnp.minimum(elapsed, STEP_LIMIT)
    weight_real, weight_imag = rotation(decay, freq, elapsed)
    earlier = iota((devices, width), 0) < mine
    weight_real = jnp.where(earlier, weight_real, 0.0)
    weight_imag = jnp.where(earlier, weight_imag, 0.0)
    carry_real = jnp.sum(weight_real * got_real - weight_imag * got_imag, axis=0, keepdims=True)
    carry_imag = jnp.sum(weight_real * got_imag + weight_imag * got_real, axis=0, keepdims=True)
    c_real, c_imag = (cum_real[...], cum_imag[...])
    result = local_out[...] + read_out(
        c_real * carry_real - c_imag * carry_imag, c_real * carry_imag + c_imag * carry_real, read
    )
    mixed[...] = jax.nn.gelu(result).astype(BF16)


def routing(ids, logits, place, weigh):
    slots = ids.shape[1]
    tall = (slots, slots)
    rows = slots // 4
    member, lane = (iota(tall, 0) % rows, iota(tall, 1))
    here = lane == lax.axis_index("tp") * rows + member

    def column(line):
        return jnp.sum(jnp.where(here, line, 0.0), axis=1, keepdims=True)

    named = ids[...].astype(F32)
    expert = (lane // 2).astype(F32)
    is_first = ones_where(column(named[0:1]) == expert)
    is_second = ones_where(column(named[1:2]) == expert)
    before = ones_where((lane % rows < member) & (lane // rows == iota(tall, 0) // rows), BF16)
    count = dot(before, (is_first + is_second).astype(BF16))
    kept = ones_where(count == (lane % 2).astype(F32))
    first = jax.nn.sigmoid(column(logits[0:1, :]) - column(logits[1:2, :]))
    long = (slots * 4, slots)
    repeat = ones_where(iota(long, 0) // 4 == iota(long, 1), BF16)
    put = dot(repeat, ((is_first + is_second) * kept).astype(BF16), (1, 1))
    place[...] = jnp.where(iota(long, 0) % 4 == iota(long, 1) // rows, put, 0.0).astype(BF16)
    weight = (is_first * first + is_second * (1.0 - first)) * kept
    back = (slots, slots * 4)
    repeat = ones_where(iota(back, 1) // 4 == iota(back, 0), BF16)
    took = dot(jnp.concatenate(split(weight, 3), axis=0), repeat)
    fits = iota(took.shape, 1) % 4 == (iota(took.shape, 0) % slots) // rows
    weigh[...] = jnp.where(fits, took, 0.0).astype(BF16)


def normalized(values, gain):
    return values * lax.rsqrt(jnp.mean(values * values, axis=-1, keepdims=True) + EPS) * gain


def project_kernel(
    tokens, weight_0, weight_1, weight_2, weight_3, residual, post_gain, pre_gain, place,
    stream, outgoing,
):
    rows, width = residual.shape
    quarter = lax.axis_index("tp")
    projected = jnp.zeros((rows, width), F32)
    for by, weight in enumerate((weight_0, weight_1, weight_2, weight_3)):
        source = lax.rem(quarter + 4 - by, 4)
        part = tokens[pl.ds(pl.multiple_of(source * rows, rows), rows), :]
        projected = projected + dot(part, weight[...])
    own = (residual[...].astype(F32) + normalized(projected, post_gain[...])).astype(BF16)
    stream[...] = own
    normed = normalized(own.astype(F32), pre_gain[...]).astype(BF16)
    cut = width // 4
    stacked = jnp.concatenate([normed[:, q * cut : (q + 1) * cut] for q in range(4)], axis=0)
    outgoing[...] = dot(place[...], stacked).astype(BF16)


def expert_kernel(halves, weights, results, arrived=None):
    gate, up, down = weights
    count = len(halves) // 2
    lines, cut = (2 * halves[0].shape[0], halves[0].shape[1])
    slots = lines // 4
    square = (lines, lines)
    by_quarter = ones_where(
        iota(square, 1) == (iota(square, 0) % slots) * 4 + iota(square, 0) // slots, BF16
    )
    parts = []
    for k in range(count):
        rows = jnp.concatenate([halves[2 * k][...], halves[2 * k + 1][...]], axis=0)
        rows = dot(by_quarter, rows).astype(BF16)
        parts.append([rows[q * slots : (q + 1) * slots] for q in range(4)])
    parts = [jnp.concatenate(part, axis=0) for part in zip(*parts)]
    if arrived is None:
        whole = jnp.concatenate(parts, axis=1)
        gate_hidden, up_hidden = (dot(whole, gate[0]), dot(whole, up[0]))
    else:
        gate_hidden = up_hidden = 0.0
        for q, part in enumerate(parts):
            span = slice(q * cut, (q + 1) * cut)
            arrived(0, q)
            gate_hidden = gate_hidden + dot(part, gate[0, span, :])
            arrived(1, q)
            up_hidden = up_hidden + dot(part, up[0, span, :])
    active = (jax.nn.silu(gate_hidden) * up_hidden).astype(BF16)
    made = []
    for q in range(4):
        if arrived is not None:
            arrived(2, q)
        made.append(dot(active, down[0, :, q * cut : (q + 1) * cut]).astype(BF16))
    in_lines = ones_where(
        iota(square, 1) == (iota(square, 0) % 4) * slots + iota(square, 0) // 4, BF16
    )
    for k in range(count):
        stacked = jnp.concatenate([m[k * slots : (k + 1) * slots] for m in made], axis=0)
        product = dot(in_lines, stacked).astype(BF16)
        results[2 * k][...] = product[: lines // 2]
        results[2 * k + 1][...] = product[lines // 2 :]


def own_rows_kernel(first, last, gate, up, down, made_first, made_last, *held):
    *weights, semaphores = held
    cut = first.shape[1]

    def fetch(which, q):
        source = (gate, up, down)[which]
        span = pl.ds(q * cut, cut)
        place = (0, slice(None), span) if which == 2 else (0, span, slice(None))
        return pltpu.make_async_copy(
            source.at[place], weights[which].at[place], semaphores.at[which * 4 + q]
        )

    for q in range(4):
        fetch(0, q).start()
        fetch(1, q).start()
    for q in range(4):
        fetch(2, q).start()
    expert_kernel(
        (first, last), weights, (made_first, made_last), lambda which, q: fetch(which, q).wait()
    )


def other_rows_kernel(count, *refs):
    expert_kernel(refs[:count], refs[count : count + 3], refs[count + 3 : 2 * count + 3])


def total_kernel(*refs):
    *parts, out = refs
    half = out.shape[0] // 2
    for side in range(2):
        chosen = parts[3 * side : 3 * side + 3]
        out[side * half : (side + 1) * half, :] = sum(p[...].astype(F32) for p in chosen).astype(BF16)


def combine_kernel(results, weigh, stream, final_gain, out):
    rows = stream.shape[0]
    mixture = dot(weigh[...], results[...])
    height = mixture.shape[0] // 3
    mixture = (mixture[:height] + mixture[height : 2 * height]) + mixture[2 * height :]
    mixture = jnp.concatenate([mixture[q * rows : (q + 1) * rows] for q in range(4)], axis=1)
    out[...] = (stream[...].astype(F32) + normalized(mixture, final_gain[...])).astype(BF16)


def call(kernel, outs, *args, flops=0, in_place=(), scratch=()):
    whole = pl.BlockSpec(memory_space=pltpu.VMEM)
    left = pl.BlockSpec(memory_space=pl.ANY)
    single = not isinstance(outs, list)
    shapes = [
        jax.ShapeDtypeStruct(*out) if isinstance(out, tuple) else out
        for out in ([outs] if single else outs)
    ]
    made = pl.pallas_call(
        kernel,
        out_shape=shapes,
        in_specs=[left if k in in_place else whole for k in range(len(args))],
        out_specs=[whole] * len(shapes),
        scratch_shapes=list(scratch),
        cost_estimate=pl.CostEstimate(flops=flops, bytes_accessed=0, transcendentals=0),
        compiler_params=pltpu.CompilerParams(vmem_limit_bytes=VMEM_LIMIT),
    )(*args)
    return made[0] if single else made


VMEM_LIMIT = 24 * 2**20


def in_hbm(value):
    return pltpu.with_memory_space_constraint(value, pltpu.HBM)


def across_sp(pieces):
    return lax.all_to_all(pieces, "sp", split_axis=0, concat_axis=0, tiled=True)


def shifted(part, by):
    size = lax.axis_size("tp")
    return lax.ppermute(part, "tp", [(i, (i + by) % size) for i in range(size)])


def added(first, second):
    return (first.astype(F32) + second.astype(F32)).astype(BF16)


def run_expert(weights, own):
    lines, cut = own.shape
    half = (lines // 2, cut)
    work = 2 * (lines // 4) * 3 * weights[0].shape[1] * weights[0].shape[2]
    first, last = (own[: half[0]], own[half[0] :])
    left_first, right_last = (shifted(first, 1), shifted(last, -1))
    left_last, right_first = (shifted(last, 1), shifted(first, -1))
    across_first, across_last = (shifted(left_first, 1), shifted(right_last, -1))
    own_first, own_last, *held = call(
        own_rows_kernel,
        [(half, BF16), (half, BF16), *(pltpu.VMEM(w.shape, w.dtype) for w in weights)],
        first,
        last,
        *(in_hbm(w) for w in weights),
        flops=work,
        in_place=(2, 3, 4),
        scratch=[pltpu.SemaphoreType.DMA((12,))],
    )

    def part(*halves):
        count = len(halves)
        return call(
            lambda *refs: other_rows_kernel(count, *refs), [(half, BF16)] * count,
            *halves, *held, flops=work * count // 2,
        )

    to_left_first, to_right_last = part(left_first, right_last)
    from_left_last, from_right_first = (shifted(to_right_last, 1), shifted(to_left_first, -1))
    to_left_last, to_right_first = part(left_last, right_first)
    far_first, far_last = part(across_first, across_last)
    to_right_first = added(to_right_first, shifted(far_first, 1))
    to_left_last = added(to_left_last, shifted(far_last, -1))
    from_left_first, from_right_last = (shifted(to_right_first, 1), shifted(to_left_last, -1))

    return call(
        total_kernel, (own.shape, BF16),
        own_first, from_left_first, from_right_first,
        own_last, from_left_last, from_right_last,
        flops=10**6,
    )


def on_device(
    mixer_input,
    step_shift,
    log_step,
    decay_real,
    freq_imag,
    in_real,
    in_imag,
    out_real,
    out_imag,
    skip_gain,
    out_weight,
    residual,
    post_gain,
    pre_gain,
    final_gain,
    route_ids,
    route_logits,
    expert_gate,
    expert_up,
    expert_down,
):
    devices, quarters = (lax.axis_size("sp"), lax.axis_size("tp"))
    rows, width = residual.shape
    length, wide = (mixer_input.shape[0], decay_real.size)
    channels = mixer_input.shape[1]
    slots = 2 * devices
    gathered = [out_weight, *(shifted(out_weight, by) for by in range(1, quarters))]
    message, rates, read, cum_real, cum_imag, local_out = call(
        mixer_kernel,
        [
            ((devices, *MESSAGE), BF16),
            ((8, wide), F32),
            ((2 * wide, 2 * channels), BF16),
            ((length, wide), F32),
            ((length, wide), F32),
            ((length, channels), F32),
        ],
        *map(
            in_hbm,
            (
                step_shift.T,
                mixer_input,
                log_step[None],
                decay_real,
                freq_imag,
                jnp.swapaxes(in_real, 1, 2),
                jnp.swapaxes(in_imag, 1, 2),
                out_real,
                out_imag,
                skip_gain[None],
            ),
        ),
        flops=10**9,
    )
    got = across_sp(message)
    mixed, place, weigh = call(
        carry_kernel,
        [
            ((length, channels), BF16),
            ((4 * slots, slots), BF16),
            ((3 * slots, 4 * slots), BF16),
        ],
        got.reshape(-1, MESSAGE[1]), rates, read, cum_real, cum_imag, local_out,
        route_ids.T,
        route_logits.T,
        flops=10**9,
    )
    tokens = lax.all_to_all(
        mixed.reshape(quarters, rows, channels), "tp", split_axis=0, concat_axis=0, tiled=True
    )
    stream, outgoing = call(
        project_kernel,
        [((rows, width), BF16), ((4 * slots, width // 4), BF16)],
        tokens.reshape(-1, channels),
        *gathered,
        residual,
        post_gain[None],
        pre_gain[None],
        place,
        flops=10**9,
    )
    pieces = (devices, 4 * slots // devices, width // 4)
    arrived = across_sp(outgoing.reshape(pieces))
    summed = run_expert((expert_gate, expert_up, expert_down), arrived.reshape(outgoing.shape))
    results = across_sp(summed.reshape(pieces))
    return call(
        combine_kernel, ((rows, width), BF16),
        results.reshape(outgoing.shape), weigh, stream, final_gain[None], flops=10**9,
    )


def solution(mesh):
    in_specs = (
        P("sp", "tp"),
        P("sp", "tp"),
        P("tp"),
        P("tp", None),
        P("tp", None),
        P("tp", None, None),
        P("tp", None, None),
        P("tp", None, None),
        P("tp", None, None),
        P("tp"),
        P("tp", None),
        P(("sp", "tp"), None),
        P(),
        P(),
        P(),
        P("sp", None),
        P("sp", None),
        P("sp", None, "tp"),
        P("sp", None, "tp"),
        P("sp", "tp", None),
    )
    out_specs = P(("sp", "tp"), None)

    return jax.shard_map(
        on_device, mesh=mesh, in_specs=in_specs, out_specs=out_specs, check_vma=False
    )
```

```python
import jax
import jax.numpy as jnp
from jax import lax
from jax.experimental import pallas as pl
from jax.experimental.pallas import tpu as pltpu
from jax.sharding import PartitionSpec as P


F32 = jnp.float32
BF16 = jnp.bfloat16
EPS = 1e-06
STEP_LIMIT = 300.0
MESSAGE = (2, 640)


def dot(first, second, over=(1, 0)):
    dims = (((over[0],), (over[1],)), ((), ()))
    return lax.dot_general(first, second, dims, preferred_element_type=F32)


def iota(shape, dim):
    return lax.broadcasted_iota(jnp.int32, shape, dim)


def ones_where(mask, dtype=F32):
    return jnp.where(mask, 1.0, 0.0).astype(dtype)


def sine_cosine(angle):
    quarter = jnp.floor(angle * 0.6366197723675814 + 0.5)
    rest = angle - quarter * 1.5703125
    rest = rest - quarter * 0.0004825592041015625
    rest = rest - quarter * 1.26759079e-06
    square = rest * rest
    sine = ((-1.9515295891e-4 * square + 8.3321608736e-3) * square - 1.6666654611e-1) * square
    sine = sine * rest + rest
    cosine = (2.443315711809948e-5 * square - 1.388731625493765e-3) * square
    cosine = (cosine + 4.166664568298827e-2) * square * square - 0.5 * square + 1.0
    turn = quarter.astype(jnp.int32)
    odd = (turn & 1) == 1
    first, second = (jnp.where(odd, cosine, sine), jnp.where(odd, sine, cosine))
    return (
        jnp.where((turn & 2) == 2, -first, first),
        jnp.where(((turn + 1) & 2) == 2, -second, second),
    )


def rotation(decay, freq, step):
    sine, cosine = sine_cosine(freq * step)
    magnitude = jnp.exp(decay * step)
    return (magnitude * cosine, magnitude * sine)


def delayed(values, by, fill):
    if by >= 8:
        head = jnp.full((by, values.shape[1]), fill, F32)
        return jnp.concatenate([head, values[: values.shape[0] - by]], axis=0)
    return jnp.where(iota(values.shape, 0) >= by, pltpu.roll(values, by, 0), fill)


def split(values, count):
    found = []
    for _ in range(count):
        found.append(values.astype(BF16))
        values = values - found[-1].astype(F32)
    return found


def repeated(values, width):
    pair = jnp.concatenate([values, values], axis=1)
    return jnp.concatenate([pair] * (width // pair.shape[1]), axis=1)


def read_out(state_real, state_imag, read):
    high, low = split(jnp.concatenate([state_real, state_imag], axis=1), 2)
    both = dot(jnp.concatenate([high, low], axis=0), read[...])
    rows, cut = (state_real.shape[0], both.shape[1] // 2)
    return (both[:rows, :cut] + both[:rows, cut:]) + (both[rows:, :cut] + both[rows:, cut:])


def mixer_kernel(
    shift, inputs, log_step, decay_real, freq_imag, in_real, in_imag, out_real, out_imag, skip,
    message, rates, read, cum_real, cum_imag, local_out,
):
    groups, length = shift.shape
    states = decay_real.shape[1]
    channels = in_real.shape[1]
    width = groups * states
    own = iota((groups, width), 1) // states == iota((groups, width), 0)
    square = (groups, groups)
    log_column = jnp.sum(
        jnp.where(iota(square, 0) == iota(square, 1), log_step[...], 0.0), axis=1, keepdims=True
    )
    small_step = jnp.minimum(jnp.exp(log_column + shift[...]), STEP_LIMIT)
    step = dot(jnp.concatenate(split(small_step.T, 3), axis=0), ones_where(own, BF16))
    step = (step[:length] + step[length : 2 * length]) + step[2 * length :]

    def row(ref):
        return jnp.sum(jnp.where(own, repeated(ref[...], width), 0.0), axis=0, keepdims=True)

    decay, freq = (row(decay_real), row(freq_imag))
    rates[...] = jnp.concatenate([decay, freq, jnp.zeros((6, width), F32)], axis=0)
    wide = (groups * channels, width)
    block = iota(wide, 0) // channels == iota(wide, 1) // states
    values = inputs[...]
    doubled = jnp.concatenate([values, values], axis=1)

    def driven(ref):
        spread = jnp.where(block, repeated(ref[...].reshape(wide[0], states), width), 0.0)
        return dot(doubled, jnp.concatenate(split(spread, 2), axis=0))

    into_real, into_imag = (driven(in_real), driven(in_imag))
    tall = (width, wide[0])
    block = iota(tall, 0) // states == iota(tall, 1) // channels

    def reading(ref):
        turned = ref[...].reshape(wide[0], states).T
        return jnp.where(block, jnp.concatenate([turned] * groups, axis=0), 0.0)

    read[...] = jnp.concatenate(
        split(jnp.concatenate([reading(out_real), -reading(out_imag)], axis=0), 2), axis=1
    )
    inverse = 1.0 / (decay * decay + freq * freq)
    states_real, states_imag = ([], [])
    for start in range(0, width, 128):
        cut = slice(start, start + 128)
        a_real, a_imag = rotation(decay[:, cut], freq[:, cut], step[:, cut])
        minus_one = a_real - 1.0
        coef_real = (minus_one * decay[:, cut] + a_imag * freq[:, cut]) * inverse[:, cut]
        coef_imag = (a_imag * decay[:, cut] - minus_one * freq[:, cut]) * inverse[:, cut]
        s_real = coef_real * into_real[:, cut] - coef_imag * into_imag[:, cut]
        s_imag = coef_real * into_imag[:, cut] + coef_imag * into_real[:, cut]
        by = 1
        while by < length:
            p_real, p_imag = (delayed(s_real, by, 0.0), delayed(s_imag, by, 0.0))
            b_real, b_imag = (delayed(a_real, by, 1.0), delayed(a_imag, by, 0.0))
            s_real, s_imag = (
                s_real + a_real * p_real - a_imag * p_imag,
                s_imag + a_real * p_imag + a_imag * p_real,
            )
            a_real, a_imag = (a_real * b_real - a_imag * b_imag, a_real * b_imag + a_imag * b_real)
            by *= 2
        cum_real[:, cut] = a_real
        cum_imag[:, cut] = a_imag
        states_real.append(s_real)
        states_imag.append(s_imag)
    local_out[...] = skip[...] * values.astype(F32) + read_out(
        jnp.concatenate(states_real, axis=1), jnp.concatenate(states_imag, axis=1), read
    )
    lanes = MESSAGE[1] - width
    pick = (width, lanes)
    compress = ones_where(
        (iota(pick, 0) == (iota(pick, 1) % groups) * states) & (iota(pick, 1) < 3 * groups), BF16
    )
    total = jnp.concatenate(split(jnp.sum(step, axis=0, keepdims=True), 3), axis=0)
    first, second, third = [part[None] for part in dot(total, compress)]
    lane = iota(first.shape, 1)
    total = jnp.where(lane < groups, first, jnp.where(lane < 2 * groups, second, third))
    lines = [
        jnp.concatenate([s[length - 1 :] for s in part] + [last], axis=1)
        for part, last in ((states_real, total), (states_imag, jnp.zeros_like(total)))
    ]
    sent = jnp.concatenate(lines, axis=0)
    message[...] = jnp.broadcast_to(sent[None], message.shape).astype(BF16)


def carry_kernel(
    got, rates, read, cum_real, cum_imag, local_out, out_weight, ids, logits,
    partial, place, weigh,
):
    routing(ids, logits, place, weigh)
    devices = got.shape[0]
    width = rates.shape[1]
    lanes = MESSAGE[1] - width
    groups = 8
    states = width // groups
    mine = lax.axis_index("sp")
    decay, freq = (rates[0:1, :], rates[1:2, :])
    everything = got[...].astype(F32)
    got_real, got_imag = (everything[:, 0, :width], everything[:, 1, :width])
    totals = everything[:, 0, width:]
    square = (devices, devices)
    between = (iota(square, 0) < iota(square, 1)) & (iota(square, 1) < mine)
    sums = dot(ones_where(between, BF16), totals.astype(BF16))
    wide = (lanes, width)
    spread = ones_where(
        (iota(wide, 0) < 3 * groups) & (iota(wide, 0) % groups == iota(wide, 1) // states), BF16
    )
    elapsed = dot(jnp.concatenate(split(sums, 3), axis=0), spread)
    elapsed = (elapsed[:devices] + elapsed[devices : 2 * devices]) + elapsed[2 * devices :]
    elapsed = jnp.minimum(elapsed, STEP_LIMIT)
    weight_real, weight_imag = rotation(decay, freq, elapsed)
    earlier = iota((devices, width), 0) < mine
    weight_real = jnp.where(earlier, weight_real, 0.0)
    weight_imag = jnp.where(earlier, weight_imag, 0.0)
    carry_real = jnp.sum(weight_real * got_real - weight_imag * got_imag, axis=0, keepdims=True)
    carry_imag = jnp.sum(weight_real * got_imag + weight_imag * got_real, axis=0, keepdims=True)
    c_real, c_imag = (cum_real[...], cum_imag[...])
    result = local_out[...] + read_out(
        c_real * carry_real - c_imag * carry_imag, c_real * carry_imag + c_imag * carry_real, read
    )
    mixed = jax.nn.gelu(result).astype(BF16)
    partial[...] = dot(mixed, out_weight[...]).astype(BF16)


def routing(ids, logits, place, weigh):
    slots = ids.shape[1]
    tall = (slots, slots)
    rows = slots // 4
    member, lane = (iota(tall, 0) % rows, iota(tall, 1))
    here = lane == lax.axis_index("tp") * rows + member

    def column(line):
        return jnp.sum(jnp.where(here, line, 0.0), axis=1, keepdims=True)

    named = ids[...].astype(F32)
    expert = (lane // 2).astype(F32)
    is_first = ones_where(column(named[0:1]) == expert)
    is_second = ones_where(column(named[1:2]) == expert)
    before = ones_where((lane % rows < member) & (lane // rows == iota(tall, 0) // rows), BF16)
    count = dot(before, (is_first + is_second).astype(BF16))
    kept = ones_where(count == (lane % 2).astype(F32))
    first = jax.nn.sigmoid(column(logits[0:1, :]) - column(logits[1:2, :]))
    long = (slots * 4, slots)
    repeat = ones_where(iota(long, 0) // 4 == iota(long, 1), BF16)
    put = dot(repeat, ((is_first + is_second) * kept).astype(BF16), (1, 1))
    place[...] = jnp.where(iota(long, 0) % 4 == iota(long, 1) // rows, put, 0.0).astype(BF16)
    weight = (is_first * first + is_second * (1.0 - first)) * kept
    back = (slots, slots * 4)
    repeat = ones_where(iota(back, 1) // 4 == iota(back, 0), BF16)
    took = dot(jnp.concatenate(split(weight, 3), axis=0), repeat)
    fits = iota(took.shape, 1) % 4 == (iota(took.shape, 0) % slots) // rows
    weigh[...] = jnp.where(fits, took, 0.0).astype(BF16)


def normalized(values, gain):
    return values * lax.rsqrt(jnp.mean(values * values, axis=-1, keepdims=True) + EPS) * gain


def project_kernel(parts, residual, post_gain, pre_gain, place, stream, outgoing):
    rows, width = residual.shape
    projected = sum(parts[k * rows : (k + 1) * rows, :].astype(F32) for k in range(4))
    own = (residual[...].astype(F32) + normalized(projected, post_gain[...])).astype(BF16)
    stream[...] = own
    normed = normalized(own.astype(F32), pre_gain[...]).astype(BF16)
    cut = width // 4
    stacked = jnp.concatenate([normed[:, q * cut : (q + 1) * cut] for q in range(4)], axis=0)
    outgoing[...] = dot(place[...], stacked).astype(BF16)


def expert_kernel(halves, weights, results, arrived=None):
    gate, up, down = weights
    count = len(halves) // 2
    lines, cut = (2 * halves[0].shape[0], halves[0].shape[1])
    slots = lines // 4
    square = (lines, lines)
    by_quarter = ones_where(
        iota(square, 1) == (iota(square, 0) % slots) * 4 + iota(square, 0) // slots, BF16
    )
    parts = []
    for k in range(count):
        rows = jnp.concatenate([halves[2 * k][...], halves[2 * k + 1][...]], axis=0)
        rows = dot(by_quarter, rows).astype(BF16)
        parts.append([rows[q * slots : (q + 1) * slots] for q in range(4)])
    parts = [jnp.concatenate(part, axis=0) for part in zip(*parts)]
    if arrived is None:
        whole = jnp.concatenate(parts, axis=1)
        gate_hidden, up_hidden = (dot(whole, gate[0]), dot(whole, up[0]))
    else:
        gate_hidden = up_hidden = 0.0
        for q, part in enumerate(parts):
            span = slice(q * cut, (q + 1) * cut)
            arrived(0, q)
            gate_hidden = gate_hidden + dot(part, gate[0, span, :])
            arrived(1, q)
            up_hidden = up_hidden + dot(part, up[0, span, :])
    active = (jax.nn.silu(gate_hidden) * up_hidden).astype(BF16)
    made = []
    for q in range(4):
        if arrived is not None:
            arrived(2, q)
        made.append(dot(active, down[0, :, q * cut : (q + 1) * cut]).astype(BF16))
    in_lines = ones_where(
        iota(square, 1) == (iota(square, 0) % 4) * slots + iota(square, 0) // 4, BF16
    )
    for k in range(count):
        stacked = jnp.concatenate([m[k * slots : (k + 1) * slots] for m in made], axis=0)
        product = dot(in_lines, stacked).astype(BF16)
        results[2 * k][...] = product[: lines // 2]
        results[2 * k + 1][...] = product[lines // 2 :]


def own_rows_kernel(first, last, gate, up, down, made_first, made_last, *held):
    *weights, semaphores = held
    cut = first.shape[1]

    def fetch(which, q):
        source = (gate, up, down)[which]
        span = pl.ds(q * cut, cut)
        place = (0, slice(None), span) if which == 2 else (0, span, slice(None))
        return pltpu.make_async_copy(
            source.at[place], weights[which].at[place], semaphores.at[which * 4 + q]
        )

    for q in range(4):
        fetch(0, q).start()
        fetch(1, q).start()
    for q in range(4):
        fetch(2, q).start()
    expert_kernel(
        (first, last), weights, (made_first, made_last), lambda which, q: fetch(which, q).wait()
    )


def other_rows_kernel(count, *refs):
    expert_kernel(refs[:count], refs[count : count + 3], refs[count + 3 : 2 * count + 3])


def total_kernel(*refs):
    *parts, out = refs
    half = out.shape[0] // 2
    for side in range(2):
        chosen = parts[3 * side : 3 * side + 3]
        out[side * half : (side + 1) * half, :] = sum(p[...].astype(F32) for p in chosen).astype(BF16)


def combine_kernel(results, weigh, stream, final_gain, out):
    rows = stream.shape[0]
    mixture = dot(weigh[...], results[...])
    height = mixture.shape[0] // 3
    mixture = (mixture[:height] + mixture[height : 2 * height]) + mixture[2 * height :]
    mixture = jnp.concatenate([mixture[q * rows : (q + 1) * rows] for q in range(4)], axis=1)
    out[...] = (stream[...].astype(F32) + normalized(mixture, final_gain[...])).astype(BF16)


def call(kernel, outs, *args, flops=0, in_place=(), scratch=()):
    whole = pl.BlockSpec(memory_space=pltpu.VMEM)
    left = pl.BlockSpec(memory_space=pl.ANY)
    single = not isinstance(outs, list)
    shapes = [
        jax.ShapeDtypeStruct(*out) if isinstance(out, tuple) else out
        for out in ([outs] if single else outs)
    ]
    made = pl.pallas_call(
        kernel,
        out_shape=shapes,
        in_specs=[left if k in in_place else whole for k in range(len(args))],
        out_specs=[whole] * len(shapes),
        scratch_shapes=list(scratch),
        cost_estimate=pl.CostEstimate(flops=flops, bytes_accessed=0, transcendentals=0),
        compiler_params=pltpu.CompilerParams(vmem_limit_bytes=VMEM_LIMIT),
    )(*args)
    return made[0] if single else made


VMEM_LIMIT = 24 * 2**20


def in_hbm(value):
    return pltpu.with_memory_space_constraint(value, pltpu.HBM)


def across_sp(pieces):
    return lax.all_to_all(pieces, "sp", split_axis=0, concat_axis=0, tiled=True)


def shifted(part, by):
    size = lax.axis_size("tp")
    return lax.ppermute(part, "tp", [(i, (i + by) % size) for i in range(size)])


def added(first, second):
    return (first.astype(F32) + second.astype(F32)).astype(BF16)


def run_expert(weights, own):
    lines, cut = own.shape
    half = (lines // 2, cut)
    work = 2 * (lines // 4) * 3 * weights[0].shape[1] * weights[0].shape[2]
    first, last = (own[: half[0]], own[half[0] :])
    left_first, right_last = (shifted(first, 1), shifted(last, -1))
    left_last, right_first = (shifted(last, 1), shifted(first, -1))
    across_first, across_last = (shifted(left_first, 1), shifted(right_last, -1))
    own_first, own_last, *held = call(
        own_rows_kernel,
        [(half, BF16), (half, BF16), *(pltpu.VMEM(w.shape, w.dtype) for w in weights)],
        first,
        last,
        *(in_hbm(w) for w in weights),
        flops=work,
        in_place=(2, 3, 4),
        scratch=[pltpu.SemaphoreType.DMA((12,))],
    )

    def part(*halves):
        count = len(halves)
        return call(
            lambda *refs: other_rows_kernel(count, *refs), [(half, BF16)] * count,
            *halves, *held, flops=work * count // 2,
        )

    to_left_first, to_right_last = part(left_first, right_last)
    from_left_last, from_right_first = (shifted(to_right_last, 1), shifted(to_left_first, -1))
    to_left_last, to_right_first = part(left_last, right_first)
    far_first, far_last = part(across_first, across_last)
    to_right_first = added(to_right_first, shifted(far_first, 1))
    to_left_last = added(to_left_last, shifted(far_last, -1))
    from_left_first, from_right_last = (shifted(to_right_first, 1), shifted(to_left_last, -1))

    return call(
        total_kernel, (own.shape, BF16),
        own_first, from_left_first, from_right_first,
        own_last, from_left_last, from_right_last,
        flops=10**6,
    )


def on_device(
    mixer_input,
    step_shift,
    log_step,
    decay_real,
    freq_imag,
    in_real,
    in_imag,
    out_real,
    out_imag,
    skip_gain,
    out_weight,
    residual,
    post_gain,
    pre_gain,
    final_gain,
    route_ids,
    route_logits,
    expert_gate,
    expert_up,
    expert_down,
):
    devices, quarters = (lax.axis_size("sp"), lax.axis_size("tp"))
    rows, width = residual.shape
    length, wide = (mixer_input.shape[0], decay_real.size)
    channels = mixer_input.shape[1]
    slots = 2 * devices
    message, rates, read, cum_real, cum_imag, local_out = call(
        mixer_kernel,
        [
            ((devices, *MESSAGE), BF16),
            ((8, wide), F32),
            ((2 * wide, 2 * channels), BF16),
            ((length, wide), F32),
            ((length, wide), F32),
            ((length, channels), F32),
        ],
        *map(
            in_hbm,
            (
                step_shift.T,
                mixer_input,
                log_step[None],
                decay_real,
                freq_imag,
                jnp.swapaxes(in_real, 1, 2),
                jnp.swapaxes(in_imag, 1, 2),
                out_real,
                out_imag,
                skip_gain[None],
            ),
        ),
        flops=10**9,
    )
    got = across_sp(message)
    partial, place, weigh = call(
        carry_kernel,
        [
            ((length, width), BF16),
            ((4 * slots, slots), BF16),
            ((3 * slots, 4 * slots), BF16),
        ],
        got, rates, read, cum_real, cum_imag, local_out,
        out_weight,
        route_ids.T,
        route_logits.T,
        flops=10**9,
    )
    parts = lax.all_to_all(
        partial.reshape(quarters, rows, width), "tp", split_axis=0, concat_axis=0, tiled=True
    )
    stream, outgoing = call(
        project_kernel,
        [((rows, width), BF16), ((4 * slots, width // 4), BF16)],
        parts.reshape(-1, width),
        residual,
        post_gain[None],
        pre_gain[None],
        place,
        flops=10**9,
    )
    pieces = (devices, 4 * slots // devices, width // 4)
    arrived = across_sp(outgoing.reshape(pieces))
    summed = run_expert((expert_gate, expert_up, expert_down), arrived.reshape(outgoing.shape))
    results = across_sp(summed.reshape(pieces))
    return call(
        combine_kernel, ((rows, width), BF16),
        results.reshape(outgoing.shape), weigh, stream, final_gain[None], flops=10**9,
    )


def solution(mesh):
    in_specs = (
        P("sp", "tp"),
        P("sp", "tp"),
        P("tp"),
        P("tp", None),
        P("tp", None),
        P("tp", None, None),
        P("tp", None, None),
        P("tp", None, None),
        P("tp", None, None),
        P("tp"),
        P("tp", None),
        P(("sp", "tp"), None),
        P(),
        P(),
        P(),
        P("sp", None),
        P("sp", None),
        P("sp", None, "tp"),
        P("sp", None, "tp"),
        P("sp", "tp", None),
    )
    out_specs = P(("sp", "tp"), None)

    return jax.shard_map(
        on_device, mesh=mesh, in_specs=in_specs, out_specs=out_specs, check_vma=False
    )
```

```python
import jax
import jax.numpy as jnp
from jax import lax
from jax.experimental import pallas as pl
from jax.experimental.pallas import tpu as pltpu
from jax.sharding import PartitionSpec as P


F32 = jnp.float32
BF16 = jnp.bfloat16
EPS = 1e-06
STEP_LIMIT = 300.0
MESSAGE = (2, 640)


def dot(first, second, over=(1, 0)):
    dims = (((over[0],), (over[1],)), ((), ()))
    return lax.dot_general(first, second, dims, preferred_element_type=F32)


def iota(shape, dim):
    return lax.broadcasted_iota(jnp.int32, shape, dim)


def ones_where(mask, dtype=F32):
    return jnp.where(mask, 1.0, 0.0).astype(dtype)


def sine_cosine(angle):
    quarter = jnp.floor(angle * 0.6366197723675814 + 0.5)
    rest = angle - quarter * 1.5703125
    rest = rest - quarter * 0.0004825592041015625
    rest = rest - quarter * 1.26759079e-06
    square = rest * rest
    sine = ((-1.9515295891e-4 * square + 8.3321608736e-3) * square - 1.6666654611e-1) * square
    sine = sine * rest + rest
    cosine = (2.443315711809948e-5 * square - 1.388731625493765e-3) * square
    cosine = (cosine + 4.166664568298827e-2) * square * square - 0.5 * square + 1.0
    turn = quarter.astype(jnp.int32)
    odd = (turn & 1) == 1
    first, second = (jnp.where(odd, cosine, sine), jnp.where(odd, sine, cosine))
    return (
        jnp.where((turn & 2) == 2, -first, first),
        jnp.where(((turn + 1) & 2) == 2, -second, second),
    )


def rotation(decay, freq, step):
    sine, cosine = sine_cosine(freq * step)
    magnitude = jnp.exp(decay * step)
    return (magnitude * cosine, magnitude * sine)


def delayed(values, by, fill):
    if by >= 8:
        head = jnp.full((by, values.shape[1]), fill, F32)
        return jnp.concatenate([head, values[: values.shape[0] - by]], axis=0)
    return jnp.where(iota(values.shape, 0) >= by, pltpu.roll(values, by, 0), fill)


def split(values, count):
    found = []
    for _ in range(count):
        found.append(values.astype(BF16))
        values = values - found[-1].astype(F32)
    return found


def repeated(values, width):
    pair = jnp.concatenate([values, values], axis=1)
    return jnp.concatenate([pair] * (width // pair.shape[1]), axis=1)


def read_out(state_real, state_imag, read):
    high, low = split(jnp.concatenate([state_real, state_imag], axis=1), 2)
    both = dot(jnp.concatenate([high, low], axis=0), read[...])
    rows, cut = (state_real.shape[0], both.shape[1] // 2)
    return (both[:rows, :cut] + both[:rows, cut:]) + (both[rows:, :cut] + both[rows:, cut:])


def mixer_kernel(
    shift, inputs, log_step, decay_real, freq_imag, in_real, in_imag, out_real, out_imag,
    message, rates, read, cum_real, cum_imag, own_real, own_imag,
):
    groups, length = shift.shape
    states = decay_real.shape[1]
    channels = in_real.shape[1]
    width = groups * states
    own = iota((groups, width), 1) // states == iota((groups, width), 0)
    square = (groups, groups)
    log_column = jnp.sum(
        jnp.where(iota(square, 0) == iota(square, 1), log_step[...], 0.0), axis=1, keepdims=True
    )
    small_step = jnp.minimum(jnp.exp(log_column + shift[...]), STEP_LIMIT)
    step = dot(jnp.concatenate(split(small_step.T, 3), axis=0), ones_where(own, BF16))
    step = (step[:length] + step[length : 2 * length]) + step[2 * length :]

    def row(ref):
        return jnp.sum(jnp.where(own, repeated(ref[...], width), 0.0), axis=0, keepdims=True)

    decay, freq = (row(decay_real), row(freq_imag))
    rates[...] = jnp.concatenate([decay, freq, jnp.zeros((6, width), F32)], axis=0)
    wide = (groups * channels, width)
    block = iota(wide, 0) // channels == iota(wide, 1) // states
    values = inputs[...]
    doubled = jnp.concatenate([values, values], axis=1)

    def driven(ref):
        spread = jnp.where(block, repeated(ref[...].reshape(wide[0], states), width), 0.0)
        return dot(doubled, jnp.concatenate(split(spread, 2), axis=0))

    into_real, into_imag = (driven(in_real), driven(in_imag))
    tall = (width, wide[0])
    block = iota(tall, 0) // states == iota(tall, 1) // channels

    def reading(ref):
        turned = ref[...].reshape(wide[0], states).T
        return jnp.where(block, jnp.concatenate([turned] * groups, axis=0), 0.0)

    read[...] = jnp.concatenate(
        split(jnp.concatenate([reading(out_real), -reading(out_imag)], axis=0), 2), axis=1
    )
    inverse = 1.0 / (decay * decay + freq * freq)
    last_real, last_imag = ([], [])
    for start in range(0, width, 128):
        cut = slice(start, start + 128)
        a_real, a_imag = rotation(decay[:, cut], freq[:, cut], step[:, cut])
        minus_one = a_real - 1.0
        coef_real = (minus_one * decay[:, cut] + a_imag * freq[:, cut]) * inverse[:, cut]
        coef_imag = (a_imag * decay[:, cut] - minus_one * freq[:, cut]) * inverse[:, cut]
        s_real = coef_real * into_real[:, cut] - coef_imag * into_imag[:, cut]
        s_imag = coef_real * into_imag[:, cut] + coef_imag * into_real[:, cut]
        by = 1
        while by < length:
            p_real, p_imag = (delayed(s_real, by, 0.0), delayed(s_imag, by, 0.0))
            b_real, b_imag = (delayed(a_real, by, 1.0), delayed(a_imag, by, 0.0))
            s_real, s_imag = (
                s_real + a_real * p_real - a_imag * p_imag,
                s_imag + a_real * p_imag + a_imag * p_real,
            )
            a_real, a_imag = (a_real * b_real - a_imag * b_imag, a_real * b_imag + a_imag * b_real)
            by *= 2
        cum_real[:, cut] = a_real
        cum_imag[:, cut] = a_imag
        own_real[:, cut] = s_real
        own_imag[:, cut] = s_imag
        last_real.append(s_real[length - 1 :])
        last_imag.append(s_imag[length - 1 :])
    lanes = MESSAGE[1] - width
    pick = (width, lanes)
    compress = ones_where(
        (iota(pick, 0) == (iota(pick, 1) % groups) * states) & (iota(pick, 1) < 3 * groups), BF16
    )
    total = jnp.concatenate(split(jnp.sum(step, axis=0, keepdims=True), 3), axis=0)
    first, second, third = [part[None] for part in dot(total, compress)]
    lane = iota(first.shape, 1)
    total = jnp.where(lane < groups, first, jnp.where(lane < 2 * groups, second, third))
    lines = [
        jnp.concatenate([*part, rest], axis=1)
        for part, rest in ((last_real, total), (last_imag, jnp.zeros_like(total)))
    ]
    sent = jnp.concatenate(lines, axis=0)
    message[...] = jnp.broadcast_to(sent[None], message.shape).astype(BF16)


def carry_kernel(
    got, rates, read, cum_real, cum_imag, own_real, own_imag, inputs, skip, out_weight, ids,
    logits, kept, sent_1, sent_2, sent_3, place, weigh,
):
    routing(ids, logits, place, weigh)
    devices = got.shape[0]
    width = rates.shape[1]
    lanes = MESSAGE[1] - width
    groups = 8
    states = width // groups
    mine = lax.axis_index("sp")
    decay, freq = (rates[0:1, :], rates[1:2, :])
    everything = got[...].astype(F32)
    got_real, got_imag = (everything[:, 0, :width], everything[:, 1, :width])
    totals = everything[:, 0, width:]
    square = (devices, devices)
    between = (iota(square, 0) < iota(square, 1)) & (iota(square, 1) < mine)
    sums = dot(ones_where(between, BF16), totals.astype(BF16))
    wide = (lanes, width)
    spread = ones_where(
        (iota(wide, 0) < 3 * groups) & (iota(wide, 0) % groups == iota(wide, 1) // states), BF16
    )
    elapsed = dot(jnp.concatenate(split(sums, 3), axis=0), spread)
    elapsed = (elapsed[:devices] + elapsed[devices : 2 * devices]) + elapsed[2 * devices :]
    elapsed = jnp.minimum(elapsed, STEP_LIMIT)
    weight_real, weight_imag = rotation(decay, freq, elapsed)
    earlier = iota((devices, width), 0) < mine
    weight_real = jnp.where(earlier, weight_real, 0.0)
    weight_imag = jnp.where(earlier, weight_imag, 0.0)
    carry_real = jnp.sum(weight_real * got_real - weight_imag * got_imag, axis=0, keepdims=True)
    carry_imag = jnp.sum(weight_real * got_imag + weight_imag * got_real, axis=0, keepdims=True)
    c_real, c_imag = (cum_real[...], cum_imag[...])
    result = skip[...] * inputs[...].astype(F32) + read_out(
        own_real[...] + (c_real * carry_real - c_imag * carry_imag),
        own_imag[...] + (c_real * carry_imag + c_imag * carry_real),
        read,
    )
    mixed = jax.nn.gelu(result)
    rows, length = (kept.shape[0], mixed.shape[0])
    ahead = lax.rem(length - lax.axis_index("tp") * rows, length)
    partial = dot(pltpu.roll(mixed, ahead, 0).astype(BF16), out_weight[...])
    kept[...] = partial[:rows]
    for by, sent in enumerate((sent_1, sent_2, sent_3), 1):
        sent[...] = partial[by * rows : (by + 1) * rows].astype(BF16)


def routing(ids, logits, place, weigh):
    slots = ids.shape[1]
    tall = (slots, slots)
    rows = slots // 4
    member, lane = (iota(tall, 0) % rows, iota(tall, 1))
    here = lane == lax.axis_index("tp") * rows + member

    def column(line):
        return jnp.sum(jnp.where(here, line, 0.0), axis=1, keepdims=True)

    named = ids[...].astype(F32)
    expert = (lane // 2).astype(F32)
    is_first = ones_where(column(named[0:1]) == expert)
    is_second = ones_where(column(named[1:2]) == expert)
    before = ones_where((lane % rows < member) & (lane // rows == iota(tall, 0) // rows), BF16)
    count = dot(before, (is_first + is_second).astype(BF16))
    kept = ones_where(count == (lane % 2).astype(F32))
    first = jax.nn.sigmoid(column(logits[0:1, :]) - column(logits[1:2, :]))
    long = (slots * 4, slots)
    repeat = ones_where(iota(long, 0) // 4 == iota(long, 1), BF16)
    put = dot(repeat, ((is_first + is_second) * kept).astype(BF16), (1, 1))
    place[...] = jnp.where(iota(long, 0) % 4 == iota(long, 1) // rows, put, 0.0).astype(BF16)
    weight = (is_first * first + is_second * (1.0 - first)) * kept
    back = (slots, slots * 4)
    repeat = ones_where(iota(back, 1) // 4 == iota(back, 0), BF16)
    took = dot(jnp.concatenate(split(weight, 3), axis=0), repeat)
    fits = iota(took.shape, 1) % 4 == (iota(took.shape, 0) % slots) // rows
    weigh[...] = jnp.where(fits, took, 0.0).astype(BF16)


def normalized(values, gain):
    return values * lax.rsqrt(jnp.mean(values * values, axis=-1, keepdims=True) + EPS) * gain


def project_kernel(
    kept, got_1, got_2, got_3, residual, post_gain, pre_gain, place, stream, outgoing
):
    width = residual.shape[1]
    projected = kept[...] + sum(got[...].astype(F32) for got in (got_1, got_2, got_3))
    own = (residual[...].astype(F32) + normalized(projected, post_gain[...])).astype(BF16)
    stream[...] = own
    normed = normalized(own.astype(F32), pre_gain[...]).astype(BF16)
    cut = width // 4
    stacked = jnp.concatenate([normed[:, q * cut : (q + 1) * cut] for q in range(4)], axis=0)
    outgoing[...] = dot(place[...], stacked).astype(BF16)


def expert_kernel(halves, weights, results, arrived=None):
    gate, up, down = weights
    count = len(halves) // 2
    lines, cut = (2 * halves[0].shape[0], halves[0].shape[1])
    slots = lines // 4
    square = (lines, lines)
    by_quarter = ones_where(
        iota(square, 1) == (iota(square, 0) % slots) * 4 + iota(square, 0) // slots, BF16
    )
    parts = []
    for k in range(count):
        rows = jnp.concatenate([halves[2 * k][...], halves[2 * k + 1][...]], axis=0)
        rows = dot(by_quarter, rows).astype(BF16)
        parts.append([rows[q * slots : (q + 1) * slots] for q in range(4)])
    parts = [jnp.concatenate(part, axis=0) for part in zip(*parts)]
    if arrived is None:
        whole = jnp.concatenate(parts, axis=1)
        gate_hidden, up_hidden = (dot(whole, gate[0]), dot(whole, up[0]))
    else:
        gate_hidden = up_hidden = 0.0
        for q, part in enumerate(parts):
            span = slice(q * cut, (q + 1) * cut)
            arrived(0, q)
            gate_hidden = gate_hidden + dot(part, gate[0, span, :])
            arrived(1, q)
            up_hidden = up_hidden + dot(part, up[0, span, :])
    active = (jax.nn.silu(gate_hidden) * up_hidden).astype(BF16)
    made = []
    for q in range(4):
        if arrived is not None:
            arrived(2, q)
        made.append(dot(active, down[0, :, q * cut : (q + 1) * cut]).astype(BF16))
    in_lines = ones_where(
        iota(square, 1) == (iota(square, 0) % 4) * slots + iota(square, 0) // 4, BF16
    )
    for k in range(count):
        stacked = jnp.concatenate([m[k * slots : (k + 1) * slots] for m in made], axis=0)
        product = dot(in_lines, stacked).astype(BF16)
        results[2 * k][...] = product[: lines // 2]
        results[2 * k + 1][...] = product[lines // 2 :]


def own_rows_kernel(first, last, gate, up, down, made_first, made_last, *held):
    *weights, semaphores = held
    cut = first.shape[1]

    def fetch(which, q):
        source = (gate, up, down)[which]
        span = pl.ds(q * cut, cut)
        place = (0, slice(None), span) if which == 2 else (0, span, slice(None))
        return pltpu.make_async_copy(
            source.at[place], weights[which].at[place], semaphores.at[which * 4 + q]
        )

    for q in range(4):
        fetch(0, q).start()
        fetch(1, q).start()
    for q in range(4):
        fetch(2, q).start()
    expert_kernel(
        (first, last), weights, (made_first, made_last), lambda which, q: fetch(which, q).wait()
    )


def other_rows_kernel(count, *refs):
    expert_kernel(refs[:count], refs[count : count + 3], refs[count + 3 : 2 * count + 3])


def total_kernel(*refs):
    *parts, out = refs
    half = out.shape[0] // 2
    for side in range(2):
        chosen = parts[3 * side : 3 * side + 3]
        out[side * half : (side + 1) * half, :] = sum(p[...].astype(F32) for p in chosen).astype(BF16)


def combine_kernel(results, weigh, stream, final_gain, out):
    rows = stream.shape[0]
    mixture = dot(weigh[...], results[...])
    height = mixture.shape[0] // 3
    mixture = (mixture[:height] + mixture[height : 2 * height]) + mixture[2 * height :]
    mixture = jnp.concatenate([mixture[q * rows : (q + 1) * rows] for q in range(4)], axis=1)
    out[...] = (stream[...].astype(F32) + normalized(mixture, final_gain[...])).astype(BF16)


def call(kernel, outs, *args, flops=0, in_place=(), scratch=()):
    whole = pl.BlockSpec(memory_space=pltpu.VMEM)
    left = pl.BlockSpec(memory_space=pl.ANY)
    single = not isinstance(outs, list)
    shapes = [
        jax.ShapeDtypeStruct(*out) if isinstance(out, tuple) else out
        for out in ([outs] if single else outs)
    ]
    made = pl.pallas_call(
        kernel,
        out_shape=shapes,
        in_specs=[left if k in in_place else whole for k in range(len(args))],
        out_specs=[whole] * len(shapes),
        scratch_shapes=list(scratch),
        cost_estimate=pl.CostEstimate(flops=flops, bytes_accessed=0, transcendentals=0),
        compiler_params=pltpu.CompilerParams(vmem_limit_bytes=VMEM_LIMIT),
    )(*args)
    return made[0] if single else made


VMEM_LIMIT = 24 * 2**20


def in_hbm(value):
    return pltpu.with_memory_space_constraint(value, pltpu.HBM)


def across_sp(pieces):
    return lax.all_to_all(pieces, "sp", split_axis=0, concat_axis=0, tiled=True)


def shifted(part, by):
    size = lax.axis_size("tp")
    return lax.ppermute(part, "tp", [(i, (i + by) % size) for i in range(size)])


def added(first, second):
    return (first.astype(F32) + second.astype(F32)).astype(BF16)


def run_expert(weights, own):
    lines, cut = own.shape
    half = (lines // 2, cut)
    work = 2 * (lines // 4) * 3 * weights[0].shape[1] * weights[0].shape[2]
    first, last = (own[: half[0]], own[half[0] :])
    left_first, right_last = (shifted(first, 1), shifted(last, -1))
    left_last, right_first = (shifted(last, 1), shifted(first, -1))
    across_first, across_last = (shifted(left_first, 1), shifted(right_last, -1))
    own_first, own_last, *held = call(
        own_rows_kernel,
        [(half, BF16), (half, BF16), *(pltpu.VMEM(w.shape, w.dtype) for w in weights)],
        first,
        last,
        *(in_hbm(w) for w in weights),
        flops=work,
        in_place=(2, 3, 4),
        scratch=[pltpu.SemaphoreType.DMA((12,))],
    )

    def part(*halves):
        count = len(halves)
        return call(
            lambda *refs: other_rows_kernel(count, *refs), [(half, BF16)] * count,
            *halves, *held, flops=work * count // 2,
        )

    to_left_first, to_right_last = part(left_first, right_last)
    from_left_last, from_right_first = (shifted(to_right_last, 1), shifted(to_left_first, -1))
    to_left_last, to_right_first = part(left_last, right_first)
    far_first, far_last = part(across_first, across_last)
    to_right_first = added(to_right_first, shifted(far_first, 1))
    to_left_last = added(to_left_last, shifted(far_last, -1))
    from_left_first, from_right_last = (shifted(to_right_first, 1), shifted(to_left_last, -1))

    return call(
        total_kernel, (own.shape, BF16),
        own_first, from_left_first, from_right_first,
        own_last, from_left_last, from_right_last,
        flops=10**6,
    )


def on_device(
    mixer_input,
    step_shift,
    log_step,
    decay_real,
    freq_imag,
    in_real,
    in_imag,
    out_real,
    out_imag,
    skip_gain,
    out_weight,
    residual,
    post_gain,
    pre_gain,
    final_gain,
    route_ids,
    route_logits,
    expert_gate,
    expert_up,
    expert_down,
):
    devices, quarters = (lax.axis_size("sp"), lax.axis_size("tp"))
    rows, width = residual.shape
    length, wide = (mixer_input.shape[0], decay_real.size)
    channels = mixer_input.shape[1]
    slots = 2 * devices
    message, rates, read, cum_real, cum_imag, own_real, own_imag = call(
        mixer_kernel,
        [
            ((devices, *MESSAGE), BF16),
            ((8, wide), F32),
            ((2 * wide, 2 * channels), BF16),
            ((length, wide), F32),
            ((length, wide), F32),
            ((length, wide), F32),
            ((length, wide), F32),
        ],
        *map(
            in_hbm,
            (
                step_shift.T,
                mixer_input,
                log_step[None],
                decay_real,
                freq_imag,
                jnp.swapaxes(in_real, 1, 2),
                jnp.swapaxes(in_imag, 1, 2),
                out_real,
                out_imag,
            ),
        ),
        flops=10**9,
    )
    got = across_sp(message)
    kept, *sent, place, weigh = call(
        carry_kernel,
        [
            ((rows, width), F32),
            *(((rows, width), BF16),) * (quarters - 1),
            ((4 * slots, slots), BF16),
            ((3 * slots, 4 * slots), BF16),
        ],
        got, rates, read, cum_real, cum_imag, own_real, own_imag,
        mixer_input,
        skip_gain[None],
        out_weight,
        route_ids.T,
        route_logits.T,
        flops=10**9,
    )
    stream, outgoing = call(
        project_kernel,
        [((rows, width), BF16), ((4 * slots, width // 4), BF16)],
        kept,
        *(shifted(part, by) for by, part in enumerate(sent, 1)),
        residual,
        post_gain[None],
        pre_gain[None],
        place,
        flops=10**9,
    )
    pieces = (devices, 4 * slots // devices, width // 4)
    arrived = across_sp(outgoing.reshape(pieces))
    summed = run_expert((expert_gate, expert_up, expert_down), arrived.reshape(outgoing.shape))
    results = across_sp(summed.reshape(pieces))
    return call(
        combine_kernel, ((rows, width), BF16),
        results.reshape(outgoing.shape), weigh, stream, final_gain[None], flops=10**9,
    )


def solution(mesh):
    in_specs = (
        P("sp", "tp"),
        P("sp", "tp"),
        P("tp"),
        P("tp", None),
        P("tp", None),
        P("tp", None, None),
        P("tp", None, None),
        P("tp", None, None),
        P("tp", None, None),
        P("tp"),
        P("tp", None),
        P(("sp", "tp"), None),
        P(),
        P(),
        P(),
        P("sp", None),
        P("sp", None),
        P("sp", None, "tp"),
        P("sp", None, "tp"),
        P("sp", "tp", None),
    )
    out_specs = P(("sp", "tp"), None)

    return jax.shard_map(
        on_device, mesh=mesh, in_specs=in_specs, out_specs=out_specs, check_vma=False
    )
```

```python
import jax
import jax.numpy as jnp
from jax import lax
from jax.experimental import pallas as pl
from jax.experimental.pallas import tpu as pltpu
from jax.sharding import PartitionSpec as P


F32 = jnp.float32
BF16 = jnp.bfloat16
EPS = 1e-06
STEP_LIMIT = 300.0
MESSAGE = (2, 640)


def dot(first, second, over=(1, 0)):
    dims = (((over[0],), (over[1],)), ((), ()))
    return lax.dot_general(first, second, dims, preferred_element_type=F32)


def iota(shape, dim):
    return lax.broadcasted_iota(jnp.int32, shape, dim)


def ones_where(mask, dtype=F32):
    return jnp.where(mask, 1.0, 0.0).astype(dtype)


def sine_cosine(angle):
    quarter = jnp.floor(angle * 0.6366197723675814 + 0.5)
    rest = angle - quarter * 1.5703125
    rest = rest - quarter * 0.0004825592041015625
    rest = rest - quarter * 1.26759079e-06
    square = rest * rest
    sine = ((-1.9515295891e-4 * square + 8.3321608736e-3) * square - 1.6666654611e-1) * square
    sine = sine * rest + rest
    cosine = (2.443315711809948e-5 * square - 1.388731625493765e-3) * square
    cosine = (cosine + 4.166664568298827e-2) * square * square - 0.5 * square + 1.0
    turn = quarter.astype(jnp.int32)
    odd = (turn & 1) == 1
    first, second = (jnp.where(odd, cosine, sine), jnp.where(odd, sine, cosine))
    return (
        jnp.where((turn & 2) == 2, -first, first),
        jnp.where(((turn + 1) & 2) == 2, -second, second),
    )


def rotation(decay, freq, step):
    sine, cosine = sine_cosine(freq * step)
    magnitude = jnp.exp(decay * step)
    return (magnitude * cosine, magnitude * sine)


def delayed(values, by, fill):
    if by >= 8:
        head = jnp.full((by, values.shape[1]), fill, F32)
        return jnp.concatenate([head, values[: values.shape[0] - by]], axis=0)
    return jnp.where(iota(values.shape, 0) >= by, pltpu.roll(values, by, 0), fill)


def split(values, count):
    found = []
    for _ in range(count):
        found.append(values.astype(BF16))
        values = values - found[-1].astype(F32)
    return found


def repeated(values, width):
    pair = jnp.concatenate([values, values], axis=1)
    return jnp.concatenate([pair] * (width // pair.shape[1]), axis=1)


def read_out(state_real, state_imag, read):
    high, low = split(jnp.concatenate([state_real, state_imag], axis=1), 2)
    both = dot(jnp.concatenate([high, low], axis=0), read[...])
    rows, cut = (state_real.shape[0], both.shape[1] // 2)
    return (both[:rows, :cut] + both[:rows, cut:]) + (both[rows:, :cut] + both[rows:, cut:])


def mixer_kernel(
    shift, inputs, log_step, decay_real, freq_imag, in_real, in_imag, out_real, out_imag,
    message, rates, read, cum_real, cum_imag, own_real, own_imag,
):
    groups, length = shift.shape
    states = decay_real.shape[1]
    channels = in_real.shape[1]
    width = groups * states
    own = iota((groups, width), 1) // states == iota((groups, width), 0)
    square = (groups, groups)
    log_column = jnp.sum(
        jnp.where(iota(square, 0) == iota(square, 1), log_step[...], 0.0), axis=1, keepdims=True
    )
    small_step = jnp.minimum(jnp.exp(log_column + shift[...]), STEP_LIMIT)
    step = dot(jnp.concatenate(split(small_step.T, 3), axis=0), ones_where(own, BF16))
    step = (step[:length] + step[length : 2 * length]) + step[2 * length :]

    def row(ref):
        return jnp.sum(jnp.where(own, repeated(ref[...], width), 0.0), axis=0, keepdims=True)

    decay, freq = (row(decay_real), row(freq_imag))
    rates[...] = jnp.concatenate([decay, freq, jnp.zeros((6, width), F32)], axis=0)
    wide = (groups * channels, width)
    block = iota(wide, 0) // channels == iota(wide, 1) // states
    values = inputs[...]
    doubled = jnp.concatenate([values, values], axis=1)

    def driven(ref):
        spread = jnp.where(block, repeated(ref[...].reshape(wide[0], states), width), 0.0)
        return dot(doubled, jnp.concatenate(split(spread, 2), axis=0))

    into_real, into_imag = (driven(in_real), driven(in_imag))
    tall = (width, wide[0])
    block = iota(tall, 0) // states == iota(tall, 1) // channels

    def reading(ref):
        turned = ref[...].reshape(wide[0], states).T
        return jnp.where(block, jnp.concatenate([turned] * groups, axis=0), 0.0)

    read[...] = jnp.concatenate(
        split(jnp.concatenate([reading(out_real), -reading(out_imag)], axis=0), 2), axis=1
    )
    inverse = 1.0 / (decay * decay + freq * freq)
    last_real, last_imag = ([], [])
    for start in range(0, width, 128):
        cut = slice(start, start + 128)
        a_real, a_imag = rotation(decay[:, cut], freq[:, cut], step[:, cut])
        minus_one = a_real - 1.0
        coef_real = (minus_one * decay[:, cut] + a_imag * freq[:, cut]) * inverse[:, cut]
        coef_imag = (a_imag * decay[:, cut] - minus_one * freq[:, cut]) * inverse[:, cut]
        s_real = coef_real * into_real[:, cut] - coef_imag * into_imag[:, cut]
        s_imag = coef_real * into_imag[:, cut] + coef_imag * into_real[:, cut]
        by = 1
        while by < length:
            p_real, p_imag = (delayed(s_real, by, 0.0), delayed(s_imag, by, 0.0))
            b_real, b_imag = (delayed(a_real, by, 1.0), delayed(a_imag, by, 0.0))
            s_real, s_imag = (
                s_real + a_real * p_real - a_imag * p_imag,
                s_imag + a_real * p_imag + a_imag * p_real,
            )
            a_real, a_imag = (a_real * b_real - a_imag * b_imag, a_real * b_imag + a_imag * b_real)
            by *= 2
        cum_real[:, cut] = a_real
        cum_imag[:, cut] = a_imag
        own_real[:, cut] = s_real
        own_imag[:, cut] = s_imag
        last_real.append(s_real[length - 1 :])
        last_imag.append(s_imag[length - 1 :])
    lanes = MESSAGE[1] - width
    pick = (width, lanes)
    compress = ones_where(
        (iota(pick, 0) == (iota(pick, 1) % groups) * states) & (iota(pick, 1) < 3 * groups), BF16
    )
    total = jnp.concatenate(split(jnp.sum(step, axis=0, keepdims=True), 3), axis=0)
    first, second, third = [part[None] for part in dot(total, compress)]
    lane = iota(first.shape, 1)
    total = jnp.where(lane < groups, first, jnp.where(lane < 2 * groups, second, third))
    lines = [
        jnp.concatenate([*part, rest], axis=1)
        for part, rest in ((last_real, total), (last_imag, jnp.zeros_like(total)))
    ]
    sent = jnp.concatenate(lines, axis=0)
    message[...] = jnp.broadcast_to(sent[None], message.shape).astype(BF16)


def carry_kernel(
    got, rates, read, cum_real, cum_imag, own_real, own_imag, inputs, skip, out_weight,
    kept, sent_1, sent_2, sent_3,
):
    devices = got.shape[0]
    width = rates.shape[1]
    lanes = MESSAGE[1] - width
    groups = 8
    states = width // groups
    mine = lax.axis_index("sp")
    decay, freq = (rates[0:1, :], rates[1:2, :])
    everything = got[...].astype(F32)
    got_real, got_imag = (everything[:, 0, :width], everything[:, 1, :width])
    totals = everything[:, 0, width:]
    square = (devices, devices)
    between = (iota(square, 0) < iota(square, 1)) & (iota(square, 1) < mine)
    sums = dot(ones_where(between, BF16), totals.astype(BF16))
    wide = (lanes, width)
    spread = ones_where(
        (iota(wide, 0) < 3 * groups) & (iota(wide, 0) % groups == iota(wide, 1) // states), BF16
    )
    elapsed = dot(jnp.concatenate(split(sums, 3), axis=0), spread)
    elapsed = (elapsed[:devices] + elapsed[devices : 2 * devices]) + elapsed[2 * devices :]
    elapsed = jnp.minimum(elapsed, STEP_LIMIT)
    weight_real, weight_imag = rotation(decay, freq, elapsed)
    earlier = iota((devices, width), 0) < mine
    weight_real = jnp.where(earlier, weight_real, 0.0)
    weight_imag = jnp.where(earlier, weight_imag, 0.0)
    carry_real = jnp.sum(weight_real * got_real - weight_imag * got_imag, axis=0, keepdims=True)
    carry_imag = jnp.sum(weight_real * got_imag + weight_imag * got_real, axis=0, keepdims=True)
    c_real, c_imag = (cum_real[...], cum_imag[...])
    result = skip[...] * inputs[...].astype(F32) + read_out(
        own_real[...] + (c_real * carry_real - c_imag * carry_imag),
        own_imag[...] + (c_real * carry_imag + c_imag * carry_real),
        read,
    )
    mixed = jax.nn.gelu(result)
    rows, length = (kept.shape[0], mixed.shape[0])
    ahead = lax.rem(length - lax.axis_index("tp") * rows, length)
    partial = dot(pltpu.roll(mixed, ahead, 0).astype(BF16), out_weight[...])
    kept[...] = partial[:rows]
    for by, sent in enumerate((sent_1, sent_2, sent_3), 1):
        sent[...] = partial[by * rows : (by + 1) * rows].astype(BF16)


def route_kernel(ids, logits, place, weigh):
    slots = ids.shape[1]
    tall = (slots, slots)
    rows = slots // 4
    member, lane = (iota(tall, 0) % rows, iota(tall, 1))
    here = lane == lax.axis_index("tp") * rows + member

    def column(line):
        return jnp.sum(jnp.where(here, line, 0.0), axis=1, keepdims=True)

    named = ids[...].astype(F32)
    expert = (lane // 2).astype(F32)
    is_first = ones_where(column(named[0:1]) == expert)
    is_second = ones_where(column(named[1:2]) == expert)
    before = ones_where((lane % rows < member) & (lane // rows == iota(tall, 0) // rows), BF16)
    count = dot(before, (is_first + is_second).astype(BF16))
    kept = ones_where(count == (lane % 2).astype(F32))
    first = jax.nn.sigmoid(column(logits[0:1, :]) - column(logits[1:2, :]))
    long = (slots * 4, slots)
    repeat = ones_where(iota(long, 0) // 4 == iota(long, 1), BF16)
    put = dot(repeat, ((is_first + is_second) * kept).astype(BF16), (1, 1))
    place[...] = jnp.where(iota(long, 0) % 4 == iota(long, 1) // rows, put, 0.0).astype(BF16)
    weight = (is_first * first + is_second * (1.0 - first)) * kept
    back = (slots, slots * 4)
    repeat = ones_where(iota(back, 1) // 4 == iota(back, 0), BF16)
    took = dot(jnp.concatenate(split(weight, 3), axis=0), repeat)
    fits = iota(took.shape, 1) % 4 == (iota(took.shape, 0) % slots) // rows
    weigh[...] = jnp.where(fits, took, 0.0).astype(BF16)


def normalized(values, gain):
    return values * lax.rsqrt(jnp.mean(values * values, axis=-1, keepdims=True) + EPS) * gain


def project_kernel(
    kept, got_1, got_2, got_3, residual, post_gain, pre_gain, place, stream, outgoing
):
    width = residual.shape[1]
    projected = kept[...] + sum(got[...].astype(F32) for got in (got_1, got_2, got_3))
    own = (residual[...].astype(F32) + normalized(projected, post_gain[...])).astype(BF16)
    stream[...] = own
    normed = normalized(own.astype(F32), pre_gain[...]).astype(BF16)
    cut = width // 4
    stacked = jnp.concatenate([normed[:, q * cut : (q + 1) * cut] for q in range(4)], axis=0)
    outgoing[...] = dot(place[...], stacked).astype(BF16)


def expert_kernel(halves, weights, results, arrived=None):
    gate, up, down = weights
    count = len(halves) // 2
    lines, cut = (2 * halves[0].shape[0], halves[0].shape[1])
    slots = lines // 4
    square = (lines, lines)
    by_quarter = ones_where(
        iota(square, 1) == (iota(square, 0) % slots) * 4 + iota(square, 0) // slots, BF16
    )
    parts = []
    for k in range(count):
        rows = jnp.concatenate([halves[2 * k][...], halves[2 * k + 1][...]], axis=0)
        rows = dot(by_quarter, rows).astype(BF16)
        parts.append([rows[q * slots : (q + 1) * slots] for q in range(4)])
    parts = [jnp.concatenate(part, axis=0) for part in zip(*parts)]
    if arrived is None:
        whole = jnp.concatenate(parts, axis=1)
        gate_hidden, up_hidden = (dot(whole, gate[0]), dot(whole, up[0]))
    else:
        gate_hidden = up_hidden = 0.0
        for q, part in enumerate(parts):
            span = slice(q * cut, (q + 1) * cut)
            arrived(0, q)
            gate_hidden = gate_hidden + dot(part, gate[0, span, :])
            arrived(1, q)
            up_hidden = up_hidden + dot(part, up[0, span, :])
    active = (jax.nn.silu(gate_hidden) * up_hidden).astype(BF16)
    made = []
    for q in range(4):
        if arrived is not None:
            arrived(2, q)
        made.append(dot(active, down[0, :, q * cut : (q + 1) * cut]).astype(BF16))
    in_lines = ones_where(
        iota(square, 1) == (iota(square, 0) % 4) * slots + iota(square, 0) // 4, BF16
    )
    for k in range(count):
        stacked = jnp.concatenate([m[k * slots : (k + 1) * slots] for m in made], axis=0)
        product = dot(in_lines, stacked).astype(BF16)
        results[2 * k][...] = product[: lines // 2]
        results[2 * k + 1][...] = product[lines // 2 :]


def own_rows_kernel(first, last, gate, up, down, made_first, made_last, *held):
    *weights, semaphores = held
    cut = first.shape[1]

    def fetch(which, q):
        source = (gate, up, down)[which]
        span = pl.ds(q * cut, cut)
        place = (0, slice(None), span) if which == 2 else (0, span, slice(None))
        return pltpu.make_async_copy(
            source.at[place], weights[which].at[place], semaphores.at[which * 4 + q]
        )

    for q in range(4):
        fetch(0, q).start()
        fetch(1, q).start()
    for q in range(4):
        fetch(2, q).start()
    expert_kernel(
        (first, last), weights, (made_first, made_last), lambda which, q: fetch(which, q).wait()
    )


def other_rows_kernel(count, *refs):
    expert_kernel(refs[:count], refs[count : count + 3], refs[count + 3 : 2 * count + 3])


def total_kernel(*refs):
    *parts, out = refs
    half = out.shape[0] // 2
    for side in range(2):
        chosen = parts[3 * side : 3 * side + 3]
        out[side * half : (side + 1) * half, :] = sum(p[...].astype(F32) for p in chosen).astype(BF16)


def combine_kernel(results, weigh, stream, final_gain, out):
    rows = stream.shape[0]
    mixture = dot(weigh[...], results[...])
    height = mixture.shape[0] // 3
    mixture = (mixture[:height] + mixture[height : 2 * height]) + mixture[2 * height :]
    mixture = jnp.concatenate([mixture[q * rows : (q + 1) * rows] for q in range(4)], axis=1)
    out[...] = (stream[...].astype(F32) + normalized(mixture, final_gain[...])).astype(BF16)


def call(kernel, outs, *args, flops=0, in_place=(), scratch=()):
    whole = pl.BlockSpec(memory_space=pltpu.VMEM)
    left = pl.BlockSpec(memory_space=pl.ANY)
    single = not isinstance(outs, list)
    shapes = [
        jax.ShapeDtypeStruct(*out) if isinstance(out, tuple) else out
        for out in ([outs] if single else outs)
    ]
    made = pl.pallas_call(
        kernel,
        out_shape=shapes,
        in_specs=[left if k in in_place else whole for k in range(len(args))],
        out_specs=[whole] * len(shapes),
        scratch_shapes=list(scratch),
        cost_estimate=pl.CostEstimate(flops=flops, bytes_accessed=0, transcendentals=0),
        compiler_params=pltpu.CompilerParams(vmem_limit_bytes=VMEM_LIMIT),
    )(*args)
    return made[0] if single else made


VMEM_LIMIT = 24 * 2**20


def in_hbm(value):
    return pltpu.with_memory_space_constraint(value, pltpu.HBM)


def across_sp(pieces):
    return lax.all_to_all(pieces, "sp", split_axis=0, concat_axis=0, tiled=True)


def shifted(part, by):
    size = lax.axis_size("tp")
    return lax.ppermute(part, "tp", [(i, (i + by) % size) for i in range(size)])


def added(first, second):
    return (first.astype(F32) + second.astype(F32)).astype(BF16)


def run_expert(weights, own):
    lines, cut = own.shape
    half = (lines // 2, cut)
    work = 2 * (lines // 4) * 3 * weights[0].shape[1] * weights[0].shape[2]
    first, last = (own[: half[0]], own[half[0] :])
    left_first, right_last = (shifted(first, 1), shifted(last, -1))
    left_last, right_first = (shifted(last, 1), shifted(first, -1))
    across_first, across_last = (shifted(left_first, 1), shifted(right_last, -1))
    own_first, own_last, *held = call(
        own_rows_kernel,
        [(half, BF16), (half, BF16), *(pltpu.VMEM(w.shape, w.dtype) for w in weights)],
        first,
        last,
        *(in_hbm(w) for w in weights),
        flops=work,
        in_place=(2, 3, 4),
        scratch=[pltpu.SemaphoreType.DMA((12,))],
    )

    def part(*halves):
        count = len(halves)
        return call(
            lambda *refs: other_rows_kernel(count, *refs), [(half, BF16)] * count,
            *halves, *held, flops=work * count // 2,
        )

    to_left_first, to_right_last = part(left_first, right_last)
    from_left_last, from_right_first = (shifted(to_right_last, 1), shifted(to_left_first, -1))
    to_left_last, to_right_first = part(left_last, right_first)
    far_first, far_last = part(across_first, across_last)
    to_right_first = added(to_right_first, shifted(far_first, 1))
    to_left_last = added(to_left_last, shifted(far_last, -1))
    from_left_first, from_right_last = (shifted(to_right_first, 1), shifted(to_left_last, -1))

    return call(
        total_kernel, (own.shape, BF16),
        own_first, from_left_first, from_right_first,
        own_last, from_left_last, from_right_last,
        flops=10**6,
    )


def on_device(
    mixer_input,
    step_shift,
    log_step,
    decay_real,
    freq_imag,
    in_real,
    in_imag,
    out_real,
    out_imag,
    skip_gain,
    out_weight,
    residual,
    post_gain,
    pre_gain,
    final_gain,
    route_ids,
    route_logits,
    expert_gate,
    expert_up,
    expert_down,
):
    devices, quarters = (lax.axis_size("sp"), lax.axis_size("tp"))
    rows, width = residual.shape
    length, wide = (mixer_input.shape[0], decay_real.size)
    channels = mixer_input.shape[1]
    slots = 2 * devices
    message, rates, read, cum_real, cum_imag, own_real, own_imag = call(
        mixer_kernel,
        [
            ((devices, *MESSAGE), BF16),
            ((8, wide), F32),
            ((2 * wide, 2 * channels), BF16),
            ((length, wide), F32),
            ((length, wide), F32),
            ((length, wide), F32),
            ((length, wide), F32),
        ],
        *map(
            in_hbm,
            (
                step_shift.T,
                mixer_input,
                log_step[None],
                decay_real,
                freq_imag,
                jnp.swapaxes(in_real, 1, 2),
                jnp.swapaxes(in_imag, 1, 2),
                out_real,
                out_imag,
            ),
        ),
        flops=10**9,
    )
    got = across_sp(message)
    kept, *sent = call(
        carry_kernel,
        [
            ((rows, width), F32),
            *(((rows, width), BF16),) * (quarters - 1),
        ],
        got, rates, read, cum_real, cum_imag, own_real, own_imag,
        mixer_input,
        skip_gain[None],
        out_weight,
        flops=10**9,
    )
    place, weigh = call(
        route_kernel,
        [((4 * slots, slots), BF16), ((3 * slots, 4 * slots), BF16)],
        route_ids.T,
        route_logits.T,
        flops=10**8,
    )
    stream, outgoing = call(
        project_kernel,
        [((rows, width), BF16), ((4 * slots, width // 4), BF16)],
        kept,
        *(shifted(part, by) for by, part in enumerate(sent, 1)),
        residual,
        post_gain[None],
        pre_gain[None],
        place,
        flops=10**9,
    )
    pieces = (devices, 4 * slots // devices, width // 4)
    arrived = across_sp(outgoing.reshape(pieces))
    summed = run_expert((expert_gate, expert_up, expert_down), arrived.reshape(outgoing.shape))
    results = across_sp(summed.reshape(pieces))
    return call(
        combine_kernel, ((rows, width), BF16),
        results.reshape(outgoing.shape), weigh, stream, final_gain[None], flops=10**9,
    )


def solution(mesh):
    in_specs = (
        P("sp", "tp"),
        P("sp", "tp"),
        P("tp"),
        P("tp", None),
        P("tp", None),
        P("tp", None, None),
        P("tp", None, None),
        P("tp", None, None),
        P("tp", None, None),
        P("tp"),
        P("tp", None),
        P(("sp", "tp"), None),
        P(),
        P(),
        P(),
        P("sp", None),
        P("sp", None),
        P("sp", None, "tp"),
        P("sp", None, "tp"),
        P("sp", "tp", None),
    )
    out_specs = P(("sp", "tp"), None)

    return jax.shard_map(
        on_device, mesh=mesh, in_specs=in_specs, out_specs=out_specs, check_vma=False
    )
```

```python
import jax
import jax.numpy as jnp
from jax import lax
from jax.experimental import pallas as pl
from jax.experimental.pallas import tpu as pltpu
from jax.sharding import PartitionSpec as P


F32 = jnp.float32
BF16 = jnp.bfloat16
EPS = 1e-06
STEP_LIMIT = 300.0
MESSAGE = (2, 640)


def dot(first, second, over=(1, 0)):
    dims = (((over[0],), (over[1],)), ((), ()))
    return lax.dot_general(first, second, dims, preferred_element_type=F32)


def iota(shape, dim):
    return lax.broadcasted_iota(jnp.int32, shape, dim)


def ones_where(mask, dtype=F32):
    return jnp.where(mask, 1.0, 0.0).astype(dtype)


def sine_cosine(angle):
    quarter = jnp.floor(angle * 0.6366197723675814 + 0.5)
    rest = angle - quarter * 1.5703125
    rest = rest - quarter * 0.0004825592041015625
    rest = rest - quarter * 1.26759079e-06
    square = rest * rest
    sine = ((-1.9515295891e-4 * square + 8.3321608736e-3) * square - 1.6666654611e-1) * square
    sine = sine * rest + rest
    cosine = (2.443315711809948e-5 * square - 1.388731625493765e-3) * square
    cosine = (cosine + 4.166664568298827e-2) * square * square - 0.5 * square + 1.0
    turn = quarter.astype(jnp.int32)
    odd = (turn & 1) == 1
    first, second = (jnp.where(odd, cosine, sine), jnp.where(odd, sine, cosine))
    return (
        jnp.where((turn & 2) == 2, -first, first),
        jnp.where(((turn + 1) & 2) == 2, -second, second),
    )


def rotation(decay, freq, step):
    sine, cosine = sine_cosine(freq * step)
    magnitude = jnp.exp(decay * step)
    return (magnitude * cosine, magnitude * sine)


def delayed(values, by, fill):
    if by >= 8:
        head = jnp.full((by, values.shape[1]), fill, F32)
        return jnp.concatenate([head, values[: values.shape[0] - by]], axis=0)
    return jnp.where(iota(values.shape, 0) >= by, pltpu.roll(values, by, 0), fill)


def split(values, count):
    found = []
    for _ in range(count):
        found.append(values.astype(BF16))
        values = values - found[-1].astype(F32)
    return found


def repeated(values, width):
    pair = jnp.concatenate([values, values], axis=1)
    return jnp.concatenate([pair] * (width // pair.shape[1]), axis=1)


def read_out(state_real, state_imag, read):
    high, low = split(jnp.concatenate([state_real, state_imag], axis=1), 2)
    both = dot(jnp.concatenate([high, low], axis=0), read[...])
    rows, cut = (state_real.shape[0], both.shape[1] // 2)
    return (both[:rows, :cut] + both[:rows, cut:]) + (both[rows:, :cut] + both[rows:, cut:])


def mixer_kernel(
    shift, inputs, log_step, decay_real, freq_imag, in_real, in_imag, out_real, out_imag,
    message, rates, read, cum_real, cum_imag, own_real, own_imag,
):
    groups, length = shift.shape
    states = decay_real.shape[1]
    channels = in_real.shape[1]
    width = groups * states
    own = iota((groups, width), 1) // states == iota((groups, width), 0)
    square = (groups, groups)
    log_column = jnp.sum(
        jnp.where(iota(square, 0) == iota(square, 1), log_step[...], 0.0), axis=1, keepdims=True
    )
    small_step = jnp.minimum(jnp.exp(log_column + shift[...]), STEP_LIMIT)
    step = dot(jnp.concatenate(split(small_step.T, 3), axis=0), ones_where(own, BF16))
    step = (step[:length] + step[length : 2 * length]) + step[2 * length :]

    def row(ref):
        return jnp.sum(jnp.where(own, repeated(ref[...], width), 0.0), axis=0, keepdims=True)

    decay, freq = (row(decay_real), row(freq_imag))
    rates[...] = jnp.concatenate([decay, freq, jnp.zeros((6, width), F32)], axis=0)
    wide = (groups * channels, width)
    block = iota(wide, 0) // channels == iota(wide, 1) // states
    values = inputs[...]
    doubled = jnp.concatenate([values, values], axis=1)

    def driven(ref):
        spread = jnp.where(block, repeated(ref[...].reshape(wide[0], states), width), 0.0)
        return dot(doubled, jnp.concatenate(split(spread, 2), axis=0))

    into_real, into_imag = (driven(in_real), driven(in_imag))
    tall = (width, wide[0])
    block = iota(tall, 0) // states == iota(tall, 1) // channels

    def reading(ref):
        turned = ref[...].reshape(wide[0], states).T
        return jnp.where(block, jnp.concatenate([turned] * groups, axis=0), 0.0)

    read[...] = jnp.concatenate(
        split(jnp.concatenate([reading(out_real), -reading(out_imag)], axis=0), 2), axis=1
    )
    inverse = 1.0 / (decay * decay + freq * freq)
    last_real, last_imag = ([], [])
    for start in range(0, width, 128):
        cut = slice(start, start + 128)
        a_real, a_imag = rotation(decay[:, cut], freq[:, cut], step[:, cut])
        minus_one = a_real - 1.0
        coef_real = (minus_one * decay[:, cut] + a_imag * freq[:, cut]) * inverse[:, cut]
        coef_imag = (a_imag * decay[:, cut] - minus_one * freq[:, cut]) * inverse[:, cut]
        s_real = coef_real * into_real[:, cut] - coef_imag * into_imag[:, cut]
        s_imag = coef_real * into_imag[:, cut] + coef_imag * into_real[:, cut]
        by = 1
        while by < length:
            p_real, p_imag = (delayed(s_real, by, 0.0), delayed(s_imag, by, 0.0))
            b_real, b_imag = (delayed(a_real, by, 1.0), delayed(a_imag, by, 0.0))
            s_real, s_imag = (
                s_real + a_real * p_real - a_imag * p_imag,
                s_imag + a_real * p_imag + a_imag * p_real,
            )
            a_real, a_imag = (a_real * b_real - a_imag * b_imag, a_real * b_imag + a_imag * b_real)
            by *= 2
        cum_real[:, cut] = a_real
        cum_imag[:, cut] = a_imag
        own_real[:, cut] = s_real
        own_imag[:, cut] = s_imag
        last_real.append(s_real[length - 1 :])
        last_imag.append(s_imag[length - 1 :])
    lanes = MESSAGE[1] - width
    pick = (width, lanes)
    compress = ones_where(
        (iota(pick, 0) == (iota(pick, 1) % groups) * states) & (iota(pick, 1) < 3 * groups), BF16
    )
    total = jnp.concatenate(split(jnp.sum(step, axis=0, keepdims=True), 3), axis=0)
    first, second, third = [part[None] for part in dot(total, compress)]
    lane = iota(first.shape, 1)
    total = jnp.where(lane < groups, first, jnp.where(lane < 2 * groups, second, third))
    lines = [
        jnp.concatenate([*part, rest], axis=1)
        for part, rest in ((last_real, total), (last_imag, jnp.zeros_like(total)))
    ]
    sent = jnp.concatenate(lines, axis=0)
    message[...] = jnp.broadcast_to(sent[None], message.shape).astype(BF16)


def carry_kernel(
    got, rates, read, cum_real, cum_imag, own_real, own_imag, inputs, skip, out_weight,
    kept, sent_1, sent_2, sent_3,
):
    devices = got.shape[0]
    width = rates.shape[1]
    lanes = MESSAGE[1] - width
    groups = 8
    states = width // groups
    mine = lax.axis_index("sp")
    decay, freq = (rates[0:1, :], rates[1:2, :])
    everything = got[...].astype(F32)
    got_real, got_imag = (everything[:, 0, :width], everything[:, 1, :width])
    totals = everything[:, 0, width:]
    square = (devices, devices)
    between = (iota(square, 0) < iota(square, 1)) & (iota(square, 1) < mine)
    sums = dot(ones_where(between, BF16), totals.astype(BF16))
    wide = (lanes, width)
    spread = ones_where(
        (iota(wide, 0) < 3 * groups) & (iota(wide, 0) % groups == iota(wide, 1) // states), BF16
    )
    elapsed = dot(jnp.concatenate(split(sums, 3), axis=0), spread)
    elapsed = (elapsed[:devices] + elapsed[devices : 2 * devices]) + elapsed[2 * devices :]
    elapsed = jnp.minimum(elapsed, STEP_LIMIT)
    weight_real, weight_imag = rotation(decay, freq, elapsed)
    earlier = iota((devices, width), 0) < mine
    weight_real = jnp.where(earlier, weight_real, 0.0)
    weight_imag = jnp.where(earlier, weight_imag, 0.0)
    carry_real = jnp.sum(weight_real * got_real - weight_imag * got_imag, axis=0, keepdims=True)
    carry_imag = jnp.sum(weight_real * got_imag + weight_imag * got_real, axis=0, keepdims=True)
    c_real, c_imag = (cum_real[...], cum_imag[...])
    result = skip[...] * inputs[...].astype(F32) + read_out(
        own_real[...] + (c_real * carry_real - c_imag * carry_imag),
        own_imag[...] + (c_real * carry_imag + c_imag * carry_real),
        read,
    )
    mixed = jax.nn.gelu(result)
    rows, length = (kept.shape[0], mixed.shape[0])
    ahead = lax.rem(length - lax.axis_index("tp") * rows, length)
    partial = dot(pltpu.roll(mixed, ahead, 0).astype(BF16), out_weight[...])
    kept[...] = partial[:rows]
    for by, sent in enumerate((sent_1, sent_2, sent_3), 1):
        sent[...] = partial[by * rows : (by + 1) * rows].astype(BF16)


def route_kernel(ids, logits, place, weigh):
    slots = ids.shape[1]
    tall = (slots, slots)
    rows = slots // 4
    member, lane = (iota(tall, 0) % rows, iota(tall, 1))
    here = lane == lax.axis_index("tp") * rows + member

    def column(line):
        return jnp.sum(jnp.where(here, line, 0.0), axis=1, keepdims=True)

    named = ids[...].astype(F32)
    expert = (lane // 2).astype(F32)
    is_first = ones_where(column(named[0:1]) == expert)
    is_second = ones_where(column(named[1:2]) == expert)
    before = ones_where((lane % rows < member) & (lane // rows == iota(tall, 0) // rows), BF16)
    count = dot(before, (is_first + is_second).astype(BF16))
    kept = ones_where(count == (lane % 2).astype(F32))
    first = jax.nn.sigmoid(column(logits[0:1, :]) - column(logits[1:2, :]))
    long = (slots * 4, slots)
    repeat = ones_where(iota(long, 0) // 4 == iota(long, 1), BF16)
    put = dot(repeat, ((is_first + is_second) * kept).astype(BF16), (1, 1))
    place[...] = jnp.where(iota(long, 0) % 4 == iota(long, 1) // rows, put, 0.0).astype(BF16)
    weight = (is_first * first + is_second * (1.0 - first)) * kept
    back = (slots, slots * 4)
    repeat = ones_where(iota(back, 1) // 4 == iota(back, 0), BF16)
    took = dot(jnp.concatenate(split(weight, 3), axis=0), repeat)
    fits = iota(took.shape, 1) % 4 == (iota(took.shape, 0) % slots) // rows
    weigh[...] = jnp.where(fits, took, 0.0).astype(BF16)


def normalized(values, gain):
    return values * lax.rsqrt(jnp.mean(values * values, axis=-1, keepdims=True) + EPS) * gain


def project_kernel(
    kept, got_1, got_2, got_3, residual, post_gain, pre_gain, place, stream, outgoing
):
    width = residual.shape[1]
    projected = kept[...] + sum(got[...].astype(F32) for got in (got_1, got_2, got_3))
    own = (residual[...].astype(F32) + normalized(projected, post_gain[...])).astype(BF16)
    stream[...] = own
    normed = normalized(own.astype(F32), pre_gain[...]).astype(BF16)
    cut = width // 4
    stacked = jnp.concatenate([normed[:, q * cut : (q + 1) * cut] for q in range(4)], axis=0)
    outgoing[...] = dot(place[...], stacked).astype(BF16)


def hidden_rows(halves, gate, up, arrived=None):
    count = len(halves) // 2
    lines, cut = (2 * halves[0].shape[0], halves[0].shape[1])
    slots = lines // 4
    square = (lines, lines)
    by_quarter = ones_where(
        iota(square, 1) == (iota(square, 0) % slots) * 4 + iota(square, 0) // slots, BF16
    )
    parts = []
    for k in range(count):
        rows = jnp.concatenate([halves[2 * k][...], halves[2 * k + 1][...]], axis=0)
        rows = dot(by_quarter, rows).astype(BF16)
        parts.append([rows[q * slots : (q + 1) * slots] for q in range(4)])
    parts = [jnp.concatenate(part, axis=0) for part in zip(*parts)]
    if arrived is None:
        whole = jnp.concatenate(parts, axis=1)
        gate_hidden, up_hidden = (dot(whole, gate[0]), dot(whole, up[0]))
    else:
        gate_hidden = up_hidden = 0.0
        for q, part in enumerate(parts):
            span = slice(q * cut, (q + 1) * cut)
            arrived(0, q)
            gate_hidden = gate_hidden + dot(part, gate[0, span, :])
            arrived(1, q)
            up_hidden = up_hidden + dot(part, up[0, span, :])
    return (jax.nn.silu(gate_hidden) * up_hidden).astype(BF16)


def down_rows(active, down, results, arrived=None):
    lines, cut = (2 * results[0].shape[0], results[0].shape[1])
    slots = lines // 4
    square = (lines, lines)
    made = []
    for q in range(4):
        if arrived is not None:
            arrived(q)
        made.append(dot(active, down[0, :, q * cut : (q + 1) * cut]).astype(BF16))
    in_lines = ones_where(
        iota(square, 1) == (iota(square, 0) % 4) * slots + iota(square, 0) // 4, BF16
    )
    for k in range(len(results) // 2):
        stacked = jnp.concatenate([m[k * slots : (k + 1) * slots] for m in made], axis=0)
        product = dot(in_lines, stacked).astype(BF16)
        results[2 * k][...] = product[: lines // 2]
        results[2 * k + 1][...] = product[lines // 2 :]


def own_rows_kernel(first, last, gate, up, active, gate_held, up_held, semaphores):
    cut = first.shape[1]

    def fetch(which, q):
        source, held = ((gate, gate_held), (up, up_held))[which]
        place = (0, pl.ds(q * cut, cut), slice(None))
        return pltpu.make_async_copy(
            source.at[place], held.at[place], semaphores.at[which * 4 + q]
        )

    for q in range(4):
        fetch(0, q).start()
        fetch(1, q).start()
    active[...] = hidden_rows(
        (first, last), gate_held, up_held, lambda which, q: fetch(which, q).wait()
    )


def near_rows_kernel(
    first, last, own_active, gate, up, down, made_first, made_last, own_first, own_last, down_held,
    semaphores,
):
    cut = first.shape[1]

    def fetch(q):
        place = (0, slice(None), pl.ds(q * cut, cut))
        return pltpu.make_async_copy(down.at[place], down_held.at[place], semaphores.at[q])

    for q in range(4):
        fetch(q).start()
    active = jnp.concatenate([hidden_rows((first, last), gate, up), own_active[...]], axis=0)
    down_rows(
        active, down_held, (made_first, made_last, own_first, own_last), lambda q: fetch(q).wait()
    )


def other_rows_kernel(first, last, gate, up, down, made_first, made_last):
    down_rows(hidden_rows((first, last), gate, up), down, (made_first, made_last))


def total_kernel(*refs):
    *parts, out = refs
    half = out.shape[0] // 2
    for side in range(2):
        chosen = parts[3 * side : 3 * side + 3]
        out[side * half : (side + 1) * half, :] = sum(p[...].astype(F32) for p in chosen).astype(BF16)


def combine_kernel(results, weigh, stream, final_gain, out):
    rows = stream.shape[0]
    mixture = dot(weigh[...], results[...])
    height = mixture.shape[0] // 3
    mixture = (mixture[:height] + mixture[height : 2 * height]) + mixture[2 * height :]
    mixture = jnp.concatenate([mixture[q * rows : (q + 1) * rows] for q in range(4)], axis=1)
    out[...] = (stream[...].astype(F32) + normalized(mixture, final_gain[...])).astype(BF16)


def call(kernel, outs, *args, flops=0, in_place=(), scratch=()):
    whole = pl.BlockSpec(memory_space=pltpu.VMEM)
    left = pl.BlockSpec(memory_space=pl.ANY)
    single = not isinstance(outs, list)
    shapes = [
        jax.ShapeDtypeStruct(*out) if isinstance(out, tuple) else out
        for out in ([outs] if single else outs)
    ]
    made = pl.pallas_call(
        kernel,
        out_shape=shapes,
        in_specs=[left if k in in_place else whole for k in range(len(args))],
        out_specs=[whole] * len(shapes),
        scratch_shapes=list(scratch),
        cost_estimate=pl.CostEstimate(flops=flops, bytes_accessed=0, transcendentals=0),
        compiler_params=pltpu.CompilerParams(vmem_limit_bytes=VMEM_LIMIT),
    )(*args)
    return made[0] if single else made


VMEM_LIMIT = 24 * 2**20


def in_hbm(value):
    return pltpu.with_memory_space_constraint(value, pltpu.HBM)


def across_sp(pieces):
    return lax.all_to_all(pieces, "sp", split_axis=0, concat_axis=0, tiled=True)


def shifted(part, by):
    size = lax.axis_size("tp")
    return lax.ppermute(part, "tp", [(i, (i + by) % size) for i in range(size)])


def added(first, second):
    return (first.astype(F32) + second.astype(F32)).astype(BF16)


def run_expert(weights, own):
    lines, cut = own.shape
    half = (lines // 2, cut)
    work = 2 * (lines // 4) * 3 * weights[0].shape[1] * weights[0].shape[2]
    first, last = (own[: half[0]], own[half[0] :])
    left_first, right_last = (shifted(first, 1), shifted(last, -1))
    left_last, right_first = (shifted(last, 1), shifted(first, -1))
    across_first, across_last = (shifted(left_first, 1), shifted(right_last, -1))
    gate, up, down = weights
    active, gate_held, up_held = call(
        own_rows_kernel,
        [((lines // 4, gate.shape[2]), BF16), (gate.shape, BF16), (up.shape, BF16)],
        first,
        last,
        in_hbm(gate),
        in_hbm(up),
        flops=work * 2 // 3,
        in_place=(2, 3),
        scratch=[pltpu.SemaphoreType.DMA((8,))],
    )
    to_left_first, to_right_last, own_first, own_last, down_held = call(
        near_rows_kernel,
        [*((half, BF16),) * 4, (down.shape, BF16)],
        left_first,
        right_last,
        active,
        gate_held,
        up_held,
        in_hbm(down),
        flops=work * 4 // 3,
        in_place=(5,),
        scratch=[pltpu.SemaphoreType.DMA((4,))],
    )

    def part(*halves):
        return call(
            other_rows_kernel, [(half, BF16)] * 2,
            *halves, gate_held, up_held, down_held, flops=work,
        )

    from_left_last, from_right_first = (shifted(to_right_last, 1), shifted(to_left_first, -1))
    to_left_last, to_right_first = part(left_last, right_first)
    far_first, far_last = part(across_first, across_last)
    to_right_first = added(to_right_first, shifted(far_first, 1))
    to_left_last = added(to_left_last, shifted(far_last, -1))
    from_left_first, from_right_last = (shifted(to_right_first, 1), shifted(to_left_last, -1))

    return call(
        total_kernel, (own.shape, BF16),
        own_first, from_left_first, from_right_first,
        own_last, from_left_last, from_right_last,
        flops=10**6,
    )


def on_device(
    mixer_input,
    step_shift,
    log_step,
    decay_real,
    freq_imag,
    in_real,
    in_imag,
    out_real,
    out_imag,
    skip_gain,
    out_weight,
    residual,
    post_gain,
    pre_gain,
    final_gain,
    route_ids,
    route_logits,
    expert_gate,
    expert_up,
    expert_down,
):
    devices, quarters = (lax.axis_size("sp"), lax.axis_size("tp"))
    rows, width = residual.shape
    length, wide = (mixer_input.shape[0], decay_real.size)
    channels = mixer_input.shape[1]
    slots = 2 * devices
    message, rates, read, cum_real, cum_imag, own_real, own_imag = call(
        mixer_kernel,
        [
            ((devices, *MESSAGE), BF16),
            ((8, wide), F32),
            ((2 * wide, 2 * channels), BF16),
            ((length, wide), F32),
            ((length, wide), F32),
            ((length, wide), F32),
            ((length, wide), F32),
        ],
        *map(
            in_hbm,
            (
                step_shift.T,
                mixer_input,
                log_step[None],
                decay_real,
                freq_imag,
                jnp.swapaxes(in_real, 1, 2),
                jnp.swapaxes(in_imag, 1, 2),
                out_real,
                out_imag,
            ),
        ),
        flops=10**9,
    )
    got = across_sp(message)
    kept, *sent = call(
        carry_kernel,
        [
            ((rows, width), F32),
            *(((rows, width), BF16),) * (quarters - 1),
        ],
        got, rates, read, cum_real, cum_imag, own_real, own_imag,
        mixer_input,
        skip_gain[None],
        out_weight,
        flops=10**9,
    )
    place, weigh = call(
        route_kernel,
        [((4 * slots, slots), BF16), ((3 * slots, 4 * slots), BF16)],
        route_ids.T,
        route_logits.T,
        flops=10**8,
    )
    stream, outgoing = call(
        project_kernel,
        [((rows, width), BF16), ((4 * slots, width // 4), BF16)],
        kept,
        *(shifted(part, by) for by, part in enumerate(sent, 1)),
        residual,
        post_gain[None],
        pre_gain[None],
        place,
        flops=10**9,
    )
    pieces = (devices, 4 * slots // devices, width // 4)
    arrived = across_sp(outgoing.reshape(pieces))
    summed = run_expert((expert_gate, expert_up, expert_down), arrived.reshape(outgoing.shape))
    results = across_sp(summed.reshape(pieces))
    return call(
        combine_kernel, ((rows, width), BF16),
        results.reshape(outgoing.shape), weigh, stream, final_gain[None], flops=10**9,
    )


def solution(mesh):
    in_specs = (
        P("sp", "tp"),
        P("sp", "tp"),
        P("tp"),
        P("tp", None),
        P("tp", None),
        P("tp", None, None),
        P("tp", None, None),
        P("tp", None, None),
        P("tp", None, None),
        P("tp"),
        P("tp", None),
        P(("sp", "tp"), None),
        P(),
        P(),
        P(),
        P("sp", None),
        P("sp", None),
        P("sp", None, "tp"),
        P("sp", None, "tp"),
        P("sp", "tp", None),
    )
    out_specs = P(("sp", "tp"), None)

    return jax.shard_map(
        on_device, mesh=mesh, in_specs=in_specs, out_specs=out_specs, check_vma=False
    )
```

```python
import jax
import jax.numpy as jnp
from jax import lax
from jax.experimental import pallas as pl
from jax.experimental.pallas import tpu as pltpu
from jax.sharding import PartitionSpec as P


F32 = jnp.float32
BF16 = jnp.bfloat16
EPS = 1e-06
STEP_LIMIT = 300.0
MESSAGE = (2, 640)


def dot(first, second, over=(1, 0)):
    dims = (((over[0],), (over[1],)), ((), ()))
    return lax.dot_general(first, second, dims, preferred_element_type=F32)


def iota(shape, dim):
    return lax.broadcasted_iota(jnp.int32, shape, dim)


def ones_where(mask, dtype=F32):
    return jnp.where(mask, 1.0, 0.0).astype(dtype)


def sine_cosine(angle):
    quarter = jnp.floor(angle * 0.6366197723675814 + 0.5)
    rest = angle - quarter * 1.5703125
    rest = rest - quarter * 0.0004825592041015625
    rest = rest - quarter * 1.26759079e-06
    square = rest * rest
    sine = ((-1.9515295891e-4 * square + 8.3321608736e-3) * square - 1.6666654611e-1) * square
    sine = sine * rest + rest
    cosine = (2.443315711809948e-5 * square - 1.388731625493765e-3) * square
    cosine = (cosine + 4.166664568298827e-2) * square * square - 0.5 * square + 1.0
    turn = quarter.astype(jnp.int32)
    odd = (turn & 1) == 1
    first, second = (jnp.where(odd, cosine, sine), jnp.where(odd, sine, cosine))
    return (
        jnp.where((turn & 2) == 2, -first, first),
        jnp.where(((turn + 1) & 2) == 2, -second, second),
    )


def rotation(decay, freq, step):
    sine, cosine = sine_cosine(freq * step)
    magnitude = jnp.exp(decay * step)
    return (magnitude * cosine, magnitude * sine)


def delayed(values, by, fill):
    return jnp.where(iota(values.shape, 0) >= by, pltpu.roll(values, by, 0), fill)


def split(values, count):
    found = []
    for _ in range(count):
        found.append(values.astype(BF16))
        values = values - found[-1].astype(F32)
    return found


def repeated(values, width):
    pair = jnp.concatenate([values, values], axis=1)
    return jnp.concatenate([pair] * (width // pair.shape[1]), axis=1)


def read_out(state_real, state_imag, read):
    high, low = split(jnp.concatenate([state_real, state_imag], axis=1), 2)
    both = dot(jnp.concatenate([high, low], axis=0), read[...])
    rows, cut = (state_real.shape[0], both.shape[1] // 2)
    return (both[:rows, :cut] + both[:rows, cut:]) + (both[rows:, :cut] + both[rows:, cut:])


def mixer_kernel(
    shift, inputs, log_step, decay_real, freq_imag, in_real, in_imag, out_real, out_imag,
    message, rates, read, cum_real, cum_imag, own_real, own_imag,
):
    groups, length = shift.shape
    states = decay_real.shape[1]
    channels = in_real.shape[1]
    width = groups * states
    own = iota((groups, width), 1) // states == iota((groups, width), 0)
    square = (groups, groups)
    log_column = jnp.sum(
        jnp.where(iota(square, 0) == iota(square, 1), log_step[...], 0.0), axis=1, keepdims=True
    )
    small_step = jnp.minimum(jnp.exp(log_column + shift[...]), STEP_LIMIT)
    step = dot(jnp.concatenate(split(small_step.T, 3), axis=0), ones_where(own, BF16))
    step = (step[:length] + step[length : 2 * length]) + step[2 * length :]

    def row(ref):
        return jnp.sum(jnp.where(own, repeated(ref[...], width), 0.0), axis=0, keepdims=True)

    decay, freq = (row(decay_real), row(freq_imag))
    rates[...] = jnp.concatenate([decay, freq, jnp.zeros((6, width), F32)], axis=0)
    wide = (groups * channels, width)
    block = iota(wide, 0) // channels == iota(wide, 1) // states
    values = inputs[...]
    doubled = jnp.concatenate([values, values], axis=1)

    def driven(ref):
        spread = jnp.where(block, repeated(ref[...].reshape(wide[0], states), width), 0.0)
        return dot(doubled, jnp.concatenate(split(spread, 2), axis=0))

    into_real, into_imag = (driven(in_real), driven(in_imag))
    tall = (width, wide[0])
    block = iota(tall, 0) // states == iota(tall, 1) // channels

    def reading(ref):
        turned = ref[...].reshape(wide[0], states).T
        return jnp.where(block, jnp.concatenate([turned] * groups, axis=0), 0.0)

    read[...] = jnp.concatenate(
        split(jnp.concatenate([reading(out_real), -reading(out_imag)], axis=0), 2), axis=1
    )
    inverse = 1.0 / (decay * decay + freq * freq)
    last_real, last_imag = ([], [])
    for start in range(0, width, 128):
        cut = slice(start, start + 128)
        a_real, a_imag = rotation(decay[:, cut], freq[:, cut], step[:, cut])
        minus_one = a_real - 1.0
        coef_real = (minus_one * decay[:, cut] + a_imag * freq[:, cut]) * inverse[:, cut]
        coef_imag = (a_imag * decay[:, cut] - minus_one * freq[:, cut]) * inverse[:, cut]
        s_real = coef_real * into_real[:, cut] - coef_imag * into_imag[:, cut]
        s_imag = coef_real * into_imag[:, cut] + coef_imag * into_real[:, cut]
        by = 1
        while by < length:
            keep = by if by >= 8 else 0
            whole = (s_real, s_imag, a_real, a_imag)
            s_real, s_imag, a_real, a_imag = (part[keep:] for part in whole)
            if keep:
                p_real, p_imag, b_real, b_imag = (part[: length - by] for part in whole)
            else:
                p_real, p_imag = (delayed(s_real, by, 0.0), delayed(s_imag, by, 0.0))
                b_real, b_imag = (delayed(a_real, by, 1.0), delayed(a_imag, by, 0.0))
            s_real, s_imag, a_real, a_imag = (
                s_real + a_real * p_real - a_imag * p_imag,
                s_imag + a_real * p_imag + a_imag * p_real,
                a_real * b_real - a_imag * b_imag,
                a_real * b_imag + a_imag * b_real,
            )
            if keep:
                s_real, s_imag, a_real, a_imag = (
                    jnp.concatenate([before[:keep], after], axis=0)
                    for before, after in zip(whole, (s_real, s_imag, a_real, a_imag))
                )
            by *= 2
        cum_real[:, cut] = a_real
        cum_imag[:, cut] = a_imag
        own_real[:, cut] = s_real
        own_imag[:, cut] = s_imag
        last_real.append(s_real[length - 1 :])
        last_imag.append(s_imag[length - 1 :])
    lanes = MESSAGE[1] - width
    pick = (width, lanes)
    compress = ones_where(
        (iota(pick, 0) == (iota(pick, 1) % groups) * states) & (iota(pick, 1) < 3 * groups), BF16
    )
    total = jnp.concatenate(split(jnp.sum(step, axis=0, keepdims=True), 3), axis=0)
    first, second, third = [part[None] for part in dot(total, compress)]
    lane = iota(first.shape, 1)
    total = jnp.where(lane < groups, first, jnp.where(lane < 2 * groups, second, third))
    lines = [
        jnp.concatenate([*part, rest], axis=1)
        for part, rest in ((last_real, total), (last_imag, jnp.zeros_like(total)))
    ]
    sent = jnp.concatenate(lines, axis=0)
    message[...] = jnp.broadcast_to(sent[None], message.shape).astype(BF16)


def carry_kernel(
    got, rates, read, cum_real, cum_imag, own_real, own_imag, inputs, skip, out_weight,
    kept, sent_1, sent_2, sent_3,
):
    devices = got.shape[0]
    width = rates.shape[1]
    lanes = MESSAGE[1] - width
    groups = 8
    states = width // groups
    mine = lax.axis_index("sp")
    decay, freq = (rates[0:1, :], rates[1:2, :])
    everything = got[...].astype(F32)
    got_real, got_imag = (everything[:, 0, :width], everything[:, 1, :width])
    totals = everything[:, 0, width:]
    square = (devices, devices)
    between = (iota(square, 0) < iota(square, 1)) & (iota(square, 1) < mine)
    sums = dot(ones_where(between, BF16), totals.astype(BF16))
    wide = (lanes, width)
    spread = ones_where(
        (iota(wide, 0) < 3 * groups) & (iota(wide, 0) % groups == iota(wide, 1) // states), BF16
    )
    elapsed = dot(jnp.concatenate(split(sums, 3), axis=0), spread)
    elapsed = (elapsed[:devices] + elapsed[devices : 2 * devices]) + elapsed[2 * devices :]
    elapsed = jnp.minimum(elapsed, STEP_LIMIT)
    weight_real, weight_imag = rotation(decay, freq, elapsed)
    earlier = iota((devices, width), 0) < mine
    weight_real = jnp.where(earlier, weight_real, 0.0)
    weight_imag = jnp.where(earlier, weight_imag, 0.0)
    carry_real = jnp.sum(weight_real * got_real - weight_imag * got_imag, axis=0, keepdims=True)
    carry_imag = jnp.sum(weight_real * got_imag + weight_imag * got_real, axis=0, keepdims=True)
    c_real, c_imag = (cum_real[...], cum_imag[...])
    result = skip[...] * inputs[...].astype(F32) + read_out(
        own_real[...] + (c_real * carry_real - c_imag * carry_imag),
        own_imag[...] + (c_real * carry_imag + c_imag * carry_real),
        read,
    )
    mixed = jax.nn.gelu(result)
    rows, length = (kept.shape[0], mixed.shape[0])
    ahead = lax.rem(length - lax.axis_index("tp") * rows, length)
    partial = dot(pltpu.roll(mixed, ahead, 0).astype(BF16), out_weight[...])
    kept[...] = partial[:rows]
    for by, sent in enumerate((sent_1, sent_2, sent_3), 1):
        sent[...] = partial[by * rows : (by + 1) * rows].astype(BF16)


def route_kernel(ids, logits, place, weigh):
    slots = ids.shape[1]
    tall = (slots, slots)
    rows = slots // 4
    member, lane = (iota(tall, 0) % rows, iota(tall, 1))
    here = lane == lax.axis_index("tp") * rows + member

    def column(line):
        return jnp.sum(jnp.where(here, line, 0.0), axis=1, keepdims=True)

    named = ids[...].astype(F32)
    expert = (lane // 2).astype(F32)
    is_first = ones_where(column(named[0:1]) == expert)
    is_second = ones_where(column(named[1:2]) == expert)
    before = ones_where((lane % rows < member) & (lane // rows == iota(tall, 0) // rows), BF16)
    count = dot(before, (is_first + is_second).astype(BF16))
    kept = ones_where(count == (lane % 2).astype(F32))
    first = jax.nn.sigmoid(column(logits[0:1, :]) - column(logits[1:2, :]))
    long = (slots * 4, slots)
    repeat = ones_where(iota(long, 0) // 4 == iota(long, 1), BF16)
    put = dot(repeat, ((is_first + is_second) * kept).astype(BF16), (1, 1))
    place[...] = jnp.where(iota(long, 0) % 4 == iota(long, 1) // rows, put, 0.0).astype(BF16)
    weight = (is_first * first + is_second * (1.0 - first)) * kept
    back = (slots, slots * 4)
    repeat = ones_where(iota(back, 1) // 4 == iota(back, 0), BF16)
    took = dot(jnp.concatenate(split(weight, 2), axis=0), repeat)
    fits = iota(took.shape, 1) % 4 == (iota(took.shape, 0) % slots) // rows
    weigh[...] = jnp.where(fits, took, 0.0).astype(BF16)


def normalized(values, gain):
    return values * lax.rsqrt(jnp.mean(values * values, axis=-1, keepdims=True) + EPS) * gain


def project_kernel(
    kept, got_1, got_2, got_3, residual, post_gain, pre_gain, place, stream, outgoing
):
    width = residual.shape[1]
    projected = kept[...] + sum(got[...].astype(F32) for got in (got_1, got_2, got_3))
    own = (residual[...].astype(F32) + normalized(projected, post_gain[...])).astype(BF16)
    stream[...] = own
    normed = normalized(own.astype(F32), pre_gain[...]).astype(BF16)
    cut = width // 4
    stacked = jnp.concatenate([normed[:, q * cut : (q + 1) * cut] for q in range(4)], axis=0)
    outgoing[...] = dot(place[...], stacked).astype(BF16)


def expert_kernel(halves, weights, results, arrived=None):
    gate, up, down = weights
    count = len(halves) // 2
    lines, cut = (2 * halves[0].shape[0], halves[0].shape[1])
    slots = lines // 4
    square = (lines, lines)
    by_quarter = ones_where(
        iota(square, 1) == (iota(square, 0) % slots) * 4 + iota(square, 0) // slots, BF16
    )
    parts = []
    for k in range(count):
        rows = jnp.concatenate([halves[2 * k][...], halves[2 * k + 1][...]], axis=0)
        rows = dot(by_quarter, rows).astype(BF16)
        parts.append([rows[q * slots : (q + 1) * slots] for q in range(4)])
    parts = [jnp.concatenate(part, axis=0) for part in zip(*parts)]
    if arrived is None:
        whole = jnp.concatenate(parts, axis=1)
        gate_hidden, up_hidden = (dot(whole, gate[0]), dot(whole, up[0]))
    else:
        gate_hidden = up_hidden = 0.0
        for q, part in enumerate(parts):
            span = slice(q * cut, (q + 1) * cut)
            arrived(0, q)
            gate_hidden = gate_hidden + dot(part, gate[0, span, :])
            arrived(1, q)
            up_hidden = up_hidden + dot(part, up[0, span, :])
    active = (jax.nn.silu(gate_hidden) * up_hidden).astype(BF16)
    made = []
    for q in range(4):
        if arrived is not None:
            arrived(2, q)
        made.append(dot(active, down[0, :, q * cut : (q + 1) * cut]).astype(BF16))
    in_lines = ones_where(
        iota(square, 1) == (iota(square, 0) % 4) * slots + iota(square, 0) // 4, BF16
    )
    for k in range(count):
        stacked = jnp.concatenate([m[k * slots : (k + 1) * slots] for m in made], axis=0)
        product = dot(in_lines, stacked).astype(BF16)
        results[2 * k][...] = product[: lines // 2]
        results[2 * k + 1][...] = product[lines // 2 :]


def own_rows_kernel(first, last, gate, up, down, made_first, made_last, *held):
    *weights, semaphores = held
    cut = first.shape[1]

    def fetch(which, q):
        source = (gate, up, down)[which]
        span = pl.ds(q * cut, cut)
        place = (0, slice(None), span) if which == 2 else (0, span, slice(None))
        return pltpu.make_async_copy(
            source.at[place], weights[which].at[place], semaphores.at[which * 4 + q]
        )

    for q in range(4):
        fetch(0, q).start()
        fetch(1, q).start()
    for q in range(4):
        fetch(2, q).start()
    expert_kernel(
        (first, last), weights, (made_first, made_last), lambda which, q: fetch(which, q).wait()
    )


def other_rows_kernel(count, *refs):
    expert_kernel(refs[:count], refs[count : count + 3], refs[count + 3 : 2 * count + 3])


def total_kernel(*refs):
    *parts, out = refs
    half = out.shape[0] // 2
    for side in range(2):
        chosen = parts[3 * side : 3 * side + 3]
        out[side * half : (side + 1) * half, :] = sum(p[...].astype(F32) for p in chosen).astype(BF16)


def combine_kernel(results, weigh, stream, final_gain, out):
    rows = stream.shape[0]
    mixture = dot(weigh[...], results[...])
    height = mixture.shape[0] // 2
    mixture = mixture[:height] + mixture[height:]
    mixture = jnp.concatenate([mixture[q * rows : (q + 1) * rows] for q in range(4)], axis=1)
    out[...] = (stream[...].astype(F32) + normalized(mixture, final_gain[...])).astype(BF16)


def call(kernel, outs, *args, flops=0, in_place=(), scratch=()):
    whole = pl.BlockSpec(memory_space=pltpu.VMEM)
    left = pl.BlockSpec(memory_space=pl.ANY)
    single = not isinstance(outs, list)
    shapes = [
        jax.ShapeDtypeStruct(*out) if isinstance(out, tuple) else out
        for out in ([outs] if single else outs)
    ]
    made = pl.pallas_call(
        kernel,
        out_shape=shapes,
        in_specs=[left if k in in_place else whole for k in range(len(args))],
        out_specs=[whole] * len(shapes),
        scratch_shapes=list(scratch),
        cost_estimate=pl.CostEstimate(flops=flops, bytes_accessed=0, transcendentals=0),
        compiler_params=pltpu.CompilerParams(vmem_limit_bytes=VMEM_LIMIT),
    )(*args)
    return made[0] if single else made


VMEM_LIMIT = 24 * 2**20


def in_hbm(value):
    return pltpu.with_memory_space_constraint(value, pltpu.HBM)


def across_sp(pieces):
    return lax.all_to_all(pieces, "sp", split_axis=0, concat_axis=0, tiled=True)


def shifted(part, by):
    size = lax.axis_size("tp")
    return lax.ppermute(part, "tp", [(i, (i + by) % size) for i in range(size)])


def added(first, second):
    return (first.astype(F32) + second.astype(F32)).astype(BF16)


def run_expert(weights, own):
    lines, cut = own.shape
    half = (lines // 2, cut)
    work = 2 * (lines // 4) * 3 * weights[0].shape[1] * weights[0].shape[2]
    first, last = (own[: half[0]], own[half[0] :])
    left_first, right_last = (shifted(first, 1), shifted(last, -1))
    left_last, right_first = (shifted(last, 1), shifted(first, -1))
    across_first, across_last = (shifted(left_first, 1), shifted(right_last, -1))
    own_first, own_last, *held = call(
        own_rows_kernel,
        [(half, BF16), (half, BF16), *(pltpu.VMEM(w.shape, w.dtype) for w in weights)],
        first,
        last,
        *(in_hbm(w) for w in weights),
        flops=work,
        in_place=(2, 3, 4),
        scratch=[pltpu.SemaphoreType.DMA((12,))],
    )

    def part(*halves):
        count = len(halves)
        return call(
            lambda *refs: other_rows_kernel(count, *refs), [(half, BF16)] * count,
            *halves, *held, flops=work * count // 2,
        )

    to_left_first, to_right_last = part(left_first, right_last)
    from_left_last, from_right_first = (shifted(to_right_last, 1), shifted(to_left_first, -1))
    to_left_last, to_right_first = part(left_last, right_first)
    far_first, far_last = part(across_first, across_last)
    to_right_first = added(to_right_first, shifted(far_first, 1))
    to_left_last = added(to_left_last, shifted(far_last, -1))
    from_left_first, from_right_last = (shifted(to_right_first, 1), shifted(to_left_last, -1))

    return call(
        total_kernel, (own.shape, BF16),
        own_first, from_left_first, from_right_first,
        own_last, from_left_last, from_right_last,
        flops=10**6,
    )


def on_device(
    mixer_input,
    step_shift,
    log_step,
    decay_real,
    freq_imag,
    in_real,
    in_imag,
    out_real,
    out_imag,
    skip_gain,
    out_weight,
    residual,
    post_gain,
    pre_gain,
    final_gain,
    route_ids,
    route_logits,
    expert_gate,
    expert_up,
    expert_down,
):
    devices, quarters = (lax.axis_size("sp"), lax.axis_size("tp"))
    rows, width = residual.shape
    length, wide = (mixer_input.shape[0], decay_real.size)
    channels = mixer_input.shape[1]
    slots = 2 * devices
    message, rates, read, cum_real, cum_imag, own_real, own_imag = call(
        mixer_kernel,
        [
            ((devices, *MESSAGE), BF16),
            ((8, wide), F32),
            ((2 * wide, 2 * channels), BF16),
            ((length, wide), F32),
            ((length, wide), F32),
            ((length, wide), F32),
            ((length, wide), F32),
        ],
        *map(
            in_hbm,
            (
                step_shift.T,
                mixer_input,
                log_step[None],
                decay_real,
                freq_imag,
                jnp.swapaxes(in_real, 1, 2),
                jnp.swapaxes(in_imag, 1, 2),
                out_real,
                out_imag,
            ),
        ),
        flops=10**9,
    )
    got = across_sp(message)
    kept, *sent = call(
        carry_kernel,
        [
            ((rows, width), F32),
            *(((rows, width), BF16),) * (quarters - 1),
        ],
        got, rates, read, cum_real, cum_imag, own_real, own_imag,
        mixer_input,
        skip_gain[None],
        out_weight,
        flops=10**9,
    )
    place, weigh = call(
        route_kernel,
        [((4 * slots, slots), BF16), ((2 * slots, 4 * slots), BF16)],
        route_ids.T,
        route_logits.T,
        flops=10**8,
    )
    stream, outgoing = call(
        project_kernel,
        [((rows, width), BF16), ((4 * slots, width // 4), BF16)],
        kept,
        *(shifted(part, by) for by, part in enumerate(sent, 1)),
        residual,
        post_gain[None],
        pre_gain[None],
        place,
        flops=10**9,
    )
    pieces = (devices, 4 * slots // devices, width // 4)
    arrived = across_sp(outgoing.reshape(pieces))
    summed = run_expert((expert_gate, expert_up, expert_down), arrived.reshape(outgoing.shape))
    results = across_sp(summed.reshape(pieces))
    return call(
        combine_kernel, ((rows, width), BF16),
        results.reshape(outgoing.shape), weigh, stream, final_gain[None], flops=10**9,
    )


def solution(mesh):
    in_specs = (
        P("sp", "tp"),
        P("sp", "tp"),
        P("tp"),
        P("tp", None),
        P("tp", None),
        P("tp", None, None),
        P("tp", None, None),
        P("tp", None, None),
        P("tp", None, None),
        P("tp"),
        P("tp", None),
        P(("sp", "tp"), None),
        P(),
        P(),
        P(),
        P("sp", None),
        P("sp", None),
        P("sp", None, "tp"),
        P("sp", None, "tp"),
        P("sp", "tp", None),
    )
    out_specs = P(("sp", "tp"), None)

    return jax.shard_map(
        on_device, mesh=mesh, in_specs=in_specs, out_specs=out_specs, check_vma=False
    )
```
